256 devices in a mesh: sp: 64 (over z, x, core), tp: 4 (over y).
Axes of the slice: x: 4, y: 4, z: 8, core: 2. Of those that a mesh axis runs over, the one named last changes fastest.
Arguments:
- stratum_source_matrix: bfloat16 [8192, 2048], P('sp'), may hold values from -70 to 70
- acceptance_query: bfloat16 [2, 8192, 1024], P(None, 'sp', 'tp'), may hold values from -6 to 6
- cluster_lookup_matrix: bfloat16 [2, 8192, 1024], P(None, 'sp', 'tp'), may hold values from -6 to 6
- cluster_payload_matrix: bfloat16 [2, 8192, 1024], P(None, 'sp', 'tp'), may hold values from -6 to 6
- fading_logit: bfloat16 [2, 8192, 1024], P(None, 'sp', 'tp'), may hold values from -17 to 2
- adaptation_speed_logit: bfloat16 [2, 8192, 1024], P(None, 'sp', 'tp'), may hold values from -14 to 5
- additional_fading_exponent: float32 [2, 8192, 1024], P(None, 'sp', 'tp'), may hold values from -0.7 to 0
- result_switch_pair: bfloat16 [2, 8192, 1024], P(None, 'sp', 'tp'), may hold values from -6 to 6
- attender_scaling_factor: float32 [2, 1024], P(None, 'tp'), may hold values from 0.1 to 1.9
- present_item_factor: float32 [2, 1024], P(None, 'tp'), may hold values from -0.9 to 0.9
- final_mapping_matrix: bfloat16 [2, 1024, 2048], P(None, 'tp'), may hold values from -0.125 to 0.125
- perceptron_scaling_factor: float32 [2048], replicated, may hold values from 0.1 to 1.9
- switching_matrix: bfloat16 [2048, 5632], P('sp', 'tp'), may hold values from -0.125 to 0.125
- widening_matrix: bfloat16 [2048, 5632], P('sp', 'tp'), may hold values from -0.125 to 0.125
- shrinking_matrix: bfloat16 [5632, 2048], P('tp', 'sp'), may hold values from -0.078125 to 0.078125
Outputs:
- layer_out: bfloat16 [8192, 2048], P('sp', 'tp')
The draws below stay inside these ranges and needn't reach their ends.
All inputs are finite; a program needn't handle non-finite values.
Results may differ from the reference program's by a relative error of at most 0.014.
Values may be sent and summed in bfloat16 or wider, within the bound.
No kernel may reach another device: no remote copies, remote signals or barrier semaphores. Data moves between devices by JAX's collectives and lax.ppermute only.
A program may use at most 128 MiB of HBM per device.

```python
import math
import jax
import jax.numpy as jnp
from jax import lax

D = 2048
FF = 5632
CLUSTER_FEATURES = 1024
DS = 64
DL = 128
TOK_DEV = 128
SEQUENCE_TOKENS = 8192
N_TP = 4


def fast_heads(key):
    fast_share = 0.5
    small_heads = jax.random.uniform(jax.random.fold_in(key, 101), (CLUSTER_FEATURES // DS,)) < fast_share
    large_heads = jax.random.uniform(jax.random.fold_in(key, 102), (CLUSTER_FEATURES // DL,)) < fast_share
    return jnp.stack([jnp.repeat(small_heads, DS), jnp.repeat(large_heads, DL)])


def rough_entries(key):
    return jnp.clip(jax.random.normal(key, (2, SEQUENCE_TOKENS, CLUSTER_FEATURES)), -4.0, 4.0)


def draw_fading_logit(key, part):
    fast_mask = fast_heads(key)
    level = jnp.where(fast_mask, -3.5, -12.0)
    jitter = rough_entries(jax.random.fold_in(key, 201))
    block_shift = jax.random.uniform(jax.random.fold_in(key, 202), (2, SEQUENCE_TOKENS // TOK_DEV, 1), minval=-0.7, maxval=0.7)
    block_shift = jnp.repeat(block_shift, TOK_DEV, axis=1)
    return (level[:, None, :] + jitter + block_shift).astype(jnp.bfloat16)


def draw_adaptation_speed_logit(key, part):
    fast_mask = fast_heads(key)
    slow_small = math.log(0.4 * DS / SEQUENCE_TOKENS)
    slow_large = math.log(0.4 * DL / SEQUENCE_TOKENS)
    slow_level = jnp.stack([jnp.full((CLUSTER_FEATURES,), slow_small, jnp.float32), jnp.full((CLUSTER_FEATURES,), slow_large, jnp.float32)])
    level = jnp.where(fast_mask, 0.0, slow_level)
    jitter = rough_entries(jax.random.fold_in(key, 301))
    return (level[:, None, :] + jitter).astype(jnp.float32).astype(jnp.bfloat16)


def draw_additional_fading_exponent(key, part):
    extra_decay_rows = jax.random.randint(jax.random.fold_in(key, 401), (2, 3), 0, SEQUENCE_TOKENS)
    sequence_positions = jnp.arange(SEQUENCE_TOKENS)
    corrected_state = jnp.any(sequence_positions[None, :, None] == extra_decay_rows[:, None, :], axis=-1)
    extra_decay_depth = jax.random.uniform(jax.random.fold_in(key, 402), (2, SEQUENCE_TOKENS, CLUSTER_FEATURES), minval=math.log(0.5), maxval=math.log(0.8))
    return jnp.where(corrected_state[:, :, None], extra_decay_depth, 0.0).astype(jnp.float32)


def draw_stratum_source_matrix(key, part):
    spread = jnp.arange(D).astype(jnp.float32) / D
    column_scale = 0.5 * 3.0 ** spread * jnp.exp(jax.random.uniform(jax.random.fold_in(key, 501), (D,), minval=-0.6, maxval=0.6))
    row_scale = jnp.exp(jax.random.uniform(jax.random.fold_in(key, 502), (SEQUENCE_TOKENS, 1), minval=math.log(0.4), maxval=math.log(4.0)))
    entries = jnp.clip(jax.random.normal(jax.random.fold_in(key, 503), (SEQUENCE_TOKENS, D)), -6.0, 6.0)
    return (entries * row_scale * column_scale).astype(jnp.float32).astype(jnp.bfloat16)


def levels(own_key, extent, shards, smallest, top_value):
    factor_of = 1.0
    for axis_at, shards_of in shards:
        steps = jax.random.uniform(jax.random.fold_in(jax.random.fold_in(own_key, 6), axis_at), (shards_of,), jnp.float32, smallest / len(shards), top_value / len(shards))
        factor_of = factor_of * jnp.repeat(jnp.exp(steps), extent[axis_at] // shards_of).reshape((-1,) + (1,) * (len(extent) - 1 - axis_at))
    return factor_of


def scatter_about(own_key, dims, width, bound, shards=(), kind=jnp.bfloat16):
    loudness = levels(own_key, dims, shards, -0.22, 0.18) if shards else 1.0
    array = jax.random.normal(own_key, dims, jnp.float32) * width * loudness
    return jnp.minimum(jnp.maximum(array, -bound), bound).astype(kind)


def setup_inputs(seed: int = 0) -> dict:
    arg_keys = jax.random.split(jax.random.key(seed), 16)
    return {
        "stratum_source_matrix": draw_stratum_source_matrix(jax.random.fold_in(arg_keys[15], 71), 0),
        "acceptance_query": scatter_about(arg_keys[1], (2, SEQUENCE_TOKENS, CLUSTER_FEATURES), 1.0, 6.0, ((1, 64), (2, 4))),
        "cluster_lookup_matrix": scatter_about(arg_keys[2], (2, SEQUENCE_TOKENS, CLUSTER_FEATURES), 1.0, 6.0, ((1, 64), (2, 4))),
        "cluster_payload_matrix": scatter_about(arg_keys[3], (2, SEQUENCE_TOKENS, CLUSTER_FEATURES), 1.0, 6.0, ((1, 64), (2, 4))),
        "fading_logit": draw_fading_logit(jax.random.fold_in(arg_keys[15], 71), 0),
        "adaptation_speed_logit": draw_adaptation_speed_logit(jax.random.fold_in(arg_keys[15], 71), 0),
        "additional_fading_exponent": draw_additional_fading_exponent(jax.random.fold_in(arg_keys[15], 71), 0),
        "result_switch_pair": scatter_about(arg_keys[7], (2, SEQUENCE_TOKENS, CLUSTER_FEATURES), 1.0, 6.0, ((1, 64), (2, 4))),
        "attender_scaling_factor": jnp.clip(1.0 + 0.18 * jax.random.normal(arg_keys[8], (2, CLUSTER_FEATURES), jnp.float32), 0.1, 1.9),
        "present_item_factor": scatter_about(arg_keys[9], (2, CLUSTER_FEATURES), 0.15, 0.9, ((1, 4),), jnp.float32),
        "final_mapping_matrix": scatter_about(arg_keys[10], (2, CLUSTER_FEATURES, D), (2 * CLUSTER_FEATURES) ** -0.5, 0.125, ((1, 4),)),
        "perceptron_scaling_factor": jnp.clip(1.0 + 0.18 * jax.random.normal(arg_keys[11], (D,), jnp.float32), 0.1, 1.9),
        "switching_matrix": scatter_about(arg_keys[12], (D, FF), D ** -0.5, 0.125, ((0, 64), (1, 4))),
        "widening_matrix": scatter_about(arg_keys[13], (D, FF), D ** -0.5, 0.125, ((0, 64), (1, 4))),
        "shrinking_matrix": scatter_about(arg_keys[14], (FF, D), FF ** -0.5, 0.078125, ((0, 4), (1, 64))),
    }


highest = lax.Precision.HIGHEST
norm_epsilon = 1e-06
head_epsilon = 0.00064
key_epsilon = 1e-06

def per_head_terms(acceptance_query, cluster_lookup_matrix, cluster_payload_matrix, fading_logit, adaptation_speed_logit, additional_fading_exponent, attender_feature_count):
    row_count, channels = acceptance_query.shape
    lattice_layout = (row_count, channels // attender_feature_count, attender_feature_count)
    acceptance_lines = acceptance_query.astype(jnp.float32).reshape(lattice_layout)
    mapped_lookups = cluster_lookup_matrix.astype(jnp.float32).reshape(lattice_layout)
    mapped_payloads = cluster_payload_matrix.astype(jnp.float32).reshape(lattice_layout)
    learning_rate_logarithm = -jax.nn.softplus(-fading_logit.astype(jnp.float32)) - 0.5
    decay_logarithm = (additional_fading_exponent - jnp.exp(learning_rate_logarithm)).reshape(lattice_layout)
    learn_rate = jax.nn.sigmoid(adaptation_speed_logit.astype(jnp.float32)).reshape(lattice_layout)
    removal = mapped_lookups * lax.rsqrt(lax.optimization_barrier(jnp.sum(mapped_lookups * mapped_lookups, axis=-1, keepdims=True)) + key_epsilon)
    return (acceptance_lines, mapped_lookups, mapped_payloads, decay_logarithm, -removal, learn_rate * removal)

def entire_cluster(raw_retrieval, acceptance_lines, mapped_lookups, mapped_payloads, scaling_array, diagonal_reward_array, switch_amounts):
    row_count, attender_count, attender_feature_count = raw_retrieval.shape
    row_mean = lax.optimization_barrier(jnp.mean(raw_retrieval, axis=-1, keepdims=True))
    centered = raw_retrieval - row_mean
    variance = lax.optimization_barrier(jnp.mean(centered * centered, axis=-1, keepdims=True))
    normed = centered * lax.rsqrt(variance + head_epsilon) * scaling_array.reshape(attender_count, attender_feature_count)
    diagonal_item_contribution = lax.optimization_barrier(jnp.sum(acceptance_lines * mapped_lookups * diagonal_reward_array.reshape(attender_count, attender_feature_count), axis=-1, keepdims=True)) * mapped_payloads
    joined = (normed + diagonal_item_contribution).reshape(row_count, attender_count * attender_feature_count)
    return (joined * switch_amounts.astype(jnp.float32)).astype(jnp.bfloat16)

def advance_one(memory, acceptance_lines, mapped_lookups, mapped_payloads, decay_logarithm, remove_left, remove_right):
    removed = jnp.einsum('hij,hj->hi', memory, remove_left, precision=highest)
    memory = memory * jnp.exp(decay_logarithm)[:, None, :] + removed[:, :, None] * remove_right[:, None, :] + mapped_payloads[:, :, None] * mapped_lookups[:, None, :]
    return (memory, jnp.einsum('hij,hj->hi', memory, acceptance_lines, precision=highest))

def recurrence(terms_small, terms_large):

    def advance(memories, inputs):
        memory_small, read_small = advance_one(memories[0], *inputs[0])
        memory_large, read_large = advance_one(memories[1], *inputs[1])
        return ((memory_small, memory_large), (read_small, read_large))
    initial = tuple((jnp.zeros((aggregated_contributions[0].shape[1], aggregated_contributions[0].shape[2], aggregated_contributions[0].shape[2]), jnp.float32) for aggregated_contributions in (terms_small, terms_large)))
    final_memories, retrieved_result_lines = lax.scan(advance, initial, (terms_small, terms_large))
    return retrieved_result_lines

def reference(stratum_source_matrix, acceptance_query, cluster_lookup_matrix, cluster_payload_matrix, fading_logit, adaptation_speed_logit, additional_fading_exponent, result_switch_pair, attender_scaling_factor, present_item_factor, final_mapping_matrix, perceptron_scaling_factor, switching_matrix, widening_matrix, shrinking_matrix):
    group_widths = (DS, DL)
    aggregated_contributions = [per_head_terms(acceptance_query[cluster_ordinal], cluster_lookup_matrix[cluster_ordinal], cluster_payload_matrix[cluster_ordinal], fading_logit[cluster_ordinal], adaptation_speed_logit[cluster_ordinal], additional_fading_exponent[cluster_ordinal], group_widths[cluster_ordinal]) for cluster_ordinal in range(2)]
    retrieved_result_lines = recurrence(tuple(aggregated_contributions[0]), tuple(aggregated_contributions[1]))
    blended_result = [entire_cluster(retrieved_result_lines[cluster_ordinal], aggregated_contributions[cluster_ordinal][0], aggregated_contributions[cluster_ordinal][1], aggregated_contributions[cluster_ordinal][2], attender_scaling_factor[cluster_ordinal], present_item_factor[cluster_ordinal], result_switch_pair[cluster_ordinal]) for cluster_ordinal in range(2)]
    slice_width = CLUSTER_FEATURES // N_TP
    branch = jnp.zeros((SEQUENCE_TOKENS, D), jnp.float32)
    for slice_index in range(N_TP):
        lower = slice_index * slice_width
        upper = lower + slice_width
        partial_value = jnp.dot(blended_result[0][:, lower:upper], final_mapping_matrix[0, lower:upper], preferred_element_type=jnp.float32) + jnp.dot(blended_result[1][:, lower:upper], final_mapping_matrix[1, lower:upper], preferred_element_type=jnp.float32)
        branch = branch + lax.optimization_barrier(partial_value.astype(jnp.bfloat16)).astype(jnp.float32)
    hidden_state = (stratum_source_matrix.astype(jnp.float32) + branch).astype(jnp.bfloat16)
    state_float = hidden_state.astype(jnp.float32)
    mean_square = lax.optimization_barrier(jnp.mean(state_float * state_float, axis=1, keepdims=True))
    normed = (state_float * lax.rsqrt(mean_square + norm_epsilon) * perceptron_scaling_factor).astype(jnp.bfloat16)
    gate_pre = jnp.dot(normed, switching_matrix, preferred_element_type=jnp.float32)
    up_pre = jnp.dot(normed, widening_matrix, preferred_element_type=jnp.float32)
    activated = (jax.nn.silu(gate_pre) * up_pre).astype(jnp.bfloat16)
    hidden_width = FF // N_TP
    mixer = jnp.zeros((SEQUENCE_TOKENS, D), jnp.float32)
    for slice_index in range(N_TP):
        lower = slice_index * hidden_width
        upper = lower + hidden_width
        partial_value = jnp.dot(activated[:, lower:upper], shrinking_matrix[lower:upper], preferred_element_type=jnp.float32)
        mixer = mixer + lax.optimization_barrier(partial_value.astype(jnp.bfloat16)).astype(jnp.float32)
    return (state_float + mixer).astype(jnp.bfloat16)
```

```python
import jax
import jax.numpy as jnp
from jax import lax
from jax.experimental import pallas as pl
from jax.experimental.pallas import tpu as pltpu
from jax.sharding import Mesh
from jax.sharding import PartitionSpec as P

SP = ("sp_0", "sp_1", "sp_2")
ROW = ("sp_1", "sp_2")
TOK = 128
LANES = 128
HALF = 64
SHARES = 8

norm_epsilon = 1e-06
head_epsilon = 0.00064
key_epsilon = 1e-06

f32 = jnp.float32
bf16 = jnp.bfloat16


def dot_nn(a, b):
    return lax.dot_general(a, b, (((1,), (0,)), ((), ())), preferred_element_type=f32)


def dot_nt(a, b):
    return lax.dot_general(a, b, (((1,), (1,)), ((), ())), preferred_element_type=f32)


def dot_tn(a, b):
    return lax.dot_general(a, b, (((0,), (0,)), ((), ())), preferred_element_type=f32)


def halves(a):
    high = a.astype(bf16)
    return high, (a - high.astype(f32)).astype(bf16)


def mm(a, b):
    ah, al = a
    bh, bl = b
    return dot_nn(jnp.concatenate([ah, al], 1), jnp.concatenate([bh, bh], 0)) + dot_nn(ah, bl)


def mm_nt(a, b):
    ah, al = a
    bh, bl = b
    return dot_nt(jnp.concatenate([ah, al], 1), jnp.concatenate([bh, bh], 1)) + dot_nt(ah, bl)


def mm_tn(a, b):
    ah, al = a
    bh, bl = b
    return dot_tn(jnp.concatenate([ah, al], 0), jnp.concatenate([bh, bh], 0)) + dot_tn(ah, bl)


def head_masks(group):
    lane = lax.broadcasted_iota(jnp.int32, (1, LANES), 1)
    if group == 0:
        return [(lane < HALF).astype(f32), (lane >= HALF).astype(f32)]
    return [None]


def head_sum(a, masks):
    if masks[0] is None:
        return jnp.sum(a, axis=1, keepdims=True)
    return sum(jnp.sum(a * m, axis=1, keepdims=True) * m for m in masks)


def masked(a, mask):
    return a if mask is None else a * mask


def local_kernel(q_ref, k_ref, v_ref, f_ref, l_ref, e_ref, send_ref, out_ref, read_ref):
    row = lax.broadcasted_iota(jnp.int32, (TOK, TOK), 0)
    col = lax.broadcasted_iota(jnp.int32, (TOK, TOK), 1)
    strict = row > col
    inclusive = row >= col
    eye = (row == col).astype(f32)
    ones = inclusive.astype(bf16)
    slots = []
    heads = []
    for slot in range(4):
        group, cut = slot // 2, (slot % 2) * LANES
        lanes = slice(cut, cut + LANES)
        q = q_ref[group, :, lanes].astype(f32)
        k = k_ref[group, :, lanes].astype(f32)
        v = v_ref[group, :, lanes].astype(f32)
        fade = f_ref[group, :, lanes].astype(f32)
        speed = l_ref[group, :, lanes].astype(f32)
        log_decay = e_ref[group, :, lanes] - jnp.exp(-0.5) / (1.0 + jnp.exp(-fade))
        learn = 1.0 / (1.0 + jnp.exp(-speed))
        masks = head_masks(group)
        removal = k * lax.rsqrt(head_sum(k * k, masks) + key_epsilon)
        d0, rest = log_decay.astype(bf16), None
        rest = log_decay - d0.astype(f32)
        d1 = rest.astype(bf16)
        d2 = (rest - d1.astype(f32)).astype(bf16)
        cum = dot_nn(ones, d0) + dot_nn(ones, d1) + dot_nn(ones, d2)
        middle = cum[TOK // 2 : TOK // 2 + 1, :]
        forward = jnp.exp(cum - middle)
        backward = jnp.exp(middle - cum)
        undo = jnp.exp(-log_decay)
        right = learn * removal
        queries = jnp.concatenate([-removal * undo * forward, q * forward], 0)
        sources = halves(jnp.concatenate([right * backward, k * backward], 0))
        grown = jnp.exp(cum)
        final = cum[TOK - 1 : TOK, :]
        tail = jnp.exp(final - cum)
        slots.append(
            dict(
                masks=masks,
                v=halves(v),
                start=-removal * jnp.exp(cum - log_decay),
                grown=q * grown,
                right=halves(right * tail),
                keys=halves(k * tail),
                kept=jnp.exp(final),
                heads=[],
            )
        )
        for mask in masks:
            pairs = mm_nt(halves(masked(queries, mask)), sources)
            head = dict(
                slot=slot,
                mask=mask,
                n=jnp.where(strict, pairs[:TOK, :TOK], 0.0),
                rk=jnp.where(strict, pairs[:TOK, TOK:], 0.0),
                qr=jnp.where(inclusive, pairs[TOK:, :TOK], 0.0),
                qk=jnp.where(inclusive, pairs[TOK:, TOK:], 0.0),
            )
            heads.append(head)
            slots[slot]["heads"].append(head)
    same = (row // 8) == (col // 8)
    for head in heads:
        head["m"] = jnp.where(same, head["n"], 0.0)
        head["x"] = eye + head["m"]
    for _ in range(2):
        for head in heads:
            m = halves(head["m"])
            head["m"] = mm(m, m)
        for head in heads:
            head["x"] = head["x"] + mm(halves(head["x"]), halves(head["m"]))
    size = 8
    while size < TOK:
        below = (row // (2 * size) == col // (2 * size)) & (row // size != col // size)
        for head in heads:
            off = halves(jnp.where(below, head["n"], 0.0))
            head["y"] = halves(mm(off, halves(head["x"])))
        for head in heads:
            head["x"] = head["x"] + mm(halves(head["x"]), head["y"])
        size *= 2
    for slot, part in enumerate(slots):
        carried = start = local = read = None
        for head in part["heads"]:
            mask = head["mask"]
            target = jnp.concatenate([mm(halves(head["rk"]), part["v"]), part["start"]], 1)
            solved = mm(halves(head["x"]), halves(target))
            from_solved = mm(halves(head["qr"]), halves(solved))
            pieces = [
                masked(solved[:, :LANES], mask),
                masked(solved[:, LANES:], mask),
                masked(from_solved[:, :LANES] + mm(halves(head["qk"]), part["v"]), mask),
                masked(from_solved[:, LANES:], mask),
            ]
            if carried is None:
                carried, start, local, read = pieces
            else:
                carried, start, local, read = (
                    carried + pieces[0],
                    start + pieces[1],
                    local + pieces[2],
                    read + pieces[3],
                )
        transit = mm_tn(halves(start), part["right"])
        added = mm_tn(halves(carried), part["right"]) + mm_tn(part["v"], part["keys"])
        if len(part["heads"]) == 2:
            block = (row // HALF) == (col // HALF)
            transit = jnp.where(block, transit, 0.0)
            added = jnp.where(block, added, 0.0)
        transit = (transit + eye * part["kept"]).astype(bf16)
        added = added.astype(bf16)
        for half in range(2):
            send_ref[2 * slot + half, :LANES, :] = transit
            send_ref[2 * slot + half, LANES:, :] = added[half * HALF : (half + 1) * HALF, :]
        out_ref[slot] = local
        read_ref[slot] = part["grown"] + read


def row_kernel(got_ref, prefix_ref, total_ref):
    row = lax.broadcasted_iota(jnp.int32, (LANES + HALF, LANES), 0)
    col = lax.broadcasted_iota(jnp.int32, (LANES + HALF, LANES), 1)
    zero = jnp.zeros((LANES, LANES), f32)
    prefix_ref[0] = (row == col).astype(f32)
    run = got_ref[0].astype(f32)
    for k in range(1, SHARES):
        prefix_ref[k] = run
        got = got_ref[k]
        step = got[:LANES]
        high, low = halves(run)
        run = dot_nn(jnp.concatenate([high, low], 1), jnp.concatenate([step, step], 0))
        run = run + jnp.concatenate([zero, got[LANES:].astype(f32)], 0)
    total = run.astype(bf16)
    for k in range(total_ref.shape[0]):
        total_ref[k] = total


def state_kernel(place_ref, every_ref, prefix_ref, send_ref):
    place = place_ref[0]
    state = jnp.zeros((HALF, LANES), f32)
    for k in range(every_ref.shape[0] - 1):
        got = every_ref[k]
        step = got[:LANES]
        high, low = halves(state)
        grown = dot_nn(jnp.concatenate([high, low], 1), jnp.concatenate([step, step], 0))
        state = jnp.where(k < place, grown + got[LANES:].astype(f32), state)
    split = halves(state)
    for k in range(SHARES):
        moved = mm(split, halves(prefix_ref[k, :LANES, :]))
        send_ref[k] = (moved + prefix_ref[k, LANES:, :]).astype(bf16)


def mix_kernel(
    out_ref, read_ref, state_ref, q_ref, k_ref, v_ref, gate_ref, gain_ref, own_ref, w_ref, y_ref
):
    mixed = []
    for slot in range(4):
        group, cut = slot // 2, (slot % 2) * LANES
        lanes = slice(cut, cut + LANES)
        width = HALF if group == 0 else LANES
        masks = head_masks(group)
        state = jnp.concatenate([state_ref[2 * slot], state_ref[2 * slot + 1]], 0)
        high, low = halves(read_ref[slot])
        raw = out_ref[slot] + dot_nt(
            jnp.concatenate([high, low], 1), jnp.concatenate([state, state], 1)
        )
        centered = raw - head_sum(raw, masks) * (1.0 / width)
        variance = head_sum(centered * centered, masks) * (1.0 / width)
        normed = centered * lax.rsqrt(variance + head_epsilon) * gain_ref[group : group + 1, lanes]
        q = q_ref[group, :, lanes].astype(f32)
        k = k_ref[group, :, lanes].astype(f32)
        v = v_ref[group, :, lanes].astype(f32)
        own = head_sum(q * k * own_ref[group : group + 1, lanes], masks) * v
        mixed.append(((normed + own) * gate_ref[group, :, lanes].astype(f32)).astype(bf16))
    y_ref[...] = dot_nn(jnp.concatenate(mixed, 1), w_ref[...]).astype(bf16)


def call(kernel, outs, scalars=0):
    spec = pl.BlockSpec(memory_space=pltpu.VMEM)
    return lambda *args: pl.pallas_call(
        kernel,
        out_shape=outs,
        in_specs=[pl.BlockSpec(memory_space=pltpu.SMEM)] * scalars + [spec] * (len(args) - scalars),
        out_specs=jax.tree.map(lambda _: spec, outs),
        compiler_params=pltpu.CompilerParams(vmem_limit_bytes=32 * 1024 * 1024),
    )(*args)


def array(dims, kind):
    return jax.ShapeDtypeStruct(dims, kind)


def exchange(value, axis):
    return lax.all_to_all(value, axis, 0, 0, tiled=True)


def from_everyone(value, axis):
    devices = lax.axis_size(axis)
    return exchange(jnp.broadcast_to(value[None], (devices, *value.shape)), axis)


def on_device(
    stratum_source_matrix,
    acceptance_query,
    cluster_lookup_matrix,
    cluster_payload_matrix,
    fading_logit,
    adaptation_speed_logit,
    additional_fading_exponent,
    result_switch_pair,
    attender_scaling_factor,
    present_item_factor,
    final_mapping_matrix,
    perceptron_scaling_factor,
    switching_matrix,
    widening_matrix,
    shrinking_matrix,
):
    hidden = switching_matrix.shape[1]
    features = perceptron_scaling_factor.shape[0]
    whole = lax.all_gather(
        jnp.concatenate([switching_matrix, widening_matrix, shrinking_matrix.T], axis=1),
        SP,
        axis=0,
        tiled=True,
    )
    blocks = array((4, TOK, LANES), f32)
    send, local_out, start_read = call(
        local_kernel, (array((SHARES, LANES + HALF, LANES), bf16), blocks, blocks)
    )(
        acceptance_query,
        cluster_lookup_matrix,
        cluster_payload_matrix,
        fading_logit,
        adaptation_speed_logit,
        additional_fading_exponent,
    )
    planes = lax.axis_size("sp_0")
    prefix, total = call(
        row_kernel,
        (
            array((SHARES, LANES + HALF, LANES), f32),
            array((planes, LANES + HALF, LANES), bf16),
        ),
    )(exchange(send, ROW))
    states = call(state_kernel, array((SHARES, HALF, LANES), bf16), 1)(
        lax.axis_index("sp_0").astype(jnp.int32).reshape(1), exchange(total, "sp_0"), prefix
    )
    partial_value = call(mix_kernel, array((TOK, features), bf16))(
        local_out,
        start_read,
        exchange(states, ROW),
        acceptance_query,
        cluster_lookup_matrix,
        cluster_payload_matrix,
        result_switch_pair,
        attender_scaling_factor,
        present_item_factor,
        final_mapping_matrix.reshape(-1, features),
    )
    columns = features // lax.axis_size("tp")
    own_start = lax.axis_index("tp") * columns
    residual_float = stratum_source_matrix.astype(f32)
    attention = jnp.sum(from_everyone(partial_value, "tp").astype(f32), axis=0)
    state_float = (residual_float + attention).astype(bf16).astype(f32)
    mean_square = jnp.mean(state_float * state_float, axis=1, keepdims=True)
    normed = (
        state_float * lax.rsqrt(mean_square + norm_epsilon) * perceptron_scaling_factor
    ).astype(bf16)
    own_state = lax.dynamic_slice_in_dim(state_float, own_start, columns, 1)
    gate_pre = jnp.dot(normed, whole[:, :hidden], preferred_element_type=f32)
    up_pre = jnp.dot(normed, whole[:, hidden : 2 * hidden], preferred_element_type=f32)
    activated = (jax.nn.silu(gate_pre) * up_pre).astype(bf16)
    down_terms = dot_nt(activated, whole[:, 2 * hidden :]).astype(bf16)
    tiles = jnp.moveaxis(down_terms.reshape(TOK, features // columns, columns), 1, 0)
    mixer = jnp.sum(exchange(tiles, "tp").astype(f32), axis=0)
    return (own_state + mixer).astype(bf16)


def solution(mesh):
    split = Mesh(mesh.devices.reshape(8, 4, 2, mesh.shape["tp"]), ("sp_0", "sp_1", "sp_2", "tp"))
    heads = P(None, SP, "tp")
    return jax.shard_map(
        on_device,
        mesh=split,
        in_specs=(
            P(SP, None),
            heads,
            heads,
            heads,
            heads,
            heads,
            heads,
            heads,
            P(None, "tp"),
            P(None, "tp"),
            P(None, "tp", None),
            P(),
            P(SP, "tp"),
            P(SP, "tp"),
            P("tp", SP),
        ),
        out_specs=P(SP, "tp"),
        check_vma=False,
    )
```

```python
import jax
import jax.numpy as jnp
from jax import lax
from jax.experimental import pallas as pl
from jax.experimental.pallas import tpu as pltpu
from jax.sharding import Mesh
from jax.sharding import PartitionSpec as P

SP = ("sp_0", "sp_1", "sp_2")
ROW = ("sp_1", "sp_2")
TOK = 128
LANES = 128
HALF = 64
SHARES = 8

norm_epsilon = 1e-06
head_epsilon = 0.00064
key_epsilon = 1e-06

f32 = jnp.float32
bf16 = jnp.bfloat16


def dot_nn(a, b):
    return lax.dot_general(a, b, (((1,), (0,)), ((), ())), preferred_element_type=f32)


def dot_nt(a, b):
    return lax.dot_general(a, b, (((1,), (1,)), ((), ())), preferred_element_type=f32)


def dot_tn(a, b):
    return lax.dot_general(a, b, (((0,), (0,)), ((), ())), preferred_element_type=f32)


def halves(a):
    high = a.astype(bf16)
    return high, (a - high.astype(f32)).astype(bf16)


def mm(a, b):
    ah, al = a
    bh, bl = b
    return dot_nn(jnp.concatenate([ah, al], 1), jnp.concatenate([bh, bh], 0)) + dot_nn(ah, bl)


def mm_nt(a, b):
    ah, al = a
    bh, bl = b
    return dot_nt(jnp.concatenate([ah, al], 1), jnp.concatenate([bh, bh], 1)) + dot_nt(ah, bl)


def mm_tn(a, b):
    ah, al = a
    bh, bl = b
    return dot_tn(jnp.concatenate([ah, al], 0), jnp.concatenate([bh, bh], 0)) + dot_tn(ah, bl)


def head_masks(group):
    lane = lax.broadcasted_iota(jnp.int32, (1, LANES), 1)
    if group == 0:
        return [(lane < HALF).astype(f32), (lane >= HALF).astype(f32)]
    return [None]


def head_sum(a, masks):
    if masks[0] is None:
        return jnp.sum(a, axis=1, keepdims=True)
    return sum(jnp.sum(a * m, axis=1, keepdims=True) * m for m in masks)


def masked(a, mask):
    return a if mask is None else a * mask


def fetch(sources, targets, sems):
    copies = [pltpu.make_async_copy(a, b, sems.at[k]) for k, (a, b) in enumerate(zip(sources, targets))]
    for copy in copies:
        copy.start()
    return copies


def local_kernel(*refs):
    inputs, outputs, scratch, sems = refs[:9], refs[9:14], refs[14:23], refs[23]
    send_ref, out_ref, read_ref, scale_ref, extra_ref = outputs
    q_ref, k_ref, v_ref, f_ref, l_ref, e_ref, gate_ref, gain_ref, own_ref = scratch
    for copy in fetch(inputs, scratch, sems):
        copy.wait()
    row = lax.broadcasted_iota(jnp.int32, (TOK, TOK), 0)
    col = lax.broadcasted_iota(jnp.int32, (TOK, TOK), 1)
    strict = row > col
    inclusive = row >= col
    eye = (row == col).astype(f32)
    ones = inclusive.astype(bf16)
    slots = []
    heads = []
    for slot in range(4):
        group, cut = slot // 2, (slot % 2) * LANES
        lanes = slice(cut, cut + LANES)
        q = q_ref[group, :, lanes].astype(f32)
        k = k_ref[group, :, lanes].astype(f32)
        v = v_ref[group, :, lanes].astype(f32)
        fade = f_ref[group, :, lanes].astype(f32)
        speed = l_ref[group, :, lanes].astype(f32)
        log_decay = e_ref[group, :, lanes] - jnp.exp(-0.5) / (1.0 + jnp.exp(-fade))
        learn = 1.0 / (1.0 + jnp.exp(-speed))
        masks = head_masks(group)
        removal = k * lax.rsqrt(head_sum(k * k, masks) + key_epsilon)
        gate = gate_ref[group, :, lanes].astype(f32)
        scale_ref[slot] = gain_ref[group : group + 1, lanes] * gate
        own = head_sum(q * k * own_ref[group : group + 1, lanes], masks)
        extra_ref[slot] = own * v * gate
        d0 = log_decay.astype(bf16)
        rest = log_decay - d0.astype(f32)
        d1 = rest.astype(bf16)
        d2 = (rest - d1.astype(f32)).astype(bf16)
        cum = dot_nn(ones, d0) + dot_nn(ones, d1) + dot_nn(ones, d2)
        middle = cum[TOK // 2 : TOK // 2 + 1, :]
        forward = jnp.exp(cum - middle)
        backward = jnp.exp(middle - cum)
        undo = jnp.exp(-log_decay)
        right = learn * removal
        queries = jnp.concatenate([-removal * undo * forward, q * forward], 0)
        sources = halves(jnp.concatenate([right * backward, k * backward], 0))
        grown = jnp.exp(cum)
        final = cum[TOK - 1 : TOK, :]
        tail = jnp.exp(final - cum)
        slots.append(
            dict(
                masks=masks,
                v=halves(v),
                start=-removal * jnp.exp(cum - log_decay),
                grown=q * grown,
                right=halves(right * tail),
                keys=halves(k * tail),
                kept=jnp.exp(final),
                heads=[],
            )
        )
        for mask in masks:
            pairs = mm_nt(halves(masked(queries, mask)), sources)
            head = dict(
                slot=slot,
                mask=mask,
                n=jnp.where(strict, pairs[:TOK, :TOK], 0.0),
                rk=jnp.where(strict, pairs[:TOK, TOK:], 0.0),
                qr=jnp.where(inclusive, pairs[TOK:, :TOK], 0.0),
                qk=jnp.where(inclusive, pairs[TOK:, TOK:], 0.0),
            )
            heads.append(head)
            slots[slot]["heads"].append(head)
    same = (row // 8) == (col // 8)
    for head in heads:
        head["m"] = jnp.where(same, head["n"], 0.0)
        head["x"] = eye + head["m"]
    for _ in range(2):
        for head in heads:
            m = halves(head["m"])
            head["m"] = mm(m, m)
        for head in heads:
            head["x"] = head["x"] + mm(halves(head["x"]), halves(head["m"]))
    size = 8
    while size < TOK:
        below = (row // (2 * size) == col // (2 * size)) & (row // size != col // size)
        for head in heads:
            off = halves(jnp.where(below, head["n"], 0.0))
            head["y"] = halves(mm(off, halves(head["x"])))
        for head in heads:
            head["x"] = head["x"] + mm(halves(head["x"]), head["y"])
        size *= 2
    for slot, part in enumerate(slots):
        carried = start = local = read = None
        for head in part["heads"]:
            mask = head["mask"]
            target = jnp.concatenate([mm(halves(head["rk"]), part["v"]), part["start"]], 1)
            solved = mm(halves(head["x"]), halves(target))
            from_solved = mm(halves(head["qr"]), halves(solved))
            pieces = [
                masked(solved[:, :LANES], mask),
                masked(solved[:, LANES:], mask),
                masked(from_solved[:, :LANES] + mm(halves(head["qk"]), part["v"]), mask),
                masked(from_solved[:, LANES:], mask),
            ]
            if carried is None:
                carried, start, local, read = pieces
            else:
                carried, start, local, read = (
                    carried + pieces[0],
                    start + pieces[1],
                    local + pieces[2],
                    read + pieces[3],
                )
        transit = mm_tn(halves(start), part["right"])
        added = mm_tn(halves(carried), part["right"]) + mm_tn(part["v"], part["keys"])
        if len(part["heads"]) == 2:
            block = (row // HALF) == (col // HALF)
            transit = jnp.where(block, transit, 0.0)
            added = jnp.where(block, added, 0.0)
        transit = (transit + eye * part["kept"]).astype(bf16)
        added = added.astype(bf16)
        for half in range(2):
            send_ref[2 * slot + half, :LANES, :] = transit
            send_ref[2 * slot + half, LANES:, :] = added[half * HALF : (half + 1) * HALF, :]
        out_ref[slot] = local
        high, low = halves(part["grown"] + read)
        read_ref[slot, :, :LANES] = high
        read_ref[slot, :, LANES:] = low


def row_kernel(got_ref, prefix_ref, total_ref):
    row = lax.broadcasted_iota(jnp.int32, (LANES + HALF, LANES), 0)
    col = lax.broadcasted_iota(jnp.int32, (LANES + HALF, LANES), 1)
    zero = jnp.zeros((LANES, LANES), f32)
    prefix_ref[0] = (row == col).astype(f32)
    run = got_ref[0].astype(f32)
    for k in range(1, SHARES):
        prefix_ref[k] = run
        got = got_ref[k]
        step = got[:LANES]
        high, low = halves(run)
        run = dot_nn(jnp.concatenate([high, low], 1), jnp.concatenate([step, step], 0))
        run = run + jnp.concatenate([zero, got[LANES:].astype(f32)], 0)
    total = run.astype(bf16)
    for k in range(total_ref.shape[0]):
        total_ref[k] = total


def state_kernel(place_ref, every_ref, prefix_ref, send_ref):
    place = place_ref[0]
    state = jnp.zeros((HALF, LANES), f32)
    for k in range(every_ref.shape[0] - 1):
        got = every_ref[k]
        step = got[:LANES]
        high, low = halves(state)
        grown = dot_nn(jnp.concatenate([high, low], 1), jnp.concatenate([step, step], 0))
        state = jnp.where(k < place, grown + got[LANES:].astype(f32), state)
    split = halves(state)
    for k in range(SHARES):
        moved = mm(split, halves(prefix_ref[k, :LANES, :]))
        send_ref[k] = (moved + prefix_ref[k, LANES:, :]).astype(bf16)


def mix_kernel(
    out_ref, read_ref, scale_ref, extra_ref, state_ref, weight_ref, y_ref, w_ref, sems
):
    (copy,) = fetch([weight_ref], [w_ref], sems)
    mixed = []
    for slot in range(4):
        width = HALF if slot < 2 else LANES
        masks = head_masks(slot // 2)
        state = jnp.concatenate([state_ref[2 * slot], state_ref[2 * slot + 1]], 0)
        raw = out_ref[slot] + dot_nt(read_ref[slot], jnp.concatenate([state, state], 1))
        centered = raw - head_sum(raw, masks) * (1.0 / width)
        variance = head_sum(centered * centered, masks) * (1.0 / width)
        normed = centered * lax.rsqrt(variance + head_epsilon) * scale_ref[slot]
        mixed.append((normed + extra_ref[slot]).astype(bf16))
    copy.wait()
    y_ref[...] = dot_nn(jnp.concatenate(mixed, 1), w_ref[...]).astype(bf16)


AHEAD = 4


def feed_kernel(x_ref, whole_ref, y_ref, pair_ref, down_ref, act_ref, sems):
    hidden = whole_ref.shape[1] // 3
    steps = hidden // LANES
    tiles, _, rows = y_ref.shape
    waves = []
    for k in range(steps):
        for part in range(2):
            lanes = pl.ds(part * hidden + k * LANES, LANES)
            target = pair_ref.at[k, :, pl.ds(part * LANES, LANES)]
            waves.append((whole_ref.at[:, lanes], target))
    for k in range(tiles):
        waves.append((whole_ref.at[pl.ds(k * rows, rows), pl.ds(2 * hidden, hidden)], down_ref.at[k]))
    copies = [pltpu.make_async_copy(a, b, sems.at[k]) for k, (a, b) in enumerate(waves)]
    for copy in copies[: 2 * AHEAD]:
        copy.start()
    sent = 2 * AHEAD
    x = x_ref[...]
    for k in range(steps):
        copies[2 * k].wait()
        copies[2 * k + 1].wait()
        for _ in range(2):
            if sent < len(copies):
                copies[sent].start()
                sent += 1
        both = dot_nn(x, pair_ref[k])
        gate = both[:, :LANES]
        active = gate / (1.0 + jnp.exp(-gate)) * both[:, LANES:]
        act_ref[:, k * LANES : (k + 1) * LANES] = active.astype(bf16)
    active = act_ref[...]
    for k in range(tiles):
        copies[2 * steps + k].wait()
        y_ref[k] = dot_nt(active, down_ref[k]).astype(bf16)


def feed_forward(normed, whole, tiles):
    tokens, features = normed.shape
    hidden = whole.shape[1] // 3
    steps = hidden // LANES
    rows = features // tiles
    return pl.pallas_call(
        feed_kernel,
        out_shape=array((tiles, tokens, rows), bf16),
        in_specs=[VMEM, HBM],
        out_specs=VMEM,
        scratch_shapes=[
            pltpu.VMEM((steps, features, 2 * LANES), bf16),
            pltpu.VMEM((tiles, rows, hidden), bf16),
            pltpu.VMEM((tokens, hidden), bf16),
            pltpu.SemaphoreType.DMA((2 * steps + tiles,)),
        ],
        compiler_params=pltpu.CompilerParams(vmem_limit_bytes=40 * 1024 * 1024),
    )(normed, whole)


VMEM = pl.BlockSpec(memory_space=pltpu.VMEM)
HBM = pl.BlockSpec(memory_space=pltpu.HBM)
SMEM = pl.BlockSpec(memory_space=pltpu.SMEM)


def call(kernel, outs, specs, fetched=(), limit=24 * 1024 * 1024):
    scratch = [pltpu.VMEM(a.shape, a.dtype) for a in fetched]
    if scratch:
        scratch.append(pltpu.SemaphoreType.DMA((len(scratch),)))
    return pl.pallas_call(
        kernel,
        out_shape=outs,
        in_specs=specs,
        out_specs=jax.tree.map(lambda _: VMEM, outs),
        scratch_shapes=scratch,
        compiler_params=pltpu.CompilerParams(vmem_limit_bytes=limit),
    )


def array(dims, kind):
    return jax.ShapeDtypeStruct(dims, kind)


def exchange(value, axis):
    return lax.all_to_all(value, axis, 0, 0, tiled=True)


def from_everyone(value, axis):
    devices = lax.axis_size(axis)
    return exchange(jnp.broadcast_to(value[None], (devices, *value.shape)), axis)


def on_device(
    stratum_source_matrix,
    acceptance_query,
    cluster_lookup_matrix,
    cluster_payload_matrix,
    fading_logit,
    adaptation_speed_logit,
    additional_fading_exponent,
    result_switch_pair,
    attender_scaling_factor,
    present_item_factor,
    final_mapping_matrix,
    perceptron_scaling_factor,
    switching_matrix,
    widening_matrix,
    shrinking_matrix,
):
    features = perceptron_scaling_factor.shape[0]
    whole = lax.all_gather(
        jnp.concatenate([switching_matrix, widening_matrix, shrinking_matrix.T], axis=1),
        SP,
        axis=0,
        tiled=True,
    )
    blocks = array((4, TOK, LANES), f32)
    inputs = (
        acceptance_query,
        cluster_lookup_matrix,
        cluster_payload_matrix,
        fading_logit,
        adaptation_speed_logit,
        additional_fading_exponent,
        result_switch_pair,
        attender_scaling_factor,
        present_item_factor,
    )
    send, local_out, start_read, scale, extra = call(
        local_kernel,
        (
            array((SHARES, LANES + HALF, LANES), bf16),
            blocks,
            array((4, TOK, 2 * LANES), bf16),
            blocks,
            blocks,
        ),
        [HBM] * len(inputs),
        inputs,
        66_400_000,
    )(*inputs)
    planes = lax.axis_size("sp_0")
    prefix, total = call(
        row_kernel,
        (
            array((SHARES, LANES + HALF, LANES), f32),
            array((planes, LANES + HALF, LANES), bf16),
        ),
        [VMEM],
    )(exchange(send, ROW))
    states = call(state_kernel, array((SHARES, HALF, LANES), bf16), [SMEM, VMEM, VMEM])(
        lax.axis_index("sp_0").astype(jnp.int32).reshape(1), exchange(total, "sp_0"), prefix
    )
    mapping = final_mapping_matrix.reshape(-1, features)
    partial_value = call(mix_kernel, array((TOK, features), bf16), [VMEM] * 5 + [HBM], (mapping,), 64_000_000)(
        local_out, start_read, scale, extra, exchange(states, ROW), mapping
    )
    columns = features // lax.axis_size("tp")
    own_start = lax.axis_index("tp") * columns
    residual_float = stratum_source_matrix.astype(f32)
    attention = jnp.sum(from_everyone(partial_value, "tp").astype(f32), axis=0)
    state_float = (residual_float + attention).astype(bf16).astype(f32)
    mean_square = jnp.mean(state_float * state_float, axis=1, keepdims=True)
    normed = (
        state_float * lax.rsqrt(mean_square + norm_epsilon) * perceptron_scaling_factor
    ).astype(bf16)
    own_state = lax.dynamic_slice_in_dim(state_float, own_start, columns, 1)
    tiles = feed_forward(normed, whole, features // columns)
    mixer = jnp.sum(exchange(tiles, "tp").astype(f32), axis=0)
    return (own_state + mixer).astype(bf16)


def solution(mesh):
    split = Mesh(mesh.devices.reshape(8, 4, 2, mesh.shape["tp"]), ("sp_0", "sp_1", "sp_2", "tp"))
    heads = P(None, SP, "tp")
    return jax.shard_map(
        on_device,
        mesh=split,
        in_specs=(
            P(SP, None),
            heads,
            heads,
            heads,
            heads,
            heads,
            heads,
            heads,
            P(None, "tp"),
            P(None, "tp"),
            P(None, "tp", None),
            P(),
            P(SP, "tp"),
            P(SP, "tp"),
            P("tp", SP),
        ),
        out_specs=P(SP, "tp"),
        check_vma=False,
    )
```

```python
import jax
import jax.numpy as jnp
from jax import lax
from jax.experimental import pallas as pl
from jax.experimental.pallas import tpu as pltpu
from jax.sharding import Mesh
from jax.sharding import PartitionSpec as P

PLANE, FAR, NEAR, CORE, TP = "plane", "far", "near", "core", "tp"
SP = (PLANE, FAR, NEAR, CORE)
ROW = (FAR, NEAR, CORE)
GATHER = (PLANE, NEAR, CORE)
POOL = (FAR, TP)
TOK = 128
LANES = 128
HALF = 64
SHARES = 8

norm_epsilon = 1e-06
head_epsilon = 0.00064
key_epsilon = 1e-06

f32 = jnp.float32
bf16 = jnp.bfloat16


def dot_nn(a, b):
    return lax.dot_general(a, b, (((1,), (0,)), ((), ())), preferred_element_type=f32)


def dot_nt(a, b):
    return lax.dot_general(a, b, (((1,), (1,)), ((), ())), preferred_element_type=f32)


def dot_tn(a, b):
    return lax.dot_general(a, b, (((0,), (0,)), ((), ())), preferred_element_type=f32)


def halves(a):
    high = a.astype(bf16)
    return high, (a - high.astype(f32)).astype(bf16)


def mm(a, b):
    ah, al = a
    bh, bl = b
    return dot_nn(jnp.concatenate([ah, al], 1), jnp.concatenate([bh, bh], 0)) + dot_nn(ah, bl)


def mm_nt(a, b):
    ah, al = a
    bh, bl = b
    return dot_nt(jnp.concatenate([ah, al], 1), jnp.concatenate([bh, bh], 1)) + dot_nt(ah, bl)


def mm_tn(a, b):
    ah, al = a
    bh, bl = b
    return dot_tn(jnp.concatenate([ah, al], 0), jnp.concatenate([bh, bh], 0)) + dot_tn(ah, bl)


def head_masks(group):
    lane = lax.broadcasted_iota(jnp.int32, (1, LANES), 1)
    if group == 0:
        return [(lane < HALF).astype(f32), (lane >= HALF).astype(f32)]
    return [None]


def head_sum(a, masks):
    if masks[0] is None:
        return jnp.sum(a, axis=1, keepdims=True)
    return sum(jnp.sum(a * m, axis=1, keepdims=True) * m for m in masks)


def masked(a, mask):
    return a if mask is None else a * mask


def fetch(sources, targets, sems):
    copies = [pltpu.make_async_copy(a, b, sems.at[k]) for k, (a, b) in enumerate(zip(sources, targets))]
    for copy in copies:
        copy.start()
    return copies


def local_kernel(*refs):
    inputs, outputs, scratch, sems = refs[:9], refs[9:14], refs[14:23], refs[23]
    send_ref, out_ref, read_ref, scale_ref, extra_ref = outputs
    q_ref, k_ref, v_ref, f_ref, l_ref, e_ref, gate_ref, gain_ref, own_ref = scratch
    for copy in fetch(inputs, scratch, sems):
        copy.wait()
    row = lax.broadcasted_iota(jnp.int32, (TOK, TOK), 0)
    col = lax.broadcasted_iota(jnp.int32, (TOK, TOK), 1)
    strict = row > col
    inclusive = row >= col
    eye = (row == col).astype(f32)
    ones = inclusive.astype(bf16)
    slots = []
    heads = []
    for slot in range(4):
        group, cut = slot // 2, (slot % 2) * LANES
        lanes = slice(cut, cut + LANES)
        q = q_ref[group, :, lanes].astype(f32)
        k = k_ref[group, :, lanes].astype(f32)
        v = v_ref[group, :, lanes].astype(f32)
        fade = f_ref[group, :, lanes].astype(f32)
        speed = l_ref[group, :, lanes].astype(f32)
        log_decay = e_ref[group, :, lanes] - jnp.exp(-0.5) / (1.0 + jnp.exp(-fade))
        learn = 1.0 / (1.0 + jnp.exp(-speed))
        masks = head_masks(group)
        removal = k * lax.rsqrt(head_sum(k * k, masks) + key_epsilon)
        gate = gate_ref[group, :, lanes].astype(f32)
        scale_ref[slot] = gain_ref[group : group + 1, lanes] * gate
        own = head_sum(q * k * own_ref[group : group + 1, lanes], masks)
        extra_ref[slot] = own * v * gate
        d0 = log_decay.astype(bf16)
        rest = log_decay - d0.astype(f32)
        d1 = rest.astype(bf16)
        d2 = (rest - d1.astype(f32)).astype(bf16)
        cum = dot_nn(ones, d0) + dot_nn(ones, d1) + dot_nn(ones, d2)
        middle = cum[TOK // 2 : TOK // 2 + 1, :]
        forward = jnp.exp(cum - middle)
        backward = jnp.exp(middle - cum)
        undo = jnp.exp(-log_decay)
        right = learn * removal
        queries = jnp.concatenate([-removal * undo * forward, q * forward], 0)
        sources = halves(jnp.concatenate([right * backward, k * backward], 0))
        grown = jnp.exp(cum)
        final = cum[TOK - 1 : TOK, :]
        tail = jnp.exp(final - cum)
        slots.append(
            dict(
                masks=masks,
                v=halves(v),
                start=-removal * jnp.exp(cum - log_decay),
                grown=q * grown,
                right=halves(right * tail),
                keys=halves(k * tail),
                kept=jnp.exp(final),
                heads=[],
            )
        )
        for mask in masks:
            pairs = mm_nt(halves(masked(queries, mask)), sources)
            head = dict(
                slot=slot,
                mask=mask,
                n=jnp.where(strict, pairs[:TOK, :TOK], 0.0),
                rk=jnp.where(strict, pairs[:TOK, TOK:], 0.0),
                qr=jnp.where(inclusive, pairs[TOK:, :TOK], 0.0),
                qk=jnp.where(inclusive, pairs[TOK:, TOK:], 0.0),
            )
            heads.append(head)
            slots[slot]["heads"].append(head)
    same = (row // 8) == (col // 8)
    for head in heads:
        head["m"] = jnp.where(same, head["n"], 0.0)
        head["x"] = eye + head["m"]
    for _ in range(2):
        for head in heads:
            m = halves(head["m"])
            head["m"] = mm(m, m)
        for head in heads:
            head["x"] = head["x"] + mm(halves(head["x"]), halves(head["m"]))
    size = 8
    while size < TOK:
        below = (row // (2 * size) == col // (2 * size)) & (row // size != col // size)
        for head in heads:
            off = halves(jnp.where(below, head["n"], 0.0))
            head["y"] = halves(mm(off, halves(head["x"])))
        for head in heads:
            head["x"] = head["x"] + mm(halves(head["x"]), head["y"])
        size *= 2
    for slot, part in enumerate(slots):
        carried = start = local = read = None
        for head in part["heads"]:
            mask = head["mask"]
            target = jnp.concatenate([mm(halves(head["rk"]), part["v"]), part["start"]], 1)
            solved = mm(halves(head["x"]), halves(target))
            from_solved = mm(halves(head["qr"]), halves(solved))
            pieces = [
                masked(solved[:, :LANES], mask),
                masked(solved[:, LANES:], mask),
                masked(from_solved[:, :LANES] + mm(halves(head["qk"]), part["v"]), mask),
                masked(from_solved[:, LANES:], mask),
            ]
            if carried is None:
                carried, start, local, read = pieces
            else:
                carried, start, local, read = (
                    carried + pieces[0],
                    start + pieces[1],
                    local + pieces[2],
                    read + pieces[3],
                )
        transit = mm_tn(halves(start), part["right"])
        added = mm_tn(halves(carried), part["right"]) + mm_tn(part["v"], part["keys"])
        if len(part["heads"]) == 2:
            block = (row // HALF) == (col // HALF)
            transit = jnp.where(block, transit, 0.0)
            added = jnp.where(block, added, 0.0)
        transit = (transit + eye * part["kept"]).astype(bf16)
        added = added.astype(bf16)
        for half in range(2):
            send_ref[2 * slot + half, :LANES, :] = transit
            send_ref[2 * slot + half, LANES:, :] = added[half * HALF : (half + 1) * HALF, :]
        out_ref[slot] = local
        high, low = halves(part["grown"] + read)
        read_ref[slot, :, :LANES] = high
        read_ref[slot, :, LANES:] = low


def row_kernel(got_ref, prefix_ref, total_ref):
    row = lax.broadcasted_iota(jnp.int32, (LANES + HALF, LANES), 0)
    col = lax.broadcasted_iota(jnp.int32, (LANES + HALF, LANES), 1)
    zero = jnp.zeros((LANES, LANES), f32)
    prefix_ref[0] = (row == col).astype(f32)
    run = got_ref[0].astype(f32)
    for k in range(1, SHARES):
        prefix_ref[k] = run
        got = got_ref[k]
        step = got[:LANES]
        high, low = halves(run)
        run = dot_nn(jnp.concatenate([high, low], 1), jnp.concatenate([step, step], 0))
        run = run + jnp.concatenate([zero, got[LANES:].astype(f32)], 0)
    total = run.astype(bf16)
    for k in range(total_ref.shape[0]):
        total_ref[k] = total


def state_kernel(place_ref, every_ref, prefix_ref, send_ref):
    place = place_ref[0]
    state = jnp.zeros((HALF, LANES), f32)
    for k in range(every_ref.shape[0] - 1):
        got = every_ref[k]
        step = got[:LANES]
        high, low = halves(state)
        grown = dot_nn(jnp.concatenate([high, low], 1), jnp.concatenate([step, step], 0))
        state = jnp.where(k < place, grown + got[LANES:].astype(f32), state)
    split = halves(state)
    for k in range(SHARES):
        moved = mm(split, halves(prefix_ref[k, :LANES, :]))
        send_ref[k] = (moved + prefix_ref[k, LANES:, :]).astype(bf16)


def mix_kernel(*refs):
    inputs, y_ref, scratch, sems = refs[:6], refs[6], refs[7:13], refs[13]
    out_ref, read_ref, scale_ref, extra_ref, state_ref, w_ref = scratch
    copies = fetch(inputs, scratch, sems)
    for copy in copies[:5]:
        copy.wait()
    mixed = []
    for slot in range(4):
        width = HALF if slot < 2 else LANES
        masks = head_masks(slot // 2)
        state = jnp.concatenate([state_ref[2 * slot], state_ref[2 * slot + 1]], 0)
        raw = out_ref[slot] + dot_nt(read_ref[slot], jnp.concatenate([state, state], 1))
        centered = raw - head_sum(raw, masks) * (1.0 / width)
        variance = head_sum(centered * centered, masks) * (1.0 / width)
        normed = centered * lax.rsqrt(variance + head_epsilon) * scale_ref[slot]
        mixed.append((normed + extra_ref[slot]).astype(bf16))
    mixed = jnp.concatenate(mixed, 1)
    copies[5].wait()
    tiles, _, columns = y_ref.shape
    for k in range(tiles):
        y_ref[k] = dot_nn(mixed, w_ref[:, k * columns : (k + 1) * columns]).astype(bf16)


AHEAD = 4


def feed_kernel(far_ref, x_ref, gain_ref, whole_ref, y_ref, w_ref, n_ref, acc_ref, sems):
    planes, sides, near, rows, width = w_ref.shape
    third = width // 3
    far = far_ref[0]
    copies = [
        [
            pltpu.make_async_copy(
                whole_ref.at[k, :, jnp.where(far == side, 0, 1)],
                w_ref.at[k, side],
                sems.at[k, side],
            )
            for side in range(sides)
        ]
        for k in range(planes)
    ]
    for k in range(AHEAD):
        for copy in copies[k]:
            copy.start()
    shares, tokens, columns = x_ref.shape
    tiles = shares // sides
    for side in range(sides):
        parts = [x_ref[side * tiles + k].astype(f32) for k in range(tiles)]
        total = sum(jnp.sum(a * a, axis=1, keepdims=True) for a in parts)
        scale = lax.rsqrt(total * (1.0 / (tiles * columns)) + norm_epsilon)
        for k, a in enumerate(parts):
            lanes = slice(k * columns, (k + 1) * columns)
            n_ref[side * tokens : (side + 1) * tokens, lanes] = (
                a * scale * gain_ref[:, lanes]
            ).astype(bf16)
    block = sides * near * rows
    for k in range(0, planes, 2):
        for step in (k, k + 1):
            for copy in copies[step]:
                copy.wait()
            if step + AHEAD < planes:
                for copy in copies[step + AHEAD]:
                    copy.start()
        part = dot_nn(
            n_ref[:, k * block : (k + 2) * block],
            w_ref[k : k + 2, :, :, :, : 2 * third].reshape(2 * block, 2 * third),
        )
        if k == 0:
            acc_ref[...] = part
        else:
            acc_ref[...] += part
    gate = acc_ref[:, :third]
    active = (gate / (1.0 + jnp.exp(-gate)) * acc_ref[:, third:]).astype(bf16)
    per = planes // tiles
    for k in range(tiles):
        down = w_ref[k * per : (k + 1) * per, :, :, :, 2 * third :].reshape(per * block, third)
        out = dot_nt(active, down).astype(bf16)
        for side in range(sides):
            y_ref[side * tiles + k] = out[side * tokens : (side + 1) * tokens]


def feed_forward(far, state, gain, whole):
    planes, near, sides, rows, width = whole.shape
    shares, tokens, columns = state.shape
    return pl.pallas_call(
        feed_kernel,
        out_shape=array((shares, tokens, columns), bf16),
        in_specs=[SMEM, VMEM, VMEM, HBM],
        out_specs=VMEM,
        scratch_shapes=[
            pltpu.VMEM((planes, sides, near, rows, width), bf16),
            pltpu.VMEM((sides * tokens, gain.shape[1]), bf16),
            pltpu.VMEM((sides * tokens, 2 * width // 3), f32),
            pltpu.SemaphoreType.DMA((planes, sides)),
        ],
        compiler_params=pltpu.CompilerParams(vmem_limit_bytes=60_000_000),
    )(far, state, gain, whole)


def halved(value, side, wide):
    part = value[:, side * wide : (side + 1) * wide]
    return jnp.pad(part, ((0, 0), (0, wide - part.shape[1])))


def swapped(parts):
    rows, hidden = parts[0].shape
    wide = -(-hidden // (2 * LANES)) * LANES
    packed = [jnp.concatenate([halved(a, side, wide) for a in parts], axis=1) for side in range(2)]
    first = lax.axis_index(FAR) == 0
    kept = jnp.where(first, packed[0], packed[1])
    given = jnp.where(first, packed[1], packed[0])
    return kept, lax.ppermute(given, FAR, [(0, 1), (1, 0)])


def gathered(kept, taken):
    both = jnp.concatenate([kept, taken], axis=0)
    whole = lax.all_gather(both, GATHER, axis=0, tiled=True)
    planes = lax.axis_size(PLANE)
    near = lax.axis_size(NEAR) * lax.axis_size(CORE)
    return whole.reshape(planes, near, 2, *kept.shape)


VMEM = pl.BlockSpec(memory_space=pltpu.VMEM)
HBM = pl.BlockSpec(memory_space=pltpu.HBM)
SMEM = pl.BlockSpec(memory_space=pltpu.SMEM)


def call(kernel, outs, specs, fetched=(), limit=24 * 1024 * 1024):
    scratch = [pltpu.VMEM(a.shape, a.dtype) for a in fetched]
    if scratch:
        scratch.append(pltpu.SemaphoreType.DMA((len(scratch),)))
    return pl.pallas_call(
        kernel,
        out_shape=outs,
        in_specs=specs,
        out_specs=jax.tree.map(lambda _: VMEM, outs),
        scratch_shapes=scratch,
        compiler_params=pltpu.CompilerParams(vmem_limit_bytes=limit),
    )


def array(dims, kind):
    return jax.ShapeDtypeStruct(dims, kind)


def exchange(value, axis):
    return lax.all_to_all(value, axis, 0, 0, tiled=True)


def from_everyone(value, axis):
    devices = lax.psum(1, axis)
    return exchange(jnp.broadcast_to(value[None], (devices, *value.shape)), axis)


def on_device(
    stratum_source_matrix,
    acceptance_query,
    cluster_lookup_matrix,
    cluster_payload_matrix,
    fading_logit,
    adaptation_speed_logit,
    additional_fading_exponent,
    result_switch_pair,
    attender_scaling_factor,
    present_item_factor,
    final_mapping_matrix,
    perceptron_scaling_factor,
    switching_matrix,
    widening_matrix,
    shrinking_matrix,
):
    features = perceptron_scaling_factor.shape[0]
    columns = features // lax.axis_size(TP)
    kept, taken = swapped([switching_matrix, widening_matrix, shrinking_matrix.T])
    blocks = array((4, TOK, LANES), f32)
    inputs = (
        acceptance_query,
        cluster_lookup_matrix,
        cluster_payload_matrix,
        fading_logit,
        adaptation_speed_logit,
        additional_fading_exponent,
        result_switch_pair,
        attender_scaling_factor,
        present_item_factor,
    )
    send, local_out, start_read, scale, extra = call(
        local_kernel,
        (
            array((SHARES, LANES + HALF, LANES), bf16),
            blocks,
            array((4, TOK, 2 * LANES), bf16),
            blocks,
            blocks,
        ),
        [HBM] * len(inputs),
        inputs,
        66_400_000,
    )(*inputs)
    send, taken = lax.optimization_barrier((send, taken))
    whole = gathered(kept, taken)
    planes = lax.axis_size(PLANE)
    prefix, total = call(
        row_kernel,
        (
            array((SHARES, LANES + HALF, LANES), f32),
            array((planes, LANES + HALF, LANES), bf16),
        ),
        [VMEM],
    )(exchange(send, ROW))
    states = call(state_kernel, array((SHARES, HALF, LANES), bf16), [SMEM, VMEM, VMEM])(
        lax.axis_index(PLANE).astype(jnp.int32).reshape(1), exchange(total, PLANE), prefix
    )
    mixing = (
        local_out,
        start_read,
        scale,
        extra,
        exchange(states, ROW),
        final_mapping_matrix.reshape(-1, features),
    )
    terms = call(
        mix_kernel,
        array((features // columns, TOK, columns), bf16),
        [HBM] * len(mixing),
        mixing,
        64_000_000,
    )(*mixing)
    residual = lax.dynamic_slice_in_dim(
        stratum_source_matrix, lax.axis_index(TP) * columns, columns, 1
    )
    attention = jnp.sum(exchange(terms, TP).astype(f32), axis=0)
    own_state = (residual.astype(f32) + attention).astype(bf16)
    tiles = feed_forward(
        lax.axis_index(FAR).astype(jnp.int32).reshape(1),
        from_everyone(own_state, POOL),
        perceptron_scaling_factor.reshape(1, features),
        whole,
    )
    mixer = jnp.sum(exchange(tiles, POOL).astype(f32), axis=0)
    return (own_state.astype(f32) + mixer).astype(bf16)


def solution(mesh):
    split = Mesh(mesh.devices.reshape(8, 2, 2, 2, mesh.shape["tp"]), (*SP, TP))
    heads = P(None, SP, "tp")
    return jax.shard_map(
        on_device,
        mesh=split,
        in_specs=(
            P(SP, None),
            heads,
            heads,
            heads,
            heads,
            heads,
            heads,
            heads,
            P(None, TP),
            P(None, TP),
            P(None, TP, None),
            P(),
            P(SP, TP),
            P(SP, TP),
            P(TP, SP),
        ),
        out_specs=P(SP, TP),
        check_vma=False,
    )
```

```python
import jax
import jax.numpy as jnp
from jax import lax
from jax.experimental import pallas as pl
from jax.experimental.pallas import tpu as pltpu
from jax.sharding import Mesh
from jax.sharding import PartitionSpec as P

PLANE, FAR, NEAR, CORE, TP = "plane", "far", "near", "core", "tp"
SP = (PLANE, FAR, NEAR, CORE)
ROW = (FAR, NEAR, CORE)
GATHER = (PLANE, NEAR, CORE)
POOL = (FAR, TP)
TOK = 128
LANES = 128
HALF = 64
SHARES = 8

norm_epsilon = 1e-06
head_epsilon = 0.00064
key_epsilon = 1e-06

f32 = jnp.float32
bf16 = jnp.bfloat16


def dot_nn(a, b):
    return lax.dot_general(a, b, (((1,), (0,)), ((), ())), preferred_element_type=f32)


def dot_nt(a, b):
    return lax.dot_general(a, b, (((1,), (1,)), ((), ())), preferred_element_type=f32)


def dot_tn(a, b):
    return lax.dot_general(a, b, (((0,), (0,)), ((), ())), preferred_element_type=f32)


def halves(a):
    high = a.astype(bf16)
    return high, (a - high.astype(f32)).astype(bf16)


def mm(a, b):
    ah, al = a
    bh, bl = b
    return dot_nn(jnp.concatenate([ah, al], 1), jnp.concatenate([bh, bh], 0)) + dot_nn(ah, bl)


def mm_nt(a, b):
    ah, al = a
    bh, bl = b
    return dot_nt(jnp.concatenate([ah, al], 1), jnp.concatenate([bh, bh], 1)) + dot_nt(ah, bl)


def mm_tn(a, b):
    ah, al = a
    bh, bl = b
    return dot_tn(jnp.concatenate([ah, al], 0), jnp.concatenate([bh, bh], 0)) + dot_tn(ah, bl)


def head_masks(group):
    lane = lax.broadcasted_iota(jnp.int32, (1, LANES), 1)
    if group == 0:
        return [(lane < HALF).astype(f32), (lane >= HALF).astype(f32)]
    return [None]


def head_sum(a, masks):
    if masks[0] is None:
        return jnp.sum(a, axis=1, keepdims=True)
    return sum(jnp.sum(a * m, axis=1, keepdims=True) * m for m in masks)


def masked(a, mask):
    return a if mask is None else a * mask


def fetch(sources, targets, sems):
    copies = [pltpu.make_async_copy(a, b, sems.at[k]) for k, (a, b) in enumerate(zip(sources, targets))]
    for copy in copies:
        copy.start()
    return copies


def local_kernel(*refs):
    inputs, outputs, scratch, results = refs[:9], refs[9:14], refs[14:23], refs[23:28]
    sems, out_sems = refs[28:]
    send_ref, out_ref, read_ref, scale_ref, extra_ref = results
    q_ref, k_ref, v_ref, f_ref, l_ref, e_ref, gate_ref, gain_ref, own_ref = scratch
    copies = fetch(inputs, scratch, sems)
    for copy in copies:
        copy.wait()
    pending = []

    def put(which, slot, count):
        part = pl.ds(slot * count, count)
        copy = pltpu.make_async_copy(
            results[which].at[part], outputs[which].at[part], out_sems.at[which, slot]
        )
        copy.start()
        pending.append(copy)

    row = lax.broadcasted_iota(jnp.int32, (TOK, TOK), 0)
    col = lax.broadcasted_iota(jnp.int32, (TOK, TOK), 1)
    strict = row > col
    inclusive = row >= col
    eye = (row == col).astype(f32)
    ones = inclusive.astype(bf16)
    slots = []
    heads = []
    for slot in range(4):
        group, cut = slot // 2, (slot % 2) * LANES
        lanes = slice(cut, cut + LANES)
        q = q_ref[group, :, lanes].astype(f32)
        k = k_ref[group, :, lanes].astype(f32)
        v = v_ref[group, :, lanes].astype(f32)
        fade = f_ref[group, :, lanes].astype(f32)
        speed = l_ref[group, :, lanes].astype(f32)
        log_decay = e_ref[group, :, lanes] - jnp.exp(-0.5) / (1.0 + jnp.exp(-fade))
        learn = 1.0 / (1.0 + jnp.exp(-speed))
        masks = head_masks(group)
        removal = k * lax.rsqrt(head_sum(k * k, masks) + key_epsilon)
        gate = gate_ref[group, :, lanes].astype(f32)
        scale_ref[slot] = gain_ref[group : group + 1, lanes] * gate
        own = head_sum(q * k * own_ref[group : group + 1, lanes], masks)
        extra_ref[slot] = own * v * gate
        put(3, slot, 1)
        put(4, slot, 1)
        d0 = log_decay.astype(bf16)
        rest = log_decay - d0.astype(f32)
        d1 = rest.astype(bf16)
        d2 = (rest - d1.astype(f32)).astype(bf16)
        cum = dot_nn(ones, d0) + dot_nn(ones, d1) + dot_nn(ones, d2)
        middle = cum[TOK // 2 : TOK // 2 + 1, :]
        forward = jnp.exp(cum - middle)
        backward = jnp.exp(middle - cum)
        undo = jnp.exp(-log_decay)
        right = learn * removal
        queries = jnp.concatenate([-removal * undo * forward, q * forward], 0)
        sources = halves(jnp.concatenate([right * backward, k * backward], 0))
        grown = jnp.exp(cum)
        final = cum[TOK - 1 : TOK, :]
        tail = jnp.exp(final - cum)
        slots.append(
            dict(
                masks=masks,
                v=halves(v),
                start=-removal * jnp.exp(cum - log_decay),
                grown=q * grown,
                right=halves(right * tail),
                keys=halves(k * tail),
                kept=jnp.exp(final),
                heads=[],
            )
        )
        for mask in masks:
            pairs = mm_nt(halves(masked(queries, mask)), sources)
            head = dict(
                slot=slot,
                mask=mask,
                n=jnp.where(strict, pairs[:TOK, :TOK], 0.0),
                rk=jnp.where(strict, pairs[:TOK, TOK:], 0.0),
                qr=jnp.where(inclusive, pairs[TOK:, :TOK], 0.0),
                qk=jnp.where(inclusive, pairs[TOK:, TOK:], 0.0),
            )
            heads.append(head)
            slots[slot]["heads"].append(head)
    same = (row // 8) == (col // 8)
    for head in heads:
        head["m"] = jnp.where(same, head["n"], 0.0)
        head["x"] = eye + head["m"]
    for _ in range(2):
        for head in heads:
            m = halves(head["m"])
            head["m"] = mm(m, m)
        for head in heads:
            head["x"] = head["x"] + mm(halves(head["x"]), halves(head["m"]))
    size = 8
    while size < TOK:
        below = (row // (2 * size) == col // (2 * size)) & (row // size != col // size)
        for head in heads:
            off = halves(jnp.where(below, head["n"], 0.0))
            head["y"] = halves(mm(off, halves(head["x"])))
        for head in heads:
            head["x"] = head["x"] + mm(halves(head["x"]), head["y"])
        size *= 2
    for slot, part in enumerate(slots):
        carried = start = local = read = None
        for head in part["heads"]:
            mask = head["mask"]
            target = jnp.concatenate([mm(halves(head["rk"]), part["v"]), part["start"]], 1)
            solved = mm(halves(head["x"]), halves(target))
            from_solved = mm(halves(head["qr"]), halves(solved))
            pieces = [
                masked(solved[:, :LANES], mask),
                masked(solved[:, LANES:], mask),
                masked(from_solved[:, :LANES] + mm(halves(head["qk"]), part["v"]), mask),
                masked(from_solved[:, LANES:], mask),
            ]
            if carried is None:
                carried, start, local, read = pieces
            else:
                carried, start, local, read = (
                    carried + pieces[0],
                    start + pieces[1],
                    local + pieces[2],
                    read + pieces[3],
                )
        transit = mm_tn(halves(start), part["right"])
        added = mm_tn(halves(carried), part["right"]) + mm_tn(part["v"], part["keys"])
        if len(part["heads"]) == 2:
            block = (row // HALF) == (col // HALF)
            transit = jnp.where(block, transit, 0.0)
            added = jnp.where(block, added, 0.0)
        transit = (transit + eye * part["kept"]).astype(bf16)
        added = added.astype(bf16)
        for half in range(2):
            send_ref[2 * slot + half, :LANES, :] = transit
            send_ref[2 * slot + half, LANES:, :] = added[half * HALF : (half + 1) * HALF, :]
        put(0, slot, 2)
        out_ref[slot] = local
        high, low = halves(part["grown"] + read)
        read_ref[slot, :, :LANES] = high
        read_ref[slot, :, LANES:] = low
        put(1, slot, 1)
        put(2, slot, 1)
    for copy in pending:
        copy.wait()


def row_kernel(got_ref, prefix_ref, total_ref):
    row = lax.broadcasted_iota(jnp.int32, (LANES + HALF, LANES), 0)
    col = lax.broadcasted_iota(jnp.int32, (LANES + HALF, LANES), 1)
    zero = jnp.zeros((LANES, LANES), f32)
    prefix_ref[0] = (row == col).astype(f32)
    run = got_ref[0].astype(f32)
    for k in range(1, SHARES):
        prefix_ref[k] = run
        got = got_ref[k]
        step = got[:LANES]
        high, low = halves(run)
        run = dot_nn(jnp.concatenate([high, low], 1), jnp.concatenate([step, step], 0))
        run = run + jnp.concatenate([zero, got[LANES:].astype(f32)], 0)
    total = run.astype(bf16)
    for k in range(total_ref.shape[0]):
        total_ref[k] = total


def state_kernel(place_ref, every_ref, prefix_ref, send_ref):
    place = place_ref[0]
    state = jnp.zeros((HALF, LANES), f32)
    for k in range(every_ref.shape[0] - 1):
        got = every_ref[k]
        step = got[:LANES]
        high, low = halves(state)
        grown = dot_nn(jnp.concatenate([high, low], 1), jnp.concatenate([step, step], 0))
        state = jnp.where(k < place, grown + got[LANES:].astype(f32), state)
    split = halves(state)
    for k in range(SHARES):
        moved = mm(split, halves(prefix_ref[k, :LANES, :]))
        send_ref[k] = (moved + prefix_ref[k, LANES:, :]).astype(bf16)


def mix_kernel(*refs):
    inputs, y_ref, scratch, sems = refs[:6], refs[6], refs[7:13], refs[13]
    out_ref, read_ref, scale_ref, extra_ref, state_ref, w_ref = scratch
    copies = fetch(inputs, scratch, sems)
    for copy in copies[:5]:
        copy.wait()
    mixed = []
    for slot in range(4):
        width = HALF if slot < 2 else LANES
        masks = head_masks(slot // 2)
        state = jnp.concatenate([state_ref[2 * slot], state_ref[2 * slot + 1]], 0)
        raw = out_ref[slot] + dot_nt(read_ref[slot], jnp.concatenate([state, state], 1))
        centered = raw - head_sum(raw, masks) * (1.0 / width)
        variance = head_sum(centered * centered, masks) * (1.0 / width)
        normed = centered * lax.rsqrt(variance + head_epsilon) * scale_ref[slot]
        mixed.append((normed + extra_ref[slot]).astype(bf16))
    mixed = jnp.concatenate(mixed, 1)
    copies[5].wait()
    tiles, _, columns = y_ref.shape
    for k in range(tiles):
        y_ref[k] = dot_nn(mixed, w_ref[:, k * columns : (k + 1) * columns]).astype(bf16)


AHEAD = 4


def feed_kernel(far_ref, x_ref, gain_ref, whole_ref, y_ref, w_ref, n_ref, acc_ref, sems):
    planes, sides, near, rows, width = w_ref.shape
    third = width // 3
    far = far_ref[0]
    copies = [
        [
            pltpu.make_async_copy(
                whole_ref.at[k, :, jnp.where(far == side, 0, 1)],
                w_ref.at[k, side],
                sems.at[k, side],
            )
            for side in range(sides)
        ]
        for k in range(planes)
    ]
    for k in range(AHEAD):
        for copy in copies[k]:
            copy.start()
    shares, tokens, columns = x_ref.shape
    tiles = shares // sides
    for side in range(sides):
        parts = [x_ref[side * tiles + k].astype(f32) for k in range(tiles)]
        total = sum(jnp.sum(a * a, axis=1, keepdims=True) for a in parts)
        scale = lax.rsqrt(total * (1.0 / (tiles * columns)) + norm_epsilon)
        for k, a in enumerate(parts):
            lanes = slice(k * columns, (k + 1) * columns)
            n_ref[side * tokens : (side + 1) * tokens, lanes] = (
                a * scale * gain_ref[:, lanes]
            ).astype(bf16)
    block = sides * near * rows
    for k in range(0, planes, 2):
        for step in (k, k + 1):
            for copy in copies[step]:
                copy.wait()
            if step + AHEAD < planes:
                for copy in copies[step + AHEAD]:
                    copy.start()
        part = dot_nn(
            n_ref[:, k * block : (k + 2) * block],
            w_ref[k : k + 2, :, :, :, : 2 * third].reshape(2 * block, 2 * third),
        )
        if k == 0:
            acc_ref[...] = part
        else:
            acc_ref[...] += part
    gate = acc_ref[:, :third]
    active = (gate / (1.0 + jnp.exp(-gate)) * acc_ref[:, third:]).astype(bf16)
    per = planes // tiles
    for k in range(tiles):
        down = w_ref[k * per : (k + 1) * per, :, :, :, 2 * third :].reshape(per * block, third)
        out = dot_nt(active, down).astype(bf16)
        for side in range(sides):
            y_ref[side * tiles + k] = out[side * tokens : (side + 1) * tokens]


def feed_forward(far, state, gain, whole):
    planes, near, sides, rows, width = whole.shape
    shares, tokens, columns = state.shape
    return pl.pallas_call(
        feed_kernel,
        out_shape=array((shares, tokens, columns), bf16),
        in_specs=[SMEM, VMEM, VMEM, HBM],
        out_specs=VMEM,
        scratch_shapes=[
            pltpu.VMEM((planes, sides, near, rows, width), bf16),
            pltpu.VMEM((sides * tokens, gain.shape[1]), bf16),
            pltpu.VMEM((sides * tokens, 2 * width // 3), f32),
            pltpu.SemaphoreType.DMA((planes, sides)),
        ],
        compiler_params=pltpu.CompilerParams(vmem_limit_bytes=60_000_000),
    )(far, state, gain, whole)


def pack_kernel(far_ref, *refs):
    inputs, (kept_ref, given_ref), scratch, sems = refs[:3], refs[3:5], refs[5:8], refs[8]
    copies = fetch(inputs, scratch, sems)
    wide = kept_ref.shape[1] // 3
    first = far_ref[0] == 0
    for k, copy in enumerate(copies):
        copy.wait()
        lanes = slice(k * wide, (k + 1) * wide)
        near = scratch[k][:, :wide]
        rest = scratch[k][:, wide:]
        blank = jnp.zeros((rest.shape[0], 2 * wide - scratch[k].shape[1]), bf16)
        far = jnp.concatenate([rest, blank], axis=1)
        kept_ref[:, lanes] = jnp.where(first, near, far)
        given_ref[:, lanes] = jnp.where(first, far, near)


def swapped(far, parts):
    rows, hidden = parts[0].shape
    wide = -(-hidden // (2 * LANES)) * LANES
    packed = array((rows, 3 * wide), bf16)
    kept, given = call(pack_kernel, (packed, packed), [SMEM] + [HBM] * 3, parts, 62_000_000)(
        far, *parts
    )
    return kept, lax.ppermute(given, FAR, [(0, 1), (1, 0)])


def gathered(kept, taken):
    both = jnp.concatenate([kept, taken], axis=0)
    whole = lax.all_gather(both, GATHER, axis=0, tiled=True)
    planes = lax.axis_size(PLANE)
    near = lax.axis_size(NEAR) * lax.axis_size(CORE)
    return whole.reshape(planes, near, 2, *kept.shape)


VMEM = pl.BlockSpec(memory_space=pltpu.VMEM)
HBM = pl.BlockSpec(memory_space=pltpu.HBM)
SMEM = pl.BlockSpec(memory_space=pltpu.SMEM)


def call(kernel, outs, specs, fetched=(), limit=24 * 1024 * 1024, written=0):
    scratch = [pltpu.VMEM(a.shape, a.dtype) for a in fetched]
    where = VMEM
    if written:
        where = HBM
        scratch += [pltpu.VMEM(a.shape, a.dtype) for a in outs]
    if fetched:
        scratch.append(pltpu.SemaphoreType.DMA((len(fetched),)))
    if written:
        scratch.append(pltpu.SemaphoreType.DMA((len(outs), written)))
    return pl.pallas_call(
        kernel,
        out_shape=outs,
        in_specs=specs,
        out_specs=jax.tree.map(lambda _: where, outs),
        scratch_shapes=scratch,
        compiler_params=pltpu.CompilerParams(vmem_limit_bytes=limit),
    )


def array(dims, kind):
    return jax.ShapeDtypeStruct(dims, kind)


def exchange(value, axis):
    return lax.all_to_all(value, axis, 0, 0, tiled=True)


def from_everyone(value, axis):
    devices = lax.psum(1, axis)
    return exchange(jnp.broadcast_to(value[None], (devices, *value.shape)), axis)


def on_device(
    stratum_source_matrix,
    acceptance_query,
    cluster_lookup_matrix,
    cluster_payload_matrix,
    fading_logit,
    adaptation_speed_logit,
    additional_fading_exponent,
    result_switch_pair,
    attender_scaling_factor,
    present_item_factor,
    final_mapping_matrix,
    perceptron_scaling_factor,
    switching_matrix,
    widening_matrix,
    shrinking_matrix,
):
    features = perceptron_scaling_factor.shape[0]
    columns = features // lax.axis_size(TP)
    far = lax.axis_index(FAR).astype(jnp.int32).reshape(1)
    kept, taken = swapped(far, [switching_matrix, widening_matrix, shrinking_matrix.T])
    blocks = array((4, TOK, LANES), f32)
    inputs = (
        acceptance_query,
        cluster_lookup_matrix,
        cluster_payload_matrix,
        fading_logit,
        adaptation_speed_logit,
        additional_fading_exponent,
        result_switch_pair,
        attender_scaling_factor,
        present_item_factor,
    )
    send, local_out, start_read, scale, extra = call(
        local_kernel,
        (
            array((SHARES, LANES + HALF, LANES), bf16),
            blocks,
            array((4, TOK, 2 * LANES), bf16),
            blocks,
            blocks,
        ),
        [HBM] * len(inputs),
        inputs,
        66_400_000,
        4,
    )(*inputs)
    send, taken = lax.optimization_barrier((send, taken))
    whole = gathered(kept, taken)
    planes = lax.axis_size(PLANE)
    prefix, total = call(
        row_kernel,
        (
            array((SHARES, LANES + HALF, LANES), f32),
            array((planes, LANES + HALF, LANES), bf16),
        ),
        [VMEM],
    )(exchange(send, ROW))
    states = call(state_kernel, array((SHARES, HALF, LANES), bf16), [SMEM, VMEM, VMEM])(
        lax.axis_index(PLANE).astype(jnp.int32).reshape(1), exchange(total, PLANE), prefix
    )
    mixing = (
        local_out,
        start_read,
        scale,
        extra,
        exchange(states, ROW),
        final_mapping_matrix.reshape(-1, features),
    )
    terms = call(
        mix_kernel,
        array((features // columns, TOK, columns), bf16),
        [HBM] * len(mixing),
        mixing,
        64_000_000,
    )(*mixing)
    residual = lax.dynamic_slice_in_dim(
        stratum_source_matrix, lax.axis_index(TP) * columns, columns, 1
    )
    attention = jnp.sum(exchange(terms, TP).astype(f32), axis=0)
    own_state = (residual.astype(f32) + attention).astype(bf16)
    tiles = feed_forward(
        far,
        from_everyone(own_state, POOL),
        perceptron_scaling_factor.reshape(1, features),
        whole,
    )
    mixer = jnp.sum(exchange(tiles, POOL).astype(f32), axis=0)
    return (own_state.astype(f32) + mixer).astype(bf16)


def solution(mesh):
    split = Mesh(mesh.devices.reshape(8, 2, 2, 2, mesh.shape["tp"]), (*SP, TP))
    heads = P(None, SP, "tp")
    return jax.shard_map(
        on_device,
        mesh=split,
        in_specs=(
            P(SP, None),
            heads,
            heads,
            heads,
            heads,
            heads,
            heads,
            heads,
            P(None, TP),
            P(None, TP),
            P(None, TP, None),
            P(),
            P(SP, TP),
            P(SP, TP),
            P(TP, SP),
        ),
        out_specs=P(SP, TP),
        check_vma=False,
    )
```

```python
import jax
import jax.numpy as jnp
from jax import lax
from jax.experimental import pallas as pl
from jax.experimental.pallas import tpu as pltpu
from jax.sharding import Mesh
from jax.sharding import PartitionSpec as P

PLANE, FAR, NEAR, CORE, TP = "plane", "far", "near", "core", "tp"
SP = (PLANE, FAR, NEAR, CORE)
ROW = (FAR, NEAR, CORE)
GATHER = (PLANE, NEAR, CORE)
POOL = (FAR, TP)
TOK = 128
LANES = 128
HALF = 64
SHARES = 8

norm_epsilon = 1e-06
head_epsilon = 0.00064
key_epsilon = 1e-06

f32 = jnp.float32
bf16 = jnp.bfloat16


def dot_nn(a, b):
    return lax.dot_general(a, b, (((1,), (0,)), ((), ())), preferred_element_type=f32)


def dot_nt(a, b):
    return lax.dot_general(a, b, (((1,), (1,)), ((), ())), preferred_element_type=f32)


def dot_tn(a, b):
    return lax.dot_general(a, b, (((0,), (0,)), ((), ())), preferred_element_type=f32)


def halves(a):
    high = a.astype(bf16)
    return high, (a - high.astype(f32)).astype(bf16)


def mm(a, b):
    ah, al = a
    bh, bl = b
    return dot_nn(jnp.concatenate([ah, al], 1), jnp.concatenate([bh, bh], 0)) + dot_nn(ah, bl)


def mm_nt(a, b):
    ah, al = a
    bh, bl = b
    return dot_nt(jnp.concatenate([ah, al], 1), jnp.concatenate([bh, bh], 1)) + dot_nt(ah, bl)


def mm_tn(a, b):
    ah, al = a
    bh, bl = b
    return dot_tn(jnp.concatenate([ah, al], 0), jnp.concatenate([bh, bh], 0)) + dot_tn(ah, bl)


def head_masks(group):
    lane = lax.broadcasted_iota(jnp.int32, (1, LANES), 1)
    if group == 0:
        return [(lane < HALF).astype(f32), (lane >= HALF).astype(f32)]
    return [None]


def head_sum(a, masks):
    if masks[0] is None:
        return jnp.sum(a, axis=1, keepdims=True)
    return sum(jnp.sum(a * m, axis=1, keepdims=True) * m for m in masks)


def masked(a, mask):
    return a if mask is None else a * mask


def fetch(sources, targets, sems):
    copies = [pltpu.make_async_copy(a, b, sems.at[k]) for k, (a, b) in enumerate(zip(sources, targets))]
    for copy in copies:
        copy.start()
    return copies


def local_kernel(*refs):
    inputs, outputs, scratch, results = refs[:9], refs[9:14], refs[14:23], refs[23:28]
    sems, small_sems, out_sems = refs[28:]
    send_ref, out_ref, read_ref, scale_ref, extra_ref = results
    q_ref, k_ref, v_ref, f_ref, l_ref, e_ref, gate_ref, gain_ref, own_ref = scratch
    copies = [
        pltpu.make_async_copy(a.at[group], b.at[group], sems.at[k, group])
        for group in range(2)
        for k, (a, b) in enumerate(zip(inputs[:7], scratch[:7]))
    ]
    small = fetch(inputs[7:], scratch[7:], small_sems)
    for copy in copies:
        copy.start()
    pending = []

    def put(which, slot, count):
        part = pl.ds(slot * count, count)
        copy = pltpu.make_async_copy(
            results[which].at[part], outputs[which].at[part], out_sems.at[which, slot]
        )
        copy.start()
        pending.append(copy)

    row = lax.broadcasted_iota(jnp.int32, (TOK, TOK), 0)
    col = lax.broadcasted_iota(jnp.int32, (TOK, TOK), 1)
    strict = row > col
    inclusive = row >= col
    eye = (row == col).astype(f32)
    ones = inclusive.astype(bf16)
    slots = []
    heads = []
    for slot in range(4):
        group, cut = slot // 2, (slot % 2) * LANES
        if cut == 0:
            for copy in copies[group * 7 : group * 7 + 7] + small:
                copy.wait()
            small = []
        lanes = slice(cut, cut + LANES)
        q = q_ref[group, :, lanes].astype(f32)
        k = k_ref[group, :, lanes].astype(f32)
        v = v_ref[group, :, lanes].astype(f32)
        fade = f_ref[group, :, lanes].astype(f32)
        speed = l_ref[group, :, lanes].astype(f32)
        log_decay = e_ref[group, :, lanes] - jnp.exp(-0.5) / (1.0 + jnp.exp(-fade))
        learn = 1.0 / (1.0 + jnp.exp(-speed))
        masks = head_masks(group)
        removal = k * lax.rsqrt(head_sum(k * k, masks) + key_epsilon)
        gate = gate_ref[group, :, lanes].astype(f32)
        scale_ref[slot] = gain_ref[group : group + 1, lanes] * gate
        own = head_sum(q * k * own_ref[group : group + 1, lanes], masks)
        extra_ref[slot] = own * v * gate
        put(3, slot, 1)
        put(4, slot, 1)
        d0 = log_decay.astype(bf16)
        rest = log_decay - d0.astype(f32)
        d1 = rest.astype(bf16)
        d2 = (rest - d1.astype(f32)).astype(bf16)
        cum = dot_nn(ones, d0) + dot_nn(ones, d1) + dot_nn(ones, d2)
        middle = cum[TOK // 2 : TOK // 2 + 1, :]
        forward = jnp.exp(cum - middle)
        backward = jnp.exp(middle - cum)
        undo = jnp.exp(-log_decay)
        right = learn * removal
        queries = jnp.concatenate([-removal * undo * forward, q * forward], 0)
        sources = halves(jnp.concatenate([right * backward, k * backward], 0))
        grown = jnp.exp(cum)
        final = cum[TOK - 1 : TOK, :]
        tail = jnp.exp(final - cum)
        slots.append(
            dict(
                masks=masks,
                v=halves(v),
                start=-removal * jnp.exp(cum - log_decay),
                grown=q * grown,
                right=halves(right * tail),
                keys=halves(k * tail),
                kept=jnp.exp(final),
                heads=[],
            )
        )
        for mask in masks:
            pairs = mm_nt(halves(masked(queries, mask)), sources)
            head = dict(
                slot=slot,
                mask=mask,
                n=jnp.where(strict, pairs[:TOK, :TOK], 0.0),
                rk=jnp.where(strict, pairs[:TOK, TOK:], 0.0),
                qr=jnp.where(inclusive, pairs[TOK:, :TOK], 0.0),
                qk=jnp.where(inclusive, pairs[TOK:, TOK:], 0.0),
            )
            heads.append(head)
            slots[slot]["heads"].append(head)
    same = (row // 8) == (col // 8)
    for head in heads:
        head["m"] = jnp.where(same, head["n"], 0.0)
        head["x"] = eye + head["m"]
    for _ in range(2):
        for head in heads:
            m = halves(head["m"])
            head["m"] = mm(m, m)
        for head in heads:
            head["x"] = head["x"] + mm(halves(head["x"]), halves(head["m"]))
    size = 8
    while size < TOK:
        below = (row // (2 * size) == col // (2 * size)) & (row // size != col // size)
        for head in heads:
            off = halves(jnp.where(below, head["n"], 0.0))
            head["y"] = halves(mm(off, halves(head["x"])))
        for head in heads:
            head["x"] = head["x"] + mm(halves(head["x"]), head["y"])
        size *= 2
    for slot, part in enumerate(slots):
        carried = start = local = read = None
        for head in part["heads"]:
            mask = head["mask"]
            target = jnp.concatenate([mm(halves(head["rk"]), part["v"]), part["start"]], 1)
            solved = mm(halves(head["x"]), halves(target))
            from_solved = mm(halves(head["qr"]), halves(solved))
            pieces = [
                masked(solved[:, :LANES], mask),
                masked(solved[:, LANES:], mask),
                masked(from_solved[:, :LANES] + mm(halves(head["qk"]), part["v"]), mask),
                masked(from_solved[:, LANES:], mask),
            ]
            if carried is None:
                carried, start, local, read = pieces
            else:
                carried, start, local, read = (
                    carried + pieces[0],
                    start + pieces[1],
                    local + pieces[2],
                    read + pieces[3],
                )
        transit = mm_tn(halves(start), part["right"])
        added = mm_tn(halves(carried), part["right"]) + mm_tn(part["v"], part["keys"])
        if len(part["heads"]) == 2:
            block = (row // HALF) == (col // HALF)
            transit = jnp.where(block, transit, 0.0)
            added = jnp.where(block, added, 0.0)
        transit = (transit + eye * part["kept"]).astype(bf16)
        added = added.astype(bf16)
        for half in range(2):
            send_ref[2 * slot + half, :LANES, :] = transit
            send_ref[2 * slot + half, LANES:, :] = added[half * HALF : (half + 1) * HALF, :]
        put(0, slot, 2)
        out_ref[slot] = local
        high, low = halves(part["grown"] + read)
        read_ref[slot, :, :LANES] = high
        read_ref[slot, :, LANES:] = low
        put(1, slot, 1)
        put(2, slot, 1)
    for copy in pending:
        copy.wait()


def row_kernel(got_ref, prefix_ref, total_ref):
    row = lax.broadcasted_iota(jnp.int32, (LANES + HALF, LANES), 0)
    col = lax.broadcasted_iota(jnp.int32, (LANES + HALF, LANES), 1)
    zero = jnp.zeros((LANES, LANES), f32)
    prefix_ref[0] = (row == col).astype(f32)
    run = got_ref[0].astype(f32)
    for k in range(1, SHARES):
        prefix_ref[k] = run
        got = got_ref[k]
        step = got[:LANES]
        high, low = halves(run)
        run = dot_nn(jnp.concatenate([high, low], 1), jnp.concatenate([step, step], 0))
        run = run + jnp.concatenate([zero, got[LANES:].astype(f32)], 0)
    total = run.astype(bf16)
    for k in range(total_ref.shape[0]):
        total_ref[k] = total


def state_kernel(place_ref, every_ref, prefix_ref, send_ref):
    place = place_ref[0]
    state = jnp.zeros((HALF, LANES), f32)
    for k in range(every_ref.shape[0] - 1):
        got = every_ref[k]
        step = got[:LANES]
        high, low = halves(state)
        grown = dot_nn(jnp.concatenate([high, low], 1), jnp.concatenate([step, step], 0))
        state = jnp.where(k < place, grown + got[LANES:].astype(f32), state)
    split = halves(state)
    for k in range(SHARES):
        moved = mm(split, halves(prefix_ref[k, :LANES, :]))
        send_ref[k] = (moved + prefix_ref[k, LANES:, :]).astype(bf16)


def mix_kernel(*refs):
    inputs, y_ref, scratch, sems = refs[:6], refs[6], refs[7:13], refs[13]
    out_ref, read_ref, scale_ref, extra_ref, state_ref, w_ref = scratch
    copies = fetch(inputs, scratch, sems)
    for copy in copies[:5]:
        copy.wait()
    mixed = []
    for slot in range(4):
        width = HALF if slot < 2 else LANES
        masks = head_masks(slot // 2)
        state = jnp.concatenate([state_ref[2 * slot], state_ref[2 * slot + 1]], 0)
        raw = out_ref[slot] + dot_nt(read_ref[slot], jnp.concatenate([state, state], 1))
        centered = raw - head_sum(raw, masks) * (1.0 / width)
        variance = head_sum(centered * centered, masks) * (1.0 / width)
        normed = centered * lax.rsqrt(variance + head_epsilon) * scale_ref[slot]
        mixed.append((normed + extra_ref[slot]).astype(bf16))
    mixed = jnp.concatenate(mixed, 1)
    copies[5].wait()
    tiles, _, columns = y_ref.shape
    for k in range(tiles):
        y_ref[k] = dot_nn(mixed, w_ref[:, k * columns : (k + 1) * columns]).astype(bf16)


AHEAD = 4


def feed_kernel(far_ref, x_ref, gain_ref, whole_ref, y_ref, w_ref, n_ref, acc_ref, sems):
    planes, sides, near, rows, width = w_ref.shape
    third = width // 3
    far = far_ref[0]
    copies = [
        [
            pltpu.make_async_copy(
                whole_ref.at[k, :, jnp.where(far == side, 0, 1)],
                w_ref.at[k, side],
                sems.at[k, side],
            )
            for side in range(sides)
        ]
        for k in range(planes)
    ]
    for k in range(AHEAD):
        for copy in copies[k]:
            copy.start()
    shares, tokens, columns = x_ref.shape
    tiles = shares // sides
    for side in range(sides):
        parts = [x_ref[side * tiles + k].astype(f32) for k in range(tiles)]
        total = sum(jnp.sum(a * a, axis=1, keepdims=True) for a in parts)
        scale = lax.rsqrt(total * (1.0 / (tiles * columns)) + norm_epsilon)
        for k, a in enumerate(parts):
            lanes = slice(k * columns, (k + 1) * columns)
            n_ref[side * tokens : (side + 1) * tokens, lanes] = (
                a * scale * gain_ref[:, lanes]
            ).astype(bf16)
    block = sides * near * rows
    for k in range(0, planes, 2):
        for step in (k, k + 1):
            for copy in copies[step]:
                copy.wait()
            if step + AHEAD < planes:
                for copy in copies[step + AHEAD]:
                    copy.start()
        part = dot_nn(
            n_ref[:, k * block : (k + 2) * block],
            w_ref[k : k + 2, :, :, :, : 2 * third].reshape(2 * block, 2 * third),
        )
        if k == 0:
            acc_ref[...] = part
        else:
            acc_ref[...] += part
    gate = acc_ref[:, :third]
    active = (gate / (1.0 + jnp.exp(-gate)) * acc_ref[:, third:]).astype(bf16)
    per = planes // tiles
    for k in range(tiles):
        down = w_ref[k * per : (k + 1) * per, :, :, :, 2 * third :].reshape(per * block, third)
        out = dot_nt(active, down).astype(bf16)
        for side in range(sides):
            y_ref[side * tiles + k] = out[side * tokens : (side + 1) * tokens]


def feed_forward(far, state, gain, whole):
    planes, near, sides, rows, width = whole.shape
    shares, tokens, columns = state.shape
    return pl.pallas_call(
        feed_kernel,
        out_shape=array((shares, tokens, columns), bf16),
        in_specs=[SMEM, VMEM, VMEM, HBM],
        out_specs=VMEM,
        scratch_shapes=[
            pltpu.VMEM((planes, sides, near, rows, width), bf16),
            pltpu.VMEM((sides * tokens, gain.shape[1]), bf16),
            pltpu.VMEM((sides * tokens, 2 * width // 3), f32),
            pltpu.SemaphoreType.DMA((planes, sides)),
        ],
        compiler_params=pltpu.CompilerParams(vmem_limit_bytes=60_000_000),
    )(far, state, gain, whole)


def pack_kernel(far_ref, *refs):
    inputs, (kept_ref, given_ref), scratch, sems = refs[:3], refs[3:5], refs[5:8], refs[8]
    copies = fetch(inputs, scratch, sems)
    wide = kept_ref.shape[1] // 3
    first = far_ref[0] == 0
    for k, copy in enumerate(copies):
        copy.wait()
        lanes = slice(k * wide, (k + 1) * wide)
        near = scratch[k][:, :wide]
        rest = scratch[k][:, wide:]
        blank = jnp.zeros((rest.shape[0], 2 * wide - scratch[k].shape[1]), bf16)
        far = jnp.concatenate([rest, blank], axis=1)
        kept_ref[:, lanes] = jnp.where(first, near, far)
        given_ref[:, lanes] = jnp.where(first, far, near)


def swapped(far, parts):
    rows, hidden = parts[0].shape
    wide = -(-hidden // (2 * LANES)) * LANES
    packed = array((rows, 3 * wide), bf16)
    kept, given = call(pack_kernel, (packed, packed), [SMEM] + [HBM] * 3, parts, 62_000_000)(
        far, *parts
    )
    return kept, lax.ppermute(given, FAR, [(0, 1), (1, 0)])


def gathered(kept, taken):
    both = jnp.concatenate([kept, taken], axis=0)
    whole = lax.all_gather(both, GATHER, axis=0, tiled=True)
    planes = lax.axis_size(PLANE)
    near = lax.axis_size(NEAR) * lax.axis_size(CORE)
    return whole.reshape(planes, near, 2, *kept.shape)


VMEM = pl.BlockSpec(memory_space=pltpu.VMEM)
HBM = pl.BlockSpec(memory_space=pltpu.HBM)
SMEM = pl.BlockSpec(memory_space=pltpu.SMEM)


def call(kernel, outs, specs, fetched=(), limit=24 * 1024 * 1024, written=0, sems=()):
    scratch = [pltpu.VMEM(a.shape, a.dtype) for a in fetched]
    where = VMEM
    if written:
        where = HBM
        scratch += [pltpu.VMEM(a.shape, a.dtype) for a in outs]
    scratch += [pltpu.SemaphoreType.DMA(a) for a in sems or [(len(fetched),)] if fetched]
    if written:
        scratch.append(pltpu.SemaphoreType.DMA((len(outs), written)))
    return pl.pallas_call(
        kernel,
        out_shape=outs,
        in_specs=specs,
        out_specs=jax.tree.map(lambda _: where, outs),
        scratch_shapes=scratch,
        compiler_params=pltpu.CompilerParams(vmem_limit_bytes=limit),
    )


def array(dims, kind):
    return jax.ShapeDtypeStruct(dims, kind)


def exchange(value, axis):
    return lax.all_to_all(value, axis, 0, 0, tiled=True)


def from_everyone(value, axis):
    devices = lax.psum(1, axis)
    return exchange(jnp.broadcast_to(value[None], (devices, *value.shape)), axis)


def on_device(
    stratum_source_matrix,
    acceptance_query,
    cluster_lookup_matrix,
    cluster_payload_matrix,
    fading_logit,
    adaptation_speed_logit,
    additional_fading_exponent,
    result_switch_pair,
    attender_scaling_factor,
    present_item_factor,
    final_mapping_matrix,
    perceptron_scaling_factor,
    switching_matrix,
    widening_matrix,
    shrinking_matrix,
):
    features = perceptron_scaling_factor.shape[0]
    columns = features // lax.axis_size(TP)
    far = lax.axis_index(FAR).astype(jnp.int32).reshape(1)
    kept, taken = swapped(far, [switching_matrix, widening_matrix, shrinking_matrix.T])
    blocks = array((4, TOK, LANES), f32)
    inputs = (
        acceptance_query,
        cluster_lookup_matrix,
        cluster_payload_matrix,
        fading_logit,
        adaptation_speed_logit,
        additional_fading_exponent,
        result_switch_pair,
        attender_scaling_factor,
        present_item_factor,
    )
    send, local_out, start_read, scale, extra = call(
        local_kernel,
        (
            array((SHARES, LANES + HALF, LANES), bf16),
            blocks,
            array((4, TOK, 2 * LANES), bf16),
            blocks,
            blocks,
        ),
        [HBM] * len(inputs),
        inputs,
        66_400_000,
        4,
        [(7, 2), (2,)],
    )(*inputs)
    place = lax.axis_index(PLANE).astype(jnp.int32).reshape(1)
    first_column = (lax.axis_index(TP) * columns).astype(jnp.uint32)
    send, taken, place, first_column = lax.optimization_barrier((send, taken, place, first_column))
    whole = gathered(kept, taken)
    planes = lax.axis_size(PLANE)
    prefix, total = call(
        row_kernel,
        (
            array((SHARES, LANES + HALF, LANES), f32),
            array((planes, LANES + HALF, LANES), bf16),
        ),
        [VMEM],
    )(exchange(send, ROW))
    states = call(state_kernel, array((SHARES, HALF, LANES), bf16), [SMEM, VMEM, VMEM])(
        place, exchange(total, PLANE), prefix
    )
    mixing = (
        local_out,
        start_read,
        scale,
        extra,
        exchange(states, ROW),
        final_mapping_matrix.reshape(-1, features),
    )
    terms = call(
        mix_kernel,
        array((features // columns, TOK, columns), bf16),
        [HBM] * len(mixing),
        mixing,
        64_000_000,
    )(*mixing)
    residual = lax.dynamic_slice(
        stratum_source_matrix, (jnp.uint32(0), first_column), (TOK, columns)
    )
    attention = jnp.sum(exchange(terms, TP).astype(f32), axis=0)
    own_state = (residual.astype(f32) + attention).astype(bf16)
    tiles = feed_forward(
        far,
        from_everyone(own_state, POOL),
        perceptron_scaling_factor.reshape(1, features),
        whole,
    )
    mixer = jnp.sum(exchange(tiles, POOL).astype(f32), axis=0)
    return (own_state.astype(f32) + mixer).astype(bf16)


def solution(mesh):
    split = Mesh(mesh.devices.reshape(8, 2, 2, 2, mesh.shape["tp"]), (*SP, TP))
    heads = P(None, SP, "tp")
    return jax.shard_map(
        on_device,
        mesh=split,
        in_specs=(
            P(SP, None),
            heads,
            heads,
            heads,
            heads,
            heads,
            heads,
            heads,
            P(None, TP),
            P(None, TP),
            P(None, TP, None),
            P(),
            P(SP, TP),
            P(SP, TP),
            P(TP, SP),
        ),
        out_specs=P(SP, TP),
        check_vma=False,
    )
```

```python
import jax
import jax.numpy as jnp
from jax import lax
from jax.experimental import pallas as pl
from jax.experimental.pallas import tpu as pltpu
from jax.sharding import Mesh
from jax.sharding import PartitionSpec as P

PLANE, FAR, NEAR, CORE, TP = "plane", "far", "near", "core", "tp"
SP = (PLANE, FAR, NEAR, CORE)
ROW = (FAR, NEAR, CORE)
TOK = 128
LANES = 128
HALF = 64
SHARES = 8

norm_epsilon = 1e-06
head_epsilon = 0.00064
key_epsilon = 1e-06

f32 = jnp.float32
bf16 = jnp.bfloat16


def dot_nn(a, b):
    return lax.dot_general(a, b, (((1,), (0,)), ((), ())), preferred_element_type=f32)


def dot_nt(a, b):
    return lax.dot_general(a, b, (((1,), (1,)), ((), ())), preferred_element_type=f32)


def dot_tn(a, b):
    return lax.dot_general(a, b, (((0,), (0,)), ((), ())), preferred_element_type=f32)


def halves(a):
    high = a.astype(bf16)
    return high, (a - high.astype(f32)).astype(bf16)


def mm(a, b):
    ah, al = a
    bh, bl = b
    return dot_nn(jnp.concatenate([ah, al], 1), jnp.concatenate([bh, bh], 0)) + dot_nn(ah, bl)


def mm_nt(a, b):
    ah, al = a
    bh, bl = b
    return dot_nt(jnp.concatenate([ah, al], 1), jnp.concatenate([bh, bh], 1)) + dot_nt(ah, bl)


def mm_tn(a, b):
    ah, al = a
    bh, bl = b
    return dot_tn(jnp.concatenate([ah, al], 0), jnp.concatenate([bh, bh], 0)) + dot_tn(ah, bl)


def head_masks(group):
    lane = lax.broadcasted_iota(jnp.int32, (1, LANES), 1)
    if group == 0:
        return [(lane < HALF).astype(f32), (lane >= HALF).astype(f32)]
    return [None]


def head_sum(a, masks):
    if masks[0] is None:
        return jnp.sum(a, axis=1, keepdims=True)
    return sum(jnp.sum(a * m, axis=1, keepdims=True) * m for m in masks)


def masked(a, mask):
    return a if mask is None else a * mask


def fetch(sources, targets, sems):
    copies = [pltpu.make_async_copy(a, b, sems.at[k]) for k, (a, b) in enumerate(zip(sources, targets))]
    for copy in copies:
        copy.start()
    return copies


def local_kernel(*refs):
    inputs, outputs, scratch, results = refs[:9], refs[9:14], refs[14:23], refs[23:28]
    sems, small_sems, out_sems = refs[28:]
    send_ref, out_ref, read_ref, scale_ref, extra_ref = results
    q_ref, k_ref, v_ref, f_ref, l_ref, e_ref, gate_ref, gain_ref, own_ref = scratch
    copies = [
        pltpu.make_async_copy(a.at[group], b.at[group], sems.at[k, group])
        for group in range(2)
        for k, (a, b) in enumerate(zip(inputs[:7], scratch[:7]))
    ]
    small = fetch(inputs[7:], scratch[7:], small_sems)
    for copy in copies:
        copy.start()
    pending = []

    def put(which, slot, count):
        part = pl.ds(slot * count, count)
        copy = pltpu.make_async_copy(
            results[which].at[part], outputs[which].at[part], out_sems.at[which, slot]
        )
        copy.start()
        pending.append(copy)

    row = lax.broadcasted_iota(jnp.int32, (TOK, TOK), 0)
    col = lax.broadcasted_iota(jnp.int32, (TOK, TOK), 1)
    strict = row > col
    inclusive = row >= col
    eye = (row == col).astype(f32)
    ones = inclusive.astype(bf16)
    slots = []
    heads = []
    for slot in range(4):
        group, cut = slot // 2, (slot % 2) * LANES
        if cut == 0:
            for copy in copies[group * 7 : group * 7 + 7] + small:
                copy.wait()
            small = []
        lanes = slice(cut, cut + LANES)
        q = q_ref[group, :, lanes].astype(f32)
        k = k_ref[group, :, lanes].astype(f32)
        v = v_ref[group, :, lanes].astype(f32)
        fade = f_ref[group, :, lanes].astype(f32)
        speed = l_ref[group, :, lanes].astype(f32)
        log_decay = e_ref[group, :, lanes] - jnp.exp(-0.5) / (1.0 + jnp.exp(-fade))
        learn = 1.0 / (1.0 + jnp.exp(-speed))
        masks = head_masks(group)
        removal = k * lax.rsqrt(head_sum(k * k, masks) + key_epsilon)
        gate = gate_ref[group, :, lanes].astype(f32)
        scale_ref[slot] = gain_ref[group : group + 1, lanes] * gate
        own = head_sum(q * k * own_ref[group : group + 1, lanes], masks)
        extra_ref[slot] = own * v * gate
        put(3, slot, 1)
        put(4, slot, 1)
        d0 = log_decay.astype(bf16)
        rest = log_decay - d0.astype(f32)
        d1 = rest.astype(bf16)
        d2 = (rest - d1.astype(f32)).astype(bf16)
        cum = dot_nn(ones, d0) + dot_nn(ones, d1) + dot_nn(ones, d2)
        middle = cum[TOK // 2 : TOK // 2 + 1, :]
        forward = jnp.exp(cum - middle)
        backward = jnp.exp(middle - cum)
        undo = jnp.exp(-log_decay)
        right = learn * removal
        queries = jnp.concatenate([-removal * undo * forward, q * forward], 0)
        sources = halves(jnp.concatenate([right * backward, k * backward], 0))
        grown = jnp.exp(cum)
        final = cum[TOK - 1 : TOK, :]
        tail = jnp.exp(final - cum)
        slots.append(
            dict(
                masks=masks,
                v=halves(v),
                start=-removal * jnp.exp(cum - log_decay),
                grown=q * grown,
                right=halves(right * tail),
                keys=halves(k * tail),
                kept=jnp.exp(final),
                heads=[],
            )
        )
        for mask in masks:
            pairs = mm_nt(halves(masked(queries, mask)), sources)
            head = dict(
                slot=slot,
                mask=mask,
                n=jnp.where(strict, pairs[:TOK, :TOK], 0.0),
                rk=jnp.where(strict, pairs[:TOK, TOK:], 0.0),
                qr=jnp.where(inclusive, pairs[TOK:, :TOK], 0.0),
                qk=jnp.where(inclusive, pairs[TOK:, TOK:], 0.0),
            )
            heads.append(head)
            slots[slot]["heads"].append(head)
    same = (row // 8) == (col // 8)
    for head in heads:
        head["m"] = jnp.where(same, head["n"], 0.0)
        head["x"] = eye + head["m"]
    for _ in range(2):
        for head in heads:
            m = halves(head["m"])
            head["m"] = mm(m, m)
        for head in heads:
            head["x"] = head["x"] + mm(halves(head["x"]), halves(head["m"]))
    size = 8
    while size < TOK:
        below = (row // (2 * size) == col // (2 * size)) & (row // size != col // size)
        for head in heads:
            off = halves(jnp.where(below, head["n"], 0.0))
            head["y"] = halves(mm(off, halves(head["x"])))
        for head in heads:
            head["x"] = head["x"] + mm(halves(head["x"]), head["y"])
        size *= 2
    for slot, part in enumerate(slots):
        carried = start = local = read = None
        for head in part["heads"]:
            mask = head["mask"]
            target = jnp.concatenate([mm(halves(head["rk"]), part["v"]), part["start"]], 1)
            solved = mm(halves(head["x"]), halves(target))
            from_solved = mm(halves(head["qr"]), halves(solved))
            pieces = [
                masked(solved[:, :LANES], mask),
                masked(solved[:, LANES:], mask),
                masked(from_solved[:, :LANES] + mm(halves(head["qk"]), part["v"]), mask),
                masked(from_solved[:, LANES:], mask),
            ]
            if carried is None:
                carried, start, local, read = pieces
            else:
                carried, start, local, read = (
                    carried + pieces[0],
                    start + pieces[1],
                    local + pieces[2],
                    read + pieces[3],
                )
        transit = mm_tn(halves(start), part["right"])
        added = mm_tn(halves(carried), part["right"]) + mm_tn(part["v"], part["keys"])
        if len(part["heads"]) == 2:
            block = (row // HALF) == (col // HALF)
            transit = jnp.where(block, transit, 0.0)
            added = jnp.where(block, added, 0.0)
        transit = (transit + eye * part["kept"]).astype(bf16)
        added = added.astype(bf16)
        for half in range(2):
            send_ref[2 * slot + half, :LANES, :] = transit
            send_ref[2 * slot + half, LANES:, :] = added[half * HALF : (half + 1) * HALF, :]
        put(0, slot, 2)
        out_ref[slot] = local
        high, low = halves(part["grown"] + read)
        read_ref[slot, :, :LANES] = high
        read_ref[slot, :, LANES:] = low
        put(1, slot, 1)
        put(2, slot, 1)
    for copy in pending:
        copy.wait()


def row_kernel(got_ref, prefix_ref, total_ref):
    row = lax.broadcasted_iota(jnp.int32, (LANES + HALF, LANES), 0)
    col = lax.broadcasted_iota(jnp.int32, (LANES + HALF, LANES), 1)
    zero = jnp.zeros((LANES, LANES), f32)
    prefix_ref[0] = (row == col).astype(f32)
    run = got_ref[0].astype(f32)
    for k in range(1, SHARES):
        prefix_ref[k] = run
        got = got_ref[k]
        step = got[:LANES]
        high, low = halves(run)
        run = dot_nn(jnp.concatenate([high, low], 1), jnp.concatenate([step, step], 0))
        run = run + jnp.concatenate([zero, got[LANES:].astype(f32)], 0)
    total = run.astype(bf16)
    for k in range(total_ref.shape[0]):
        total_ref[k] = total


def state_kernel(place_ref, every_ref, prefix_ref, send_ref):
    place = place_ref[0]
    state = jnp.zeros((HALF, LANES), f32)
    for k in range(every_ref.shape[0] - 1):
        got = every_ref[k]
        step = got[:LANES]
        high, low = halves(state)
        grown = dot_nn(jnp.concatenate([high, low], 1), jnp.concatenate([step, step], 0))
        state = jnp.where(k < place, grown + got[LANES:].astype(f32), state)
    split = halves(state)
    for k in range(SHARES):
        moved = mm(split, halves(prefix_ref[k, :LANES, :]))
        send_ref[k] = (moved + prefix_ref[k, LANES:, :]).astype(bf16)


def mix_kernel(*refs):
    inputs, y_ref, scratch, sems = refs[:6], refs[6], refs[7:13], refs[13]
    out_ref, read_ref, scale_ref, extra_ref, state_ref, w_ref = scratch
    copies = fetch(inputs, scratch, sems)
    for copy in copies[:5]:
        copy.wait()
    mixed = []
    for slot in range(4):
        width = HALF if slot < 2 else LANES
        masks = head_masks(slot // 2)
        state = jnp.concatenate([state_ref[2 * slot], state_ref[2 * slot + 1]], 0)
        raw = out_ref[slot] + dot_nt(read_ref[slot], jnp.concatenate([state, state], 1))
        centered = raw - head_sum(raw, masks) * (1.0 / width)
        variance = head_sum(centered * centered, masks) * (1.0 / width)
        normed = centered * lax.rsqrt(variance + head_epsilon) * scale_ref[slot]
        mixed.append((normed + extra_ref[slot]).astype(bf16))
    mixed = jnp.concatenate(mixed, 1)
    copies[5].wait()
    tiles, _, columns = y_ref.shape
    for k in range(tiles):
        y_ref[k] = dot_nn(mixed, w_ref[:, k * columns : (k + 1) * columns]).astype(bf16)


AHEAD = 4


def feed_kernel(x_ref, gain_ref, whole_ref, y_ref, w_ref, n_ref, acc_ref, sems):
    blocks, rows, width = w_ref.shape
    third = width // 3
    parts = [pl.ds(0, 2 * third), pl.ds(2 * third, third)]
    waves = [(k, part) for part in range(2) for k in range(blocks)]
    copies = [
        pltpu.make_async_copy(
            whole_ref.at[k, :, parts[part]], w_ref.at[k, :, parts[part]], sems.at[part, k]
        )
        for k, part in waves
    ]
    for copy in copies[:AHEAD]:
        copy.start()
    tiles, tokens, columns = x_ref.shape
    states = [x_ref[k].astype(f32) for k in range(tiles)]
    total = sum(jnp.sum(a * a, axis=1, keepdims=True) for a in states)
    scale = lax.rsqrt(total * (1.0 / (tiles * columns)) + norm_epsilon)
    for k, a in enumerate(states):
        lanes = slice(k * columns, (k + 1) * columns)
        n_ref[:, lanes] = (a * scale * gain_ref[:, lanes]).astype(bf16)

    def arrive(k):
        copies[k].wait()
        if k + AHEAD < len(copies):
            copies[k + AHEAD].start()

    for k in range(0, blocks, 2):
        arrive(k)
        arrive(k + 1)
        part = dot_nn(
            n_ref[:, k * rows : (k + 2) * rows],
            w_ref[k : k + 2, :, : 2 * third].reshape(2 * rows, 2 * third),
        )
        if k == 0:
            acc_ref[...] = part
        else:
            acc_ref[...] += part
    gate = acc_ref[:, :third]
    active = (gate / (1.0 + jnp.exp(-gate)) * acc_ref[:, third:]).astype(bf16)
    per = blocks // tiles
    for k in range(tiles):
        for step in range(k * per, (k + 1) * per):
            arrive(blocks + step)
        down = w_ref[k * per : (k + 1) * per, :, 2 * third :].reshape(per * rows, third)
        y_ref[k] = dot_nt(active, down).astype(bf16)


def feed_forward(state, gain, whole):
    tiles, tokens, columns = state.shape
    blocks, rows, width = whole.shape
    return pl.pallas_call(
        feed_kernel,
        out_shape=array((tiles, tokens, columns), bf16),
        in_specs=[VMEM, VMEM, HBM],
        out_specs=VMEM,
        scratch_shapes=[
            pltpu.VMEM((blocks, rows, width), bf16),
            pltpu.VMEM((tokens, gain.shape[1]), bf16),
            pltpu.VMEM((tokens, 2 * width // 3), f32),
            pltpu.SemaphoreType.DMA((2, blocks)),
        ],
        compiler_params=pltpu.CompilerParams(vmem_limit_bytes=60_000_000),
    )(state, gain, whole)


VMEM = pl.BlockSpec(memory_space=pltpu.VMEM)
HBM = pl.BlockSpec(memory_space=pltpu.HBM)
SMEM = pl.BlockSpec(memory_space=pltpu.SMEM)


def call(kernel, outs, specs, fetched=(), limit=24 * 1024 * 1024, written=0, sems=()):
    scratch = [pltpu.VMEM(a.shape, a.dtype) for a in fetched]
    where = VMEM
    if written:
        where = HBM
        scratch += [pltpu.VMEM(a.shape, a.dtype) for a in outs]
    scratch += [pltpu.SemaphoreType.DMA(a) for a in sems or [(len(fetched),)] if fetched]
    if written:
        scratch.append(pltpu.SemaphoreType.DMA((len(outs), written)))
    return pl.pallas_call(
        kernel,
        out_shape=outs,
        in_specs=specs,
        out_specs=jax.tree.map(lambda _: where, outs),
        scratch_shapes=scratch,
        compiler_params=pltpu.CompilerParams(vmem_limit_bytes=limit),
    )


def array(dims, kind):
    return jax.ShapeDtypeStruct(dims, kind)


def exchange(value, axis):
    return lax.all_to_all(value, axis, 0, 0, tiled=True)


def from_everyone(value, axis):
    devices = lax.psum(1, axis)
    return exchange(jnp.broadcast_to(value[None], (devices, *value.shape)), axis)


def on_device(
    stratum_source_matrix,
    acceptance_query,
    cluster_lookup_matrix,
    cluster_payload_matrix,
    fading_logit,
    adaptation_speed_logit,
    additional_fading_exponent,
    result_switch_pair,
    attender_scaling_factor,
    present_item_factor,
    final_mapping_matrix,
    perceptron_scaling_factor,
    switching_matrix,
    widening_matrix,
    shrinking_matrix,
):
    features = perceptron_scaling_factor.shape[0]
    columns = features // lax.axis_size(TP)
    planes = lax.axis_size(PLANE)
    whole = lax.all_gather(
        jnp.concatenate([switching_matrix, widening_matrix, shrinking_matrix.T], axis=1),
        SP,
        axis=0,
        tiled=True,
    )
    blocks = array((4, TOK, LANES), f32)
    inputs = (
        acceptance_query,
        cluster_lookup_matrix,
        cluster_payload_matrix,
        fading_logit,
        adaptation_speed_logit,
        additional_fading_exponent,
        result_switch_pair,
        attender_scaling_factor,
        present_item_factor,
    )
    send, local_out, start_read, scale, extra = call(
        local_kernel,
        (
            array((SHARES, LANES + HALF, LANES), bf16),
            blocks,
            array((4, TOK, 2 * LANES), bf16),
            blocks,
            blocks,
        ),
        [HBM] * len(inputs),
        inputs,
        66_400_000,
        4,
        [(7, 2), (2,)],
    )(*inputs)
    place = lax.axis_index(PLANE).astype(jnp.int32).reshape(1)
    first_column = (lax.axis_index(TP) * columns).astype(jnp.uint32)
    send, place, first_column = lax.optimization_barrier((send, place, first_column))
    prefix, total = call(
        row_kernel,
        (
            array((SHARES, LANES + HALF, LANES), f32),
            array((planes, LANES + HALF, LANES), bf16),
        ),
        [VMEM],
    )(exchange(send, ROW))
    states = call(state_kernel, array((SHARES, HALF, LANES), bf16), [SMEM, VMEM, VMEM])(
        place, exchange(total, PLANE), prefix
    )
    mixing = (
        local_out,
        start_read,
        scale,
        extra,
        exchange(states, ROW),
        final_mapping_matrix.reshape(-1, features),
    )
    terms = call(
        mix_kernel,
        array((features // columns, TOK, columns), bf16),
        [HBM] * len(mixing),
        mixing,
        64_000_000,
    )(*mixing)
    residual = lax.dynamic_slice(
        stratum_source_matrix, (jnp.uint32(0), first_column), (TOK, columns)
    )
    attention = jnp.sum(exchange(terms, TP).astype(f32), axis=0)
    own_state = (residual.astype(f32) + attention).astype(bf16)
    tiles = feed_forward(
        from_everyone(own_state, TP),
        perceptron_scaling_factor.reshape(1, features),
        whole.reshape(planes, features // planes, -1),
    )
    mixer = jnp.sum(exchange(tiles, TP).astype(f32), axis=0)
    return (own_state.astype(f32) + mixer).astype(bf16)


def solution(mesh):
    split = Mesh(mesh.devices.reshape(8, 2, 2, 2, mesh.shape["tp"]), (*SP, TP))
    heads = P(None, SP, "tp")
    return jax.shard_map(
        on_device,
        mesh=split,
        in_specs=(
            P(SP, None),
            heads,
            heads,
            heads,
            heads,
            heads,
            heads,
            heads,
            P(None, TP),
            P(None, TP),
            P(None, TP, None),
            P(),
            P(SP, TP),
            P(SP, TP),
            P(TP, SP),
        ),
        out_specs=P(SP, TP),
        check_vma=False,
    )
```

```python
import jax
import jax.numpy as jnp
from jax import lax
from jax.experimental import pallas as pl
from jax.experimental.pallas import tpu as pltpu
from jax.sharding import Mesh
from jax.sharding import PartitionSpec as P

PLANE, FAR, NEAR, CORE, TP = "plane", "far", "near", "core", "tp"
SP = (PLANE, FAR, NEAR, CORE)
ROW = (FAR, NEAR, CORE)
GATHER = (PLANE, NEAR, CORE)
POOL = (FAR, TP)
TOK = 128
LANES = 128
HALF = 64
SHARES = 8

norm_epsilon = 1e-06
head_epsilon = 0.00064
key_epsilon = 1e-06

f32 = jnp.float32
bf16 = jnp.bfloat16


def dot_nn(a, b):
    return lax.dot_general(a, b, (((1,), (0,)), ((), ())), preferred_element_type=f32)


def dot_nt(a, b):
    return lax.dot_general(a, b, (((1,), (1,)), ((), ())), preferred_element_type=f32)


def dot_tn(a, b):
    return lax.dot_general(a, b, (((0,), (0,)), ((), ())), preferred_element_type=f32)


def halves(a):
    high = a.astype(bf16)
    return high, (a - high.astype(f32)).astype(bf16)


def mm(a, b):
    ah, al = a
    bh, bl = b
    return dot_nn(jnp.concatenate([ah, al], 1), jnp.concatenate([bh, bh], 0)) + dot_nn(ah, bl)


def mm_nt(a, b):
    ah, al = a
    bh, bl = b
    return dot_nt(jnp.concatenate([ah, al], 1), jnp.concatenate([bh, bh], 1)) + dot_nt(ah, bl)


def head_masks(group):
    lane = lax.broadcasted_iota(jnp.int32, (1, LANES), 1)
    if group == 0:
        return [(lane < HALF).astype(f32), (lane >= HALF).astype(f32)]
    return [None]


def head_sum(a, masks):
    if masks[0] is None:
        return jnp.sum(a, axis=1, keepdims=True)
    return sum(jnp.sum(a * m, axis=1, keepdims=True) * m for m in masks)


def masked(a, mask):
    return a if mask is None else a * mask


def fetch(sources, targets, sems):
    copies = [pltpu.make_async_copy(a, b, sems.at[k]) for k, (a, b) in enumerate(zip(sources, targets))]
    for copy in copies:
        copy.start()
    return copies


def slot_lanes(slot):
    cut = (slot % 2) * LANES
    return slot // 2, slice(cut, cut + LANES)


def group_copies(inputs, scratch, sems):
    copies = [
        [
            pltpu.make_async_copy(a.at[group], b.at[group], sems.at[k, group])
            for k, (a, b) in enumerate(zip(inputs, scratch))
        ]
        for group in range(2)
    ]
    for copy in copies[0] + copies[1]:
        copy.start()
    return copies


def writer(results, outputs, sems):
    pending = []

    def put(which, index, count):
        part = pl.ds(index * count, count)
        copy = pltpu.make_async_copy(
            results[which].at[part], outputs[which].at[part], sems.at[which, index]
        )
        copy.start()
        pending.append(copy)

    def finish():
        for copy in pending:
            copy.wait()

    return put, finish


def solve_kernel(*refs):
    inputs, outputs, scratch, results = refs[:6], refs[6:11], refs[11:17], refs[17:22]
    sems, out_sems = refs[22:]
    send_ref, qr_ref, qk_ref, solved_ref, grown_ref = results
    q_ref, k_ref, v_ref, f_ref, l_ref, e_ref = scratch
    copies = group_copies(inputs, scratch, sems)
    put, finish = writer(results, outputs, out_sems)
    row = lax.broadcasted_iota(jnp.int32, (TOK, TOK), 0)
    col = lax.broadcasted_iota(jnp.int32, (TOK, TOK), 1)
    strict = row > col
    inclusive = row >= col
    eye = (row == col).astype(f32)
    ones = inclusive.astype(bf16)
    slots = []
    heads = []
    for slot in range(4):
        group, lanes = slot_lanes(slot)
        if slot % 2 == 0:
            for copy in copies[group]:
                copy.wait()
        q = q_ref[group, :, lanes].astype(f32)
        k = k_ref[group, :, lanes].astype(f32)
        fade = f_ref[group, :, lanes].astype(f32)
        speed = l_ref[group, :, lanes].astype(f32)
        log_decay = e_ref[group, :, lanes] - jnp.exp(-0.5) / (1.0 + jnp.exp(-fade))
        learn = 1.0 / (1.0 + jnp.exp(-speed))
        masks = head_masks(group)
        removal = k * lax.rsqrt(head_sum(k * k, masks) + key_epsilon)
        d0 = log_decay.astype(bf16)
        rest = log_decay - d0.astype(f32)
        d1 = rest.astype(bf16)
        d2 = (rest - d1.astype(f32)).astype(bf16)
        cum = dot_nn(ones, d0) + dot_nn(ones, d1) + dot_nn(ones, d2)
        middle = cum[TOK // 2 : TOK // 2 + 1, :]
        forward = jnp.exp(cum - middle)
        backward = jnp.exp(middle - cum)
        undo = jnp.exp(-log_decay)
        right = learn * removal
        queries = jnp.concatenate([-removal * undo * forward, q * forward], 0)
        sources = halves(jnp.concatenate([right * backward, k * backward], 0))
        final = cum[TOK - 1 : TOK, :]
        tail = jnp.exp(final - cum)
        grown_ref[slot] = q * jnp.exp(cum)
        put(4, slot, 1)
        slots.append(
            dict(
                masks=masks,
                v=v_ref[group, :, lanes],
                start=-removal * jnp.exp(cum - log_decay),
                ends=jnp.concatenate([right * tail, k * tail], 0).astype(bf16),
                kept=jnp.exp(final),
            )
        )
        for mask in masks:
            pairs = mm_nt(halves(masked(queries, mask)), sources)
            head = len(heads)
            qr_ref[head] = jnp.where(inclusive, pairs[TOK:, :TOK], 0.0).astype(bf16)
            qk_ref[head] = jnp.where(inclusive, pairs[TOK:, TOK:], 0.0).astype(bf16)
            put(1, head, 1)
            put(2, head, 1)
            heads.append(
                dict(
                    slot=slot,
                    mask=mask,
                    n=jnp.where(strict, pairs[:TOK, :TOK], 0.0),
                    rk=jnp.where(strict, pairs[:TOK, TOK:], 0.0),
                )
            )
    same = (row // 8) == (col // 8)
    for head in heads:
        head["m"] = jnp.where(same, head["n"], 0.0)
        head["x"] = eye + head["m"]
    for _ in range(2):
        for head in heads:
            m = halves(head["m"])
            head["m"] = mm(m, m)
        for head in heads:
            head["x"] = head["x"] + mm(halves(head["x"]), halves(head["m"]))
    size = 8
    while size < TOK:
        below = (row // (2 * size) == col // (2 * size)) & (row // size != col // size)
        for head in heads:
            off = halves(jnp.where(below, head["n"], 0.0))
            head["y"] = halves(mm(off, halves(head["x"])))
        for head in heads:
            head["x"] = head["x"] + mm(halves(head["x"]), head["y"])
        size *= 2
    for head in heads:
        part = slots[head["slot"]]
        high, low = halves(head["rk"])
        v = part["v"]
        pulled = dot_nn(jnp.concatenate([high, low], 1), jnp.concatenate([v, v], 0))
        head["solved"] = mm(
            halves(head["x"]), halves(jnp.concatenate([pulled, part["start"]], 1))
        )
    for slot, part in enumerate(slots):
        mine = [head for head in heads if head["slot"] == slot]
        solved = mine[0]["solved"]
        if len(mine) == 2:
            first = jnp.concatenate([mine[0]["mask"]] * 2, 1) > 0.5
            solved = jnp.where(first, solved, mine[1]["solved"])
        solved = solved.astype(bf16)
        solved_ref[slot] = solved
        put(3, slot, 1)
        carried, start = solved[:, :LANES], solved[:, LANES:]
        transit = dot_tn(start, part["ends"][:TOK])
        added = dot_tn(jnp.concatenate([carried, part["v"]], 0), part["ends"])
        if len(mine) == 2:
            block = (row // HALF) == (col // HALF)
            transit = jnp.where(block, transit, 0.0)
            added = jnp.where(block, added, 0.0)
        transit = (transit + eye * part["kept"]).astype(bf16)
        added = added.astype(bf16)
        for half in range(2):
            send_ref[2 * slot + half, :LANES, :] = transit
            send_ref[2 * slot + half, LANES:, :] = added[half * HALF : (half + 1) * HALF, :]
        put(0, slot, 2)
    finish()


def read_kernel(*refs):
    inputs, outputs, scratch, results = refs[:10], refs[10:14], refs[14:24], refs[24:28]
    sems, out_sems = refs[28:]
    qr_ref, qk_ref, solved_ref, grown_ref, q_ref, k_ref, v_ref, gate_ref, gain_ref, own_ref = scratch
    out_ref, read_ref, scale_ref, extra_ref = results
    for copy in fetch(inputs, scratch, sems):
        copy.wait()
    put, finish = writer(results, outputs, out_sems)
    head = 0
    for slot in range(4):
        group, lanes = slot_lanes(slot)
        masks = head_masks(group)
        v = v_ref[group, :, lanes]
        found = local = None
        for mask in masks:
            one = dot_nn(qr_ref[head], solved_ref[slot])
            here = one[:, :LANES] + dot_nn(qk_ref[head], v)
            if found is None:
                found, local = one[:, LANES:], here
            else:
                found = jnp.where(mask > 0.5, one[:, LANES:], found)
                local = jnp.where(mask > 0.5, here, local)
            head += 1
        out_ref[slot] = local
        high, low = halves(grown_ref[slot] + found)
        read_ref[slot, :, :LANES] = high
        read_ref[slot, :, LANES:] = low
        gate = gate_ref[group, :, lanes].astype(f32)
        scale_ref[slot] = gain_ref[group : group + 1, lanes] * gate
        q = q_ref[group, :, lanes].astype(f32)
        k = k_ref[group, :, lanes].astype(f32)
        own = head_sum(q * k * own_ref[group : group + 1, lanes], masks)
        extra_ref[slot] = own * v.astype(f32) * gate
        for which in range(4):
            put(which, slot, 1)
    finish()


def row_kernel(got_ref, prefix_ref, total_ref):
    row = lax.broadcasted_iota(jnp.int32, (LANES + HALF, LANES), 0)
    col = lax.broadcasted_iota(jnp.int32, (LANES + HALF, LANES), 1)
    zero = jnp.zeros((LANES, LANES), f32)
    prefix_ref[0] = (row == col).astype(f32)
    run = got_ref[0].astype(f32)
    for k in range(1, SHARES):
        prefix_ref[k] = run
        got = got_ref[k]
        step = got[:LANES]
        high, low = halves(run)
        run = dot_nn(jnp.concatenate([high, low], 1), jnp.concatenate([step, step], 0))
        run = run + jnp.concatenate([zero, got[LANES:].astype(f32)], 0)
    total = run.astype(bf16)
    for k in range(total_ref.shape[0]):
        total_ref[k] = total


def state_kernel(place_ref, every_ref, prefix_ref, send_ref):
    place = place_ref[0]
    state = jnp.zeros((HALF, LANES), f32)
    for k in range(every_ref.shape[0] - 1):
        got = every_ref[k]
        step = got[:LANES]
        high, low = halves(state)
        grown = dot_nn(jnp.concatenate([high, low], 1), jnp.concatenate([step, step], 0))
        state = jnp.where(k < place, grown + got[LANES:].astype(f32), state)
    split = halves(state)
    for k in range(SHARES):
        moved = mm(split, halves(prefix_ref[k, :LANES, :]))
        send_ref[k] = (moved + prefix_ref[k, LANES:, :]).astype(bf16)


def mix_kernel(*refs):
    state_ref, inputs, y_ref, scratch, sems = refs[0], refs[1:6], refs[6], refs[7:12], refs[12]
    out_ref, read_ref, scale_ref, extra_ref, w_ref = scratch
    copies = fetch(inputs, scratch, sems)
    for copy in copies[:4]:
        copy.wait()
    mixed = []
    for slot in range(4):
        width = HALF if slot < 2 else LANES
        masks = head_masks(slot // 2)
        state = jnp.concatenate([state_ref[2 * slot], state_ref[2 * slot + 1]], 0)
        raw = out_ref[slot] + dot_nt(read_ref[slot], jnp.concatenate([state, state], 1))
        centered = raw - head_sum(raw, masks) * (1.0 / width)
        variance = head_sum(centered * centered, masks) * (1.0 / width)
        normed = centered * lax.rsqrt(variance + head_epsilon) * scale_ref[slot]
        mixed.append((normed + extra_ref[slot]).astype(bf16))
    mixed = jnp.concatenate(mixed, 1)
    copies[4].wait()
    tiles, _, columns = y_ref.shape
    for k in range(tiles):
        y_ref[k] = dot_nn(mixed, w_ref[:, k * columns : (k + 1) * columns]).astype(bf16)


AHEAD = 4


def feed_kernel(far_ref, x_ref, gain_ref, whole_ref, y_ref, w_ref, n_ref, acc_ref, sems):
    planes, sides, near, rows, width = w_ref.shape
    third = width // 3
    far = far_ref[0]
    copies = [
        [
            pltpu.make_async_copy(
                whole_ref.at[k, :, jnp.where(far == side, 0, 1)],
                w_ref.at[k, side],
                sems.at[k, side],
            )
            for side in range(sides)
        ]
        for k in range(planes)
    ]
    for k in range(AHEAD):
        for copy in copies[k]:
            copy.start()
    shares, tokens, columns = x_ref.shape
    tiles = shares // sides
    for side in range(sides):
        parts = [x_ref[side * tiles + k].astype(f32) for k in range(tiles)]
        total = sum(jnp.sum(a * a, axis=1, keepdims=True) for a in parts)
        scale = lax.rsqrt(total * (1.0 / (tiles * columns)) + norm_epsilon)
        for k, a in enumerate(parts):
            lanes = slice(k * columns, (k + 1) * columns)
            n_ref[side * tokens : (side + 1) * tokens, lanes] = (
                a * scale * gain_ref[:, lanes]
            ).astype(bf16)
    block = sides * near * rows
    for k in range(0, planes, 2):
        for step in (k, k + 1):
            for copy in copies[step]:
                copy.wait()
            if step + AHEAD < planes:
                for copy in copies[step + AHEAD]:
                    copy.start()
        part = dot_nn(
            n_ref[:, k * block : (k + 2) * block],
            w_ref[k : k + 2, :, :, :, : 2 * third].reshape(2 * block, 2 * third),
        )
        if k == 0:
            acc_ref[...] = part
        else:
            acc_ref[...] += part
    gate = acc_ref[:, :third]
    active = (gate / (1.0 + jnp.exp(-gate)) * acc_ref[:, third:]).astype(bf16)
    per = planes // tiles
    for k in range(tiles):
        down = w_ref[k * per : (k + 1) * per, :, :, :, 2 * third :].reshape(per * block, third)
        out = dot_nt(active, down).astype(bf16)
        for side in range(sides):
            y_ref[side * tiles + k] = out[side * tokens : (side + 1) * tokens]


def feed_forward(far, state, gain, whole):
    planes, near, sides, rows, width = whole.shape
    shares, tokens, columns = state.shape
    return pl.pallas_call(
        feed_kernel,
        out_shape=array((shares, tokens, columns), bf16),
        in_specs=[SMEM, VMEM, VMEM, HBM],
        out_specs=VMEM,
        scratch_shapes=[
            pltpu.VMEM((planes, sides, near, rows, width), bf16),
            pltpu.VMEM((sides * tokens, gain.shape[1]), bf16),
            pltpu.VMEM((sides * tokens, 2 * width // 3), f32),
            pltpu.SemaphoreType.DMA((planes, sides)),
        ],
        compiler_params=pltpu.CompilerParams(vmem_limit_bytes=60_000_000),
    )(far, state, gain, whole)


def pack_kernel(far_ref, *refs):
    inputs, (kept_ref, given_ref), scratch, sems = refs[:3], refs[3:5], refs[5:8], refs[8]
    copies = fetch(inputs, scratch, sems)
    wide = kept_ref.shape[1] // 3
    first = far_ref[0] == 0
    for k, copy in enumerate(copies):
        copy.wait()
        lanes = slice(k * wide, (k + 1) * wide)
        kept_ref[given_ref.shape[0] :, lanes] = jnp.zeros((given_ref.shape[0], wide), bf16)
        near = scratch[k][:, :wide]
        rest = scratch[k][:, wide:]
        blank = jnp.zeros((rest.shape[0], 2 * wide - scratch[k].shape[1]), bf16)
        far = jnp.concatenate([rest, blank], axis=1)
        kept_ref[: near.shape[0], lanes] = jnp.where(first, near, far)
        given_ref[:, lanes] = jnp.where(first, far, near)


def swapped(far, parts):
    rows, hidden = parts[0].shape
    wide = -(-hidden // (2 * LANES)) * LANES
    packed = (array((2 * rows, 3 * wide), bf16), array((rows, 3 * wide), bf16))
    kept, given = call(pack_kernel, packed, [SMEM] + [HBM] * 3, parts, 62_000_000)(far, *parts)
    return kept, lax.ppermute(given, FAR, [(0, 1), (1, 0)])


def gathered(kept, taken):
    rows, width = taken.shape
    both = lax.dynamic_update_slice(kept, taken, (rows, 0))
    whole = lax.all_gather(both, GATHER, axis=0, tiled=True)
    planes = lax.axis_size(PLANE)
    near = lax.axis_size(NEAR) * lax.axis_size(CORE)
    return whole.reshape(planes, near, 2, rows, width)


VMEM = pl.BlockSpec(memory_space=pltpu.VMEM)
HBM = pl.BlockSpec(memory_space=pltpu.HBM)
SMEM = pl.BlockSpec(memory_space=pltpu.SMEM)


def call(kernel, outs, specs, fetched=(), limit=24 * 1024 * 1024, written=0, sems=()):
    scratch = [pltpu.VMEM(a.shape, a.dtype) for a in fetched]
    where = VMEM
    if written:
        where = HBM
        scratch += [pltpu.VMEM(a.shape, a.dtype) for a in outs]
    scratch += [pltpu.SemaphoreType.DMA(a) for a in sems or [(len(fetched),)] if fetched]
    if written:
        scratch.append(pltpu.SemaphoreType.DMA((len(outs), written)))
    return pl.pallas_call(
        kernel,
        out_shape=outs,
        in_specs=specs,
        out_specs=jax.tree.map(lambda _: where, outs),
        scratch_shapes=scratch,
        compiler_params=pltpu.CompilerParams(vmem_limit_bytes=limit),
    )


def array(dims, kind):
    return jax.ShapeDtypeStruct(dims, kind)


def exchange(value, axis):
    return lax.all_to_all(value, axis, 0, 0, tiled=True)


def from_everyone(value, axis):
    devices = lax.psum(1, axis)
    return exchange(jnp.broadcast_to(value[None], (devices, *value.shape)), axis)


def on_device(
    stratum_source_matrix,
    acceptance_query,
    cluster_lookup_matrix,
    cluster_payload_matrix,
    fading_logit,
    adaptation_speed_logit,
    additional_fading_exponent,
    result_switch_pair,
    attender_scaling_factor,
    present_item_factor,
    final_mapping_matrix,
    perceptron_scaling_factor,
    switching_matrix,
    widening_matrix,
    shrinking_matrix,
):
    features = perceptron_scaling_factor.shape[0]
    columns = features // lax.axis_size(TP)
    far = lax.axis_index(FAR).astype(jnp.int32).reshape(1)
    kept, taken = swapped(far, [switching_matrix, widening_matrix, shrinking_matrix.T])
    blocks = array((4, TOK, LANES), f32)
    pairs = array((6, TOK, TOK), bf16)
    doubled = array((4, TOK, 2 * LANES), bf16)
    inputs = (
        acceptance_query,
        cluster_lookup_matrix,
        cluster_payload_matrix,
        fading_logit,
        adaptation_speed_logit,
        additional_fading_exponent,
    )
    send, *found = call(
        solve_kernel,
        (array((SHARES, LANES + HALF, LANES), bf16), pairs, pairs, doubled, blocks),
        [HBM] * len(inputs),
        inputs,
        66_400_000,
        6,
        [(len(inputs), 2)],
    )(*inputs)
    place = lax.axis_index(PLANE).astype(jnp.int32).reshape(1)
    first_column = (lax.axis_index(TP) * columns).astype(jnp.uint32)
    send, taken, place, first_column = lax.optimization_barrier((send, taken, place, first_column))
    whole = gathered(kept, taken)
    planes = lax.axis_size(PLANE)
    prefix, total = call(
        row_kernel,
        (
            array((SHARES, LANES + HALF, LANES), f32),
            array((planes, LANES + HALF, LANES), bf16),
        ),
        [VMEM],
    )(exchange(send, ROW))
    total, *found = lax.optimization_barrier((total, *found))
    reading = (
        *found,
        *inputs[:3],
        result_switch_pair,
        attender_scaling_factor,
        present_item_factor,
    )
    read = call(
        read_kernel,
        (blocks, doubled, blocks, blocks),
        [HBM] * len(reading),
        reading,
        66_400_000,
        4,
    )(*reading)
    states = call(state_kernel, array((SHARES, HALF, LANES), bf16), [SMEM, VMEM, VMEM])(
        place, exchange(total, PLANE), prefix
    )
    mixing = (*read, final_mapping_matrix.reshape(-1, features))
    terms = call(
        mix_kernel,
        array((features // columns, TOK, columns), bf16),
        [VMEM] + [HBM] * len(mixing),
        mixing,
        64_000_000,
    )(exchange(states, ROW), *mixing)
    residual = lax.dynamic_slice(
        stratum_source_matrix, (jnp.uint32(0), first_column), (TOK, columns)
    )
    attention = jnp.sum(exchange(terms, TP).astype(f32), axis=0)
    own_state = (residual.astype(f32) + attention).astype(bf16)
    tiles = feed_forward(
        far,
        from_everyone(own_state, POOL),
        perceptron_scaling_factor.reshape(1, features),
        whole,
    )
    mixer = jnp.sum(exchange(tiles, POOL).astype(f32), axis=0)
    return (own_state.astype(f32) + mixer).astype(bf16)


def solution(mesh):
    split = Mesh(mesh.devices.reshape(8, 2, 2, 2, mesh.shape["tp"]), (*SP, TP))
    heads = P(None, SP, "tp")
    return jax.shard_map(
        on_device,
        mesh=split,
        in_specs=(
            P(SP, None),
            heads,
            heads,
            heads,
            heads,
            heads,
            heads,
            heads,
            P(None, TP),
            P(None, TP),
            P(None, TP, None),
            P(),
            P(SP, TP),
            P(SP, TP),
            P(TP, SP),
        ),
        out_specs=P(SP, TP),
        check_vma=False,
    )
```

```python
import jax
import jax.numpy as jnp
from jax import lax
from jax.experimental import pallas as pl
from jax.experimental.pallas import tpu as pltpu
from jax.sharding import Mesh
from jax.sharding import PartitionSpec as P

PLANE, FAR, NEAR, CORE, TP = "plane", "far", "near", "core", "tp"
SP = (PLANE, FAR, NEAR, CORE)
ROW = (FAR, NEAR, CORE)
GATHER = (PLANE, NEAR, CORE)
POOL = (FAR, TP)
TOK = 128
LANES = 128
HALF = 64
SHARES = 8

norm_epsilon = 1e-06
head_epsilon = 0.00064
key_epsilon = 1e-06

f32 = jnp.float32
bf16 = jnp.bfloat16


def dot_nn(a, b):
    return lax.dot_general(a, b, (((1,), (0,)), ((), ())), preferred_element_type=f32)


def dot_nt(a, b):
    return lax.dot_general(a, b, (((1,), (1,)), ((), ())), preferred_element_type=f32)


def dot_tn(a, b):
    return lax.dot_general(a, b, (((0,), (0,)), ((), ())), preferred_element_type=f32)


def halves(a):
    high = a.astype(bf16)
    return high, (a - high.astype(f32)).astype(bf16)


def mm(a, b):
    ah, al = a
    bh, bl = b
    return dot_nn(jnp.concatenate([ah, al], 1), jnp.concatenate([bh, bh], 0)) + dot_nn(ah, bl)


def mm_nt(a, b):
    ah, al = a
    bh, bl = b
    return dot_nt(jnp.concatenate([ah, al], 1), jnp.concatenate([bh, bh], 1)) + dot_nt(ah, bl)


def head_masks(group):
    lane = lax.broadcasted_iota(jnp.int32, (1, LANES), 1)
    if group == 0:
        return [(lane < HALF).astype(f32), (lane >= HALF).astype(f32)]
    return [None]


def head_sum(a, masks):
    if masks[0] is None:
        return jnp.sum(a, axis=1, keepdims=True)
    return sum(jnp.sum(a * m, axis=1, keepdims=True) * m for m in masks)


def masked(a, mask):
    return a if mask is None else a * mask


def fetch(sources, targets, sems):
    copies = [pltpu.make_async_copy(a, b, sems.at[k]) for k, (a, b) in enumerate(zip(sources, targets))]
    for copy in copies:
        copy.start()
    return copies


def slot_lanes(slot):
    cut = (slot % 2) * LANES
    return slot // 2, slice(cut, cut + LANES)


def group_copies(inputs, scratch, sems):
    copies = [
        [
            pltpu.make_async_copy(a.at[group], b.at[group], sems.at[k, group])
            for k, (a, b) in enumerate(zip(inputs, scratch))
        ]
        for group in range(2)
    ]
    for copy in copies[0] + copies[1]:
        copy.start()
    return copies


def writer(results, outputs, sems):
    pending = []

    def put(which, index, count):
        part = pl.ds(index * count, count)
        copy = pltpu.make_async_copy(
            results[which].at[part], outputs[which].at[part], sems.at[which, index]
        )
        copy.start()
        pending.append(copy)

    def finish():
        for copy in pending:
            copy.wait()

    return put, finish


def solve_kernel(*refs):
    inputs, outputs, scratch, results = refs[:6], refs[6:11], refs[11:17], refs[17:22]
    sems, out_sems = refs[22:]
    send_ref, qr_ref, qk_ref, solved_ref, grown_ref = results
    q_ref, k_ref, v_ref, f_ref, l_ref, e_ref = scratch
    copies = group_copies(inputs, scratch, sems)
    put, finish = writer(results, outputs, out_sems)
    row = lax.broadcasted_iota(jnp.int32, (TOK, TOK), 0)
    col = lax.broadcasted_iota(jnp.int32, (TOK, TOK), 1)
    strict = row > col
    inclusive = row >= col
    eye = (row == col).astype(f32)
    ones = inclusive.astype(bf16)
    slots = []
    heads = []
    for slot in range(4):
        group, lanes = slot_lanes(slot)
        if slot % 2 == 0:
            for copy in copies[group]:
                copy.wait()
        q = q_ref[group, :, lanes].astype(f32)
        k = k_ref[group, :, lanes].astype(f32)
        fade = f_ref[group, :, lanes].astype(f32)
        speed = l_ref[group, :, lanes].astype(f32)
        log_decay = e_ref[group, :, lanes] - jnp.exp(-0.5) / (1.0 + jnp.exp(-fade))
        learn = 1.0 / (1.0 + jnp.exp(-speed))
        masks = head_masks(group)
        removal = k * lax.rsqrt(head_sum(k * k, masks) + key_epsilon)
        d0 = log_decay.astype(bf16)
        rest = log_decay - d0.astype(f32)
        d1 = rest.astype(bf16)
        d2 = (rest - d1.astype(f32)).astype(bf16)
        cum = dot_nn(ones, d0) + dot_nn(ones, d1) + dot_nn(ones, d2)
        middle = cum[TOK // 2 : TOK // 2 + 1, :]
        forward = jnp.exp(cum - middle)
        backward = jnp.exp(middle - cum)
        undo = jnp.exp(-log_decay)
        right = learn * removal
        queries = jnp.concatenate([-removal * undo * forward, q * forward], 0)
        sources = halves(jnp.concatenate([right * backward, k * backward], 0))
        final = cum[TOK - 1 : TOK, :]
        tail = jnp.exp(final - cum)
        grown_ref[slot] = q * jnp.exp(cum)
        put(4, slot, 1)
        slots.append(
            dict(
                masks=masks,
                v=v_ref[group, :, lanes],
                start=-removal * jnp.exp(cum - log_decay),
                ends=jnp.concatenate([right * tail, k * tail], 0).astype(bf16),
                kept=jnp.exp(final),
            )
        )
        for mask in masks:
            pairs = mm_nt(halves(masked(queries, mask)), sources)
            head = len(heads)
            qr_ref[head] = jnp.where(inclusive, pairs[TOK:, :TOK], 0.0).astype(bf16)
            qk_ref[head] = jnp.where(inclusive, pairs[TOK:, TOK:], 0.0).astype(bf16)
            put(1, head, 1)
            put(2, head, 1)
            heads.append(
                dict(
                    slot=slot,
                    mask=mask,
                    n=jnp.where(strict, pairs[:TOK, :TOK], 0.0),
                    rk=jnp.where(strict, pairs[:TOK, TOK:], 0.0),
                )
            )
    same = (row // 8) == (col // 8)
    for head in heads:
        head["m"] = jnp.where(same, head["n"], 0.0)
        head["x"] = eye + head["m"]
    for _ in range(2):
        for head in heads:
            m = halves(head["m"])
            head["m"] = mm(m, m)
        for head in heads:
            head["x"] = head["x"] + mm(halves(head["x"]), halves(head["m"]))
    size = 8
    while size < TOK:
        below = (row // (2 * size) == col // (2 * size)) & (row // size != col // size)
        for head in heads:
            off = halves(jnp.where(below, head["n"], 0.0))
            head["y"] = halves(mm(off, halves(head["x"])))
        for head in heads:
            head["x"] = head["x"] + mm(halves(head["x"]), head["y"])
        size *= 2
    for head in heads:
        part = slots[head["slot"]]
        high, low = halves(head["rk"])
        v = part["v"]
        pulled = dot_nn(jnp.concatenate([high, low], 1), jnp.concatenate([v, v], 0))
        head["solved"] = mm(
            halves(head["x"]), halves(jnp.concatenate([pulled, part["start"]], 1))
        )
    for slot, part in enumerate(slots):
        mine = [head for head in heads if head["slot"] == slot]
        solved = mine[0]["solved"]
        if len(mine) == 2:
            first = jnp.concatenate([mine[0]["mask"]] * 2, 1) > 0.5
            solved = jnp.where(first, solved, mine[1]["solved"])
        solved = solved.astype(bf16)
        solved_ref[slot] = solved
        put(3, slot, 1)
        carried, start = solved[:, :LANES], solved[:, LANES:]
        transit = dot_tn(start, part["ends"][:TOK])
        added = dot_tn(jnp.concatenate([carried, part["v"]], 0), part["ends"])
        if len(mine) == 2:
            block = (row // HALF) == (col // HALF)
            transit = jnp.where(block, transit, 0.0)
            added = jnp.where(block, added, 0.0)
        transit = (transit + eye * part["kept"]).astype(bf16)
        added = added.astype(bf16)
        for half in range(2):
            send_ref[2 * slot + half, :LANES, :] = transit
            send_ref[2 * slot + half, LANES:, :] = added[half * HALF : (half + 1) * HALF, :]
        put(0, slot, 2)
    finish()


def read_kernel(*refs):
    inputs, outputs, scratch, results = refs[:10], refs[10:14], refs[14:24], refs[24:28]
    sems, out_sems = refs[28:]
    qr_ref, qk_ref, solved_ref, grown_ref, q_ref, k_ref, v_ref, gate_ref, gain_ref, own_ref = scratch
    out_ref, read_ref, scale_ref, extra_ref = results
    for copy in fetch(inputs, scratch, sems):
        copy.wait()
    put, finish = writer(results, outputs, out_sems)
    head = 0
    for slot in range(4):
        group, lanes = slot_lanes(slot)
        masks = head_masks(group)
        v = v_ref[group, :, lanes]
        found = local = None
        for mask in masks:
            one = dot_nn(qr_ref[head], solved_ref[slot])
            here = one[:, :LANES] + dot_nn(qk_ref[head], v)
            if found is None:
                found, local = one[:, LANES:], here
            else:
                found = jnp.where(mask > 0.5, one[:, LANES:], found)
                local = jnp.where(mask > 0.5, here, local)
            head += 1
        out_ref[slot] = local
        high, low = halves(grown_ref[slot] + found)
        read_ref[slot, :, :LANES] = high
        read_ref[slot, :, LANES:] = low
        gate = gate_ref[group, :, lanes].astype(f32)
        scale_ref[slot] = gain_ref[group : group + 1, lanes] * gate
        q = q_ref[group, :, lanes].astype(f32)
        k = k_ref[group, :, lanes].astype(f32)
        own = head_sum(q * k * own_ref[group : group + 1, lanes], masks)
        extra_ref[slot] = own * v.astype(f32) * gate
        for which in range(4):
            put(which, slot, 1)
    finish()


def row_kernel(got_ref, prefix_ref, total_ref):
    row = lax.broadcasted_iota(jnp.int32, (LANES + HALF, LANES), 0)
    col = lax.broadcasted_iota(jnp.int32, (LANES + HALF, LANES), 1)
    zero = jnp.zeros((LANES, LANES), f32)
    prefix_ref[0] = (row == col).astype(f32)
    run = got_ref[0].astype(f32)
    for k in range(1, SHARES):
        prefix_ref[k] = run
        got = got_ref[k]
        step = got[:LANES]
        high, low = halves(run)
        run = dot_nn(jnp.concatenate([high, low], 1), jnp.concatenate([step, step], 0))
        run = run + jnp.concatenate([zero, got[LANES:].astype(f32)], 0)
    total = run.astype(bf16)
    for k in range(total_ref.shape[0]):
        total_ref[k] = total


def state_kernel(place_ref, every_ref, prefix_ref, send_ref):
    place = place_ref[0]
    state = jnp.zeros((HALF, LANES), f32)
    for k in range(every_ref.shape[0] - 1):
        got = every_ref[k]
        step = got[:LANES]
        high, low = halves(state)
        grown = dot_nn(jnp.concatenate([high, low], 1), jnp.concatenate([step, step], 0))
        state = jnp.where(k < place, grown + got[LANES:].astype(f32), state)
    split = halves(state)
    for k in range(SHARES):
        moved = mm(split, halves(prefix_ref[k, :LANES, :]))
        send_ref[k] = (moved + prefix_ref[k, LANES:, :]).astype(bf16)


def mix_kernel(*refs):
    inputs, outputs, scratch, results, sems, out_sems = (
        refs[:6],
        refs[6:7],
        refs[7:13],
        refs[13:14],
        refs[14],
        refs[15],
    )
    state_ref, out_ref, read_ref, scale_ref, extra_ref, w_ref = scratch
    copies = fetch(inputs, scratch, sems)
    put, finish = writer(results, outputs, out_sems)
    for copy in copies[:5]:
        copy.wait()
    mixed = []
    for slot in range(4):
        width = HALF if slot < 2 else LANES
        masks = head_masks(slot // 2)
        state = jnp.concatenate([state_ref[2 * slot], state_ref[2 * slot + 1]], 0)
        raw = out_ref[slot] + dot_nt(read_ref[slot], jnp.concatenate([state, state], 1))
        centered = raw - head_sum(raw, masks) * (1.0 / width)
        variance = head_sum(centered * centered, masks) * (1.0 / width)
        normed = centered * lax.rsqrt(variance + head_epsilon) * scale_ref[slot]
        mixed.append((normed + extra_ref[slot]).astype(bf16))
    mixed = jnp.concatenate(mixed, 1)
    copies[5].wait()
    tiles, _, columns = results[0].shape
    for k in range(tiles):
        results[0][k] = dot_nn(mixed, w_ref[:, k * columns : (k + 1) * columns]).astype(bf16)
        put(0, k, 1)
    finish()


AHEAD = 4


def feed_kernel(
    far_ref,
    state_ref,
    gain_in_ref,
    whole_ref,
    sent_ref,
    w_ref,
    n_ref,
    acc_ref,
    x_ref,
    gain_ref,
    y_ref,
    sems,
    in_sems,
    out_sems,
):
    tokens_here = fetch([state_ref, gain_in_ref], [x_ref, gain_ref], in_sems)
    put, finish = writer([y_ref], [sent_ref], out_sems)
    planes, sides, near, rows, width = w_ref.shape
    third = width // 3
    far = far_ref[0]
    copies = [
        [
            pltpu.make_async_copy(
                whole_ref.at[k, :, jnp.where(far == side, 0, 1)],
                w_ref.at[k, side],
                sems.at[k, side],
            )
            for side in range(sides)
        ]
        for k in range(planes)
    ]
    for k in range(AHEAD):
        for copy in copies[k]:
            copy.start()
    shares, tokens, columns = x_ref.shape
    tiles = shares // sides
    for copy in tokens_here:
        copy.wait()
    for side in range(sides):
        parts = [x_ref[side * tiles + k].astype(f32) for k in range(tiles)]
        total = sum(jnp.sum(a * a, axis=1, keepdims=True) for a in parts)
        scale = lax.rsqrt(total * (1.0 / (tiles * columns)) + norm_epsilon)
        for k, a in enumerate(parts):
            lanes = slice(k * columns, (k + 1) * columns)
            n_ref[side * tokens : (side + 1) * tokens, lanes] = (
                a * scale * gain_ref[:, lanes]
            ).astype(bf16)
    block = sides * near * rows
    for k in range(0, planes, 2):
        for step in (k, k + 1):
            for copy in copies[step]:
                copy.wait()
            if step + AHEAD < planes:
                for copy in copies[step + AHEAD]:
                    copy.start()
        part = dot_nn(
            n_ref[:, k * block : (k + 2) * block],
            w_ref[k : k + 2, :, :, :, : 2 * third].reshape(2 * block, 2 * third),
        )
        if k == 0:
            acc_ref[...] = part
        else:
            acc_ref[...] += part
    gate = acc_ref[:, :third]
    active = (gate / (1.0 + jnp.exp(-gate)) * acc_ref[:, third:]).astype(bf16)
    per = planes // tiles
    for k in range(tiles):
        down = w_ref[k * per : (k + 1) * per, :, :, :, 2 * third :].reshape(per * block, third)
        out = dot_nt(active, down).astype(bf16)
        for side in range(sides):
            y_ref[side * tiles + k] = out[side * tokens : (side + 1) * tokens]
            put(0, side * tiles + k, 1)
    finish()


def feed_forward(far, state, gain, whole):
    planes, near, sides, rows, width = whole.shape
    shares, tokens, columns = state.shape
    return pl.pallas_call(
        feed_kernel,
        out_shape=array((shares, tokens, columns), bf16),
        in_specs=[SMEM, HBM, HBM, HBM],
        out_specs=HBM,
        scratch_shapes=[
            pltpu.VMEM((planes, sides, near, rows, width), bf16),
            pltpu.VMEM((sides * tokens, gain.shape[1]), bf16),
            pltpu.VMEM((sides * tokens, 2 * width // 3), f32),
            pltpu.VMEM(state.shape, bf16),
            pltpu.VMEM(gain.shape, f32),
            pltpu.VMEM(state.shape, bf16),
            pltpu.SemaphoreType.DMA((planes, sides)),
            pltpu.SemaphoreType.DMA((2,)),
            pltpu.SemaphoreType.DMA((1, shares)),
        ],
        compiler_params=pltpu.CompilerParams(vmem_limit_bytes=60_000_000),
    )(far, state, gain, whole)


def pack_kernel(far_ref, *refs):
    inputs, (kept_ref, given_ref), scratch, sems = refs[:3], refs[3:5], refs[5:8], refs[8]
    copies = fetch(inputs, scratch, sems)
    wide = kept_ref.shape[1] // 3
    first = far_ref[0] == 0
    for k, copy in enumerate(copies):
        copy.wait()
        lanes = slice(k * wide, (k + 1) * wide)
        kept_ref[given_ref.shape[0] :, lanes] = jnp.zeros((given_ref.shape[0], wide), bf16)
        near = scratch[k][:, :wide]
        rest = scratch[k][:, wide:]
        blank = jnp.zeros((rest.shape[0], 2 * wide - scratch[k].shape[1]), bf16)
        far = jnp.concatenate([rest, blank], axis=1)
        kept_ref[: near.shape[0], lanes] = jnp.where(first, near, far)
        given_ref[:, lanes] = jnp.where(first, far, near)


def swapped(far, parts):
    rows, hidden = parts[0].shape
    wide = -(-hidden // (2 * LANES)) * LANES
    packed = (array((2 * rows, 3 * wide), bf16), array((rows, 3 * wide), bf16))
    kept, given = call(pack_kernel, packed, [SMEM] + [HBM] * 3, parts, 62_000_000)(far, *parts)
    return kept, lax.ppermute(given, FAR, [(0, 1), (1, 0)])


def gathered(kept, taken):
    rows, width = taken.shape
    both = lax.dynamic_update_slice(kept, taken, (rows, 0))
    whole = lax.all_gather(both, GATHER, axis=0, tiled=True)
    planes = lax.axis_size(PLANE)
    near = lax.axis_size(NEAR) * lax.axis_size(CORE)
    return whole.reshape(planes, near, 2, rows, width)


VMEM = pl.BlockSpec(memory_space=pltpu.VMEM)
HBM = pl.BlockSpec(memory_space=pltpu.HBM)
SMEM = pl.BlockSpec(memory_space=pltpu.SMEM)


def call(kernel, outs, specs, fetched=(), limit=24 * 1024 * 1024, written=0, sems=()):
    scratch = [pltpu.VMEM(a.shape, a.dtype) for a in fetched]
    where = VMEM
    if written:
        where = HBM
        scratch += [pltpu.VMEM(a.shape, a.dtype) for a in outs]
    scratch += [pltpu.SemaphoreType.DMA(a) for a in sems or [(len(fetched),)] if fetched]
    if written:
        scratch.append(pltpu.SemaphoreType.DMA((len(outs), written)))
    return pl.pallas_call(
        kernel,
        out_shape=outs,
        in_specs=specs,
        out_specs=jax.tree.map(lambda _: where, outs),
        scratch_shapes=scratch,
        compiler_params=pltpu.CompilerParams(vmem_limit_bytes=limit),
    )


def array(dims, kind):
    return jax.ShapeDtypeStruct(dims, kind)


def exchange(value, axis):
    return lax.all_to_all(value, axis, 0, 0, tiled=True)


def from_everyone(value, axis):
    devices = lax.psum(1, axis)
    return exchange(jnp.broadcast_to(value[None], (devices, *value.shape)), axis)


def on_device(
    stratum_source_matrix,
    acceptance_query,
    cluster_lookup_matrix,
    cluster_payload_matrix,
    fading_logit,
    adaptation_speed_logit,
    additional_fading_exponent,
    result_switch_pair,
    attender_scaling_factor,
    present_item_factor,
    final_mapping_matrix,
    perceptron_scaling_factor,
    switching_matrix,
    widening_matrix,
    shrinking_matrix,
):
    features = perceptron_scaling_factor.shape[0]
    columns = features // lax.axis_size(TP)
    far = lax.axis_index(FAR).astype(jnp.int32).reshape(1)
    kept, taken = swapped(far, [switching_matrix, widening_matrix, shrinking_matrix.T])
    blocks = array((4, TOK, LANES), f32)
    pairs = array((6, TOK, TOK), bf16)
    doubled = array((4, TOK, 2 * LANES), bf16)
    inputs = (
        acceptance_query,
        cluster_lookup_matrix,
        cluster_payload_matrix,
        fading_logit,
        adaptation_speed_logit,
        additional_fading_exponent,
    )
    send, *found = call(
        solve_kernel,
        (array((SHARES, LANES + HALF, LANES), bf16), pairs, pairs, doubled, blocks),
        [HBM] * len(inputs),
        inputs,
        66_400_000,
        6,
        [(len(inputs), 2)],
    )(*inputs)
    place = lax.axis_index(PLANE).astype(jnp.int32).reshape(1)
    first_column = (lax.axis_index(TP) * columns).astype(jnp.uint32)
    send, taken, place, first_column = lax.optimization_barrier((send, taken, place, first_column))
    whole = gathered(kept, taken)
    planes = lax.axis_size(PLANE)
    prefix, total = call(
        row_kernel,
        (
            array((SHARES, LANES + HALF, LANES), f32),
            array((planes, LANES + HALF, LANES), bf16),
        ),
        [VMEM],
    )(exchange(send, ROW))
    total, *found = lax.optimization_barrier((total, *found))
    reading = (
        *found,
        *inputs[:3],
        result_switch_pair,
        attender_scaling_factor,
        present_item_factor,
    )
    read = call(
        read_kernel,
        (blocks, doubled, blocks, blocks),
        [HBM] * len(reading),
        reading,
        65300000,
        4,
    )(*reading)
    every, *read = lax.optimization_barrier((exchange(total, PLANE), *read))
    states = call(state_kernel, array((SHARES, HALF, LANES), bf16), [SMEM, VMEM, VMEM])(
        place, every, prefix
    )
    mixing = (exchange(states, ROW), *read, final_mapping_matrix.reshape(-1, features))
    (terms,) = call(
        mix_kernel,
        (array((features // columns, TOK, columns), bf16),),
        [HBM] * len(mixing),
        mixing,
        64_000_000,
        features // columns,
    )(*mixing)
    residual = lax.dynamic_slice(
        stratum_source_matrix, (jnp.uint32(0), first_column), (TOK, columns)
    )
    attention = jnp.sum(exchange(terms, TP).astype(f32), axis=0)
    own_state = (residual.astype(f32) + attention).astype(bf16)
    tiles = feed_forward(
        far,
        from_everyone(own_state, POOL),
        perceptron_scaling_factor.reshape(1, features),
        whole,
    )
    mixer = jnp.sum(exchange(tiles, POOL).astype(f32), axis=0)
    return (own_state.astype(f32) + mixer).astype(bf16)


def solution(mesh):
    split = Mesh(mesh.devices.reshape(8, 2, 2, 2, mesh.shape["tp"]), (*SP, TP))
    heads = P(None, SP, "tp")
    return jax.shard_map(
        on_device,
        mesh=split,
        in_specs=(
            P(SP, None),
            heads,
            heads,
            heads,
            heads,
            heads,
            heads,
            heads,
            P(None, TP),
            P(None, TP),
            P(None, TP, None),
            P(),
            P(SP, TP),
            P(SP, TP),
            P(TP, SP),
        ),
        out_specs=P(SP, TP),
        check_vma=False,
    )
```

```python
import jax
import jax.numpy as jnp
from jax import lax
from jax.experimental import pallas as pl
from jax.experimental.pallas import tpu as pltpu
from jax.sharding import Mesh
from jax.sharding import PartitionSpec as P

PLANE, FAR, NEAR, CORE, TP = "plane", "far", "near", "core", "tp"
SP = (PLANE, FAR, NEAR, CORE)
ROW = (FAR, NEAR, CORE)
GATHER = (PLANE, NEAR, CORE)
POOL = (FAR, TP)
TOK = 128
LANES = 128
HALF = 64
SHARES = 8

norm_epsilon = 1e-06
head_epsilon = 0.00064
key_epsilon = 1e-06

f32 = jnp.float32
bf16 = jnp.bfloat16


def dot_nn(a, b):
    return lax.dot_general(a, b, (((1,), (0,)), ((), ())), preferred_element_type=f32)


def dot_nt(a, b):
    return lax.dot_general(a, b, (((1,), (1,)), ((), ())), preferred_element_type=f32)


def dot_tn(a, b):
    return lax.dot_general(a, b, (((0,), (0,)), ((), ())), preferred_element_type=f32)


def halves(a):
    high = a.astype(bf16)
    return high, (a - high.astype(f32)).astype(bf16)


def mm(a, b):
    ah, al = a
    bh, bl = b
    return dot_nn(jnp.concatenate([ah, al], 1), jnp.concatenate([bh, bh], 0)) + dot_nn(ah, bl)


def mm_nt(a, b):
    ah, al = a
    bh, bl = b
    return dot_nt(jnp.concatenate([ah, al], 1), jnp.concatenate([bh, bh], 1)) + dot_nt(ah, bl)


def head_masks(group):
    lane = lax.broadcasted_iota(jnp.int32, (1, LANES), 1)
    if group == 0:
        return [(lane < HALF).astype(f32), (lane >= HALF).astype(f32)]
    return [None]


def head_sum(a, masks):
    if masks[0] is None:
        return jnp.sum(a, axis=1, keepdims=True)
    return sum(jnp.sum(a * m, axis=1, keepdims=True) * m for m in masks)


def masked(a, mask):
    return a if mask is None else a * mask


def fetch(sources, targets, sems):
    copies = [pltpu.make_async_copy(a, b, sems.at[k]) for k, (a, b) in enumerate(zip(sources, targets))]
    for copy in copies:
        copy.start()
    return copies


def slot_lanes(slot):
    cut = (slot % 2) * LANES
    return slot // 2, slice(cut, cut + LANES)


def group_copies(inputs, scratch, sems):
    copies = [
        [
            pltpu.make_async_copy(a.at[group], b.at[group], sems.at[k, group])
            for k, (a, b) in enumerate(zip(inputs, scratch))
        ]
        for group in range(2)
    ]
    for copy in copies[0] + copies[1]:
        copy.start()
    return copies


def writer(results, outputs, sems):
    pending = []

    def put(which, index, count):
        part = pl.ds(index * count, count)
        copy = pltpu.make_async_copy(
            results[which].at[part], outputs[which].at[part], sems.at[which, index]
        )
        copy.start()
        pending.append(copy)

    def finish():
        for copy in pending:
            copy.wait()

    return put, finish


def solve_kernel(*refs):
    inputs, outputs, scratch, results = refs[:6], refs[6:11], refs[11:17], refs[17:22]
    sems, out_sems = refs[22:]
    send_ref, qr_ref, qk_ref, solved_ref, grown_ref = results
    q_ref, k_ref, v_ref, f_ref, l_ref, e_ref = scratch
    copies = group_copies(inputs, scratch, sems)
    put, finish = writer(results, outputs, out_sems)
    row = lax.broadcasted_iota(jnp.int32, (TOK, TOK), 0)
    col = lax.broadcasted_iota(jnp.int32, (TOK, TOK), 1)
    strict = row > col
    inclusive = row >= col
    eye = (row == col).astype(f32)
    ones = inclusive.astype(bf16)
    slots = []
    heads = []
    for slot in range(4):
        group, lanes = slot_lanes(slot)
        if slot % 2 == 0:
            for copy in copies[group]:
                copy.wait()
        q = q_ref[group, :, lanes].astype(f32)
        k = k_ref[group, :, lanes].astype(f32)
        fade = f_ref[group, :, lanes].astype(f32)
        speed = l_ref[group, :, lanes].astype(f32)
        log_decay = e_ref[group, :, lanes] - jnp.exp(-0.5) / (1.0 + jnp.exp(-fade))
        learn = 1.0 / (1.0 + jnp.exp(-speed))
        masks = head_masks(group)
        removal = k * lax.rsqrt(head_sum(k * k, masks) + key_epsilon)
        d0 = log_decay.astype(bf16)
        rest = log_decay - d0.astype(f32)
        d1 = rest.astype(bf16)
        d2 = (rest - d1.astype(f32)).astype(bf16)
        cum = dot_nn(ones, d0) + dot_nn(ones, d1) + dot_nn(ones, d2)
        middle = cum[TOK // 2 : TOK // 2 + 1, :]
        forward = jnp.exp(cum - middle)
        backward = jnp.exp(middle - cum)
        undo = jnp.exp(-log_decay)
        right = learn * removal
        removers = -removal * undo * forward
        queries = q * forward
        sources = halves(jnp.concatenate([right * backward, k * backward], 0))
        final = cum[TOK - 1 : TOK, :]
        tail = jnp.exp(final - cum)
        grown_ref[slot] = q * jnp.exp(cum)
        put(4, slot, 1)
        slots.append(
            dict(
                masks=masks,
                v=v_ref[group, :, lanes],
                start=-removal * jnp.exp(cum - log_decay),
                ends=jnp.concatenate([right * tail, k * tail], 0).astype(bf16),
                kept=jnp.exp(final),
            )
        )
        for mask in masks:
            pairs = mm_nt(halves(masked(removers, mask)), sources)
            reads = dot_nt(masked(queries, mask).astype(bf16), sources[0])
            head = len(heads)
            qr_ref[head] = jnp.where(inclusive, reads[:, :TOK], 0.0).astype(bf16)
            qk_ref[head] = jnp.where(inclusive, reads[:, TOK:], 0.0).astype(bf16)
            put(1, head, 1)
            put(2, head, 1)
            heads.append(
                dict(
                    slot=slot,
                    mask=mask,
                    n=jnp.where(strict, pairs[:, :TOK], 0.0),
                    rk=jnp.where(strict, pairs[:, TOK:], 0.0),
                )
            )
    same = (row // 8) == (col // 8)
    for head in heads:
        head["m"] = jnp.where(same, head["n"], 0.0)
        head["x"] = eye + head["m"]
    for _ in range(2):
        for head in heads:
            m = halves(head["m"])
            head["m"] = mm(m, m)
        for head in heads:
            head["x"] = head["x"] + mm(halves(head["x"]), halves(head["m"]))
    size = 8
    while size < TOK:
        below = (row // (2 * size) == col // (2 * size)) & (row // size != col // size)
        for head in heads:
            off = halves(jnp.where(below, head["n"], 0.0))
            head["y"] = halves(mm(off, halves(head["x"])))
        for head in heads:
            head["x"] = head["x"] + mm(halves(head["x"]), head["y"])
        size *= 2
    for head in heads:
        part = slots[head["slot"]]
        high, low = halves(head["rk"])
        v = part["v"]
        pulled = dot_nn(jnp.concatenate([high, low], 1), jnp.concatenate([v, v], 0))
        target = jnp.concatenate([pulled, part["start"]], 1).astype(bf16)
        head["solved"] = dot_nn(
            jnp.concatenate(halves(head["x"]), 1), jnp.concatenate([target, target], 0)
        )
    for slot, part in enumerate(slots):
        mine = [head for head in heads if head["slot"] == slot]
        solved = mine[0]["solved"]
        if len(mine) == 2:
            first = jnp.concatenate([mine[0]["mask"]] * 2, 1) > 0.5
            solved = jnp.where(first, solved, mine[1]["solved"])
        solved = solved.astype(bf16)
        solved_ref[slot] = solved
        put(3, slot, 1)
        carried, start = solved[:, :LANES], solved[:, LANES:]
        transit = dot_tn(start, part["ends"][:TOK])
        added = dot_tn(jnp.concatenate([carried, part["v"]], 0), part["ends"])
        if len(mine) == 2:
            block = (row // HALF) == (col // HALF)
            transit = jnp.where(block, transit, 0.0)
            added = jnp.where(block, added, 0.0)
        transit = (transit + eye * part["kept"]).astype(bf16)
        added = added.astype(bf16)
        for half in range(2):
            send_ref[2 * slot + half, :LANES, :] = transit
            send_ref[2 * slot + half, LANES:, :] = added[half * HALF : (half + 1) * HALF, :]
        put(0, slot, 2)
    finish()


def read_kernel(*refs):
    inputs, outputs, scratch, results = refs[:10], refs[10:14], refs[14:24], refs[24:28]
    sems, out_sems = refs[28:]
    qr_ref, qk_ref, solved_ref, grown_ref, q_ref, k_ref, v_ref, gate_ref, gain_ref, own_ref = scratch
    out_ref, read_ref, scale_ref, extra_ref = results
    for copy in fetch(inputs, scratch, sems):
        copy.wait()
    put, finish = writer(results, outputs, out_sems)
    head = 0
    for slot in range(4):
        group, lanes = slot_lanes(slot)
        masks = head_masks(group)
        v = v_ref[group, :, lanes]
        found = local = None
        for mask in masks:
            one = dot_nn(qr_ref[head], solved_ref[slot])
            here = one[:, :LANES] + dot_nn(qk_ref[head], v)
            if found is None:
                found, local = one[:, LANES:], here
            else:
                found = jnp.where(mask > 0.5, one[:, LANES:], found)
                local = jnp.where(mask > 0.5, here, local)
            head += 1
        out_ref[slot] = local
        high, low = halves(grown_ref[slot] + found)
        read_ref[slot, :, :LANES] = high
        read_ref[slot, :, LANES:] = low
        gate = gate_ref[group, :, lanes].astype(f32)
        scale_ref[slot] = gain_ref[group : group + 1, lanes] * gate
        q = q_ref[group, :, lanes].astype(f32)
        k = k_ref[group, :, lanes].astype(f32)
        own = head_sum(q * k * own_ref[group : group + 1, lanes], masks)
        extra_ref[slot] = own * v.astype(f32) * gate
        for which in range(4):
            put(which, slot, 1)
    finish()


def row_kernel(got_ref, prefix_ref, total_ref):
    row = lax.broadcasted_iota(jnp.int32, (LANES + HALF, LANES), 0)
    col = lax.broadcasted_iota(jnp.int32, (LANES + HALF, LANES), 1)
    zero = jnp.zeros((LANES, LANES), f32)
    prefix_ref[0] = (row == col).astype(f32)
    run = got_ref[0].astype(f32)
    for k in range(1, SHARES):
        prefix_ref[k] = run
        got = got_ref[k]
        step = got[:LANES]
        high, low = halves(run)
        run = dot_nn(jnp.concatenate([high, low], 1), jnp.concatenate([step, step], 0))
        run = run + jnp.concatenate([zero, got[LANES:].astype(f32)], 0)
    total = run.astype(bf16)
    for k in range(total_ref.shape[0]):
        total_ref[k] = total


def state_kernel(place_ref, every_ref, prefix_ref, send_ref):
    place = place_ref[0]
    state = jnp.zeros((HALF, LANES), f32)
    for k in range(every_ref.shape[0] - 1):
        got = every_ref[k]
        step = got[:LANES]
        high, low = halves(state)
        grown = dot_nn(jnp.concatenate([high, low], 1), jnp.concatenate([step, step], 0))
        state = jnp.where(k < place, grown + got[LANES:].astype(f32), state)
    split = halves(state)
    for k in range(SHARES):
        moved = mm(split, halves(prefix_ref[k, :LANES, :]))
        send_ref[k] = (moved + prefix_ref[k, LANES:, :]).astype(bf16)


def mix_kernel(*refs):
    inputs, outputs, scratch, results, sems, out_sems = (
        refs[:6],
        refs[6:7],
        refs[7:13],
        refs[13:14],
        refs[14],
        refs[15],
    )
    state_ref, out_ref, read_ref, scale_ref, extra_ref, w_ref = scratch
    copies = fetch(inputs, scratch, sems)
    put, finish = writer(results, outputs, out_sems)
    for copy in copies[:5]:
        copy.wait()
    mixed = []
    for slot in range(4):
        width = HALF if slot < 2 else LANES
        masks = head_masks(slot // 2)
        state = jnp.concatenate([state_ref[2 * slot], state_ref[2 * slot + 1]], 0)
        raw = out_ref[slot] + dot_nt(read_ref[slot], jnp.concatenate([state, state], 1))
        centered = raw - head_sum(raw, masks) * (1.0 / width)
        variance = head_sum(centered * centered, masks) * (1.0 / width)
        normed = centered * lax.rsqrt(variance + head_epsilon) * scale_ref[slot]
        mixed.append((normed + extra_ref[slot]).astype(bf16))
    mixed = jnp.concatenate(mixed, 1)
    copies[5].wait()
    tiles, _, columns = results[0].shape
    for k in range(tiles):
        results[0][k] = dot_nn(mixed, w_ref[:, k * columns : (k + 1) * columns]).astype(bf16)
        put(0, k, 1)
    finish()


AHEAD = 4


def feed_kernel(
    far_ref,
    state_ref,
    gain_in_ref,
    whole_ref,
    sent_ref,
    w_ref,
    n_ref,
    acc_ref,
    x_ref,
    gain_ref,
    y_ref,
    sems,
    in_sems,
    out_sems,
):
    tokens_here = fetch([state_ref, gain_in_ref], [x_ref, gain_ref], in_sems)
    put, finish = writer([y_ref], [sent_ref], out_sems)
    planes, sides, near, rows, width = w_ref.shape
    third = width // 3
    far = far_ref[0]
    copies = [
        [
            pltpu.make_async_copy(
                whole_ref.at[k, :, jnp.where(far == side, 0, 1)],
                w_ref.at[k, side],
                sems.at[k, side],
            )
            for side in range(sides)
        ]
        for k in range(planes)
    ]
    for k in range(AHEAD):
        for copy in copies[k]:
            copy.start()
    shares, tokens, columns = x_ref.shape
    tiles = shares // sides
    for copy in tokens_here:
        copy.wait()
    for side in range(sides):
        parts = [x_ref[side * tiles + k].astype(f32) for k in range(tiles)]
        total = sum(jnp.sum(a * a, axis=1, keepdims=True) for a in parts)
        scale = lax.rsqrt(total * (1.0 / (tiles * columns)) + norm_epsilon)
        for k, a in enumerate(parts):
            lanes = slice(k * columns, (k + 1) * columns)
            n_ref[side * tokens : (side + 1) * tokens, lanes] = (
                a * scale * gain_ref[:, lanes]
            ).astype(bf16)
    block = sides * near * rows
    for k in range(0, planes, 2):
        for step in (k, k + 1):
            for copy in copies[step]:
                copy.wait()
            if step + AHEAD < planes:
                for copy in copies[step + AHEAD]:
                    copy.start()
        part = dot_nn(
            n_ref[:, k * block : (k + 2) * block],
            w_ref[k : k + 2, :, :, :, : 2 * third].reshape(2 * block, 2 * third),
        )
        if k == 0:
            acc_ref[...] = part
        else:
            acc_ref[...] += part
    gate = acc_ref[:, :third]
    active = (gate / (1.0 + jnp.exp(-gate)) * acc_ref[:, third:]).astype(bf16)
    per = planes // tiles
    for k in range(tiles):
        down = w_ref[k * per : (k + 1) * per, :, :, :, 2 * third :].reshape(per * block, third)
        out = dot_nt(active, down).astype(bf16)
        for side in range(sides):
            y_ref[side * tiles + k] = out[side * tokens : (side + 1) * tokens]
            put(0, side * tiles + k, 1)
    finish()


def feed_forward(far, state, gain, whole):
    planes, near, sides, rows, width = whole.shape
    shares, tokens, columns = state.shape
    return pl.pallas_call(
        feed_kernel,
        out_shape=array((shares, tokens, columns), bf16),
        in_specs=[SMEM, HBM, HBM, HBM],
        out_specs=HBM,
        scratch_shapes=[
            pltpu.VMEM((planes, sides, near, rows, width), bf16),
            pltpu.VMEM((sides * tokens, gain.shape[1]), bf16),
            pltpu.VMEM((sides * tokens, 2 * width // 3), f32),
            pltpu.VMEM(state.shape, bf16),
            pltpu.VMEM(gain.shape, f32),
            pltpu.VMEM(state.shape, bf16),
            pltpu.SemaphoreType.DMA((planes, sides)),
            pltpu.SemaphoreType.DMA((2,)),
            pltpu.SemaphoreType.DMA((1, shares)),
        ],
        compiler_params=pltpu.CompilerParams(vmem_limit_bytes=55_000_000),
    )(far, state, gain, whole)


def pack_kernel(far_ref, *refs):
    inputs, (kept_ref, given_ref), scratch, sems = refs[:3], refs[3:5], refs[5:8], refs[8]
    copies = fetch(inputs, scratch, sems)
    wide = kept_ref.shape[1] // 3
    first = far_ref[0] == 0
    for k, copy in enumerate(copies):
        copy.wait()
        lanes = slice(k * wide, (k + 1) * wide)
        kept_ref[given_ref.shape[0] :, lanes] = jnp.zeros((given_ref.shape[0], wide), bf16)
        near = scratch[k][:, :wide]
        rest = scratch[k][:, wide:]
        blank = jnp.zeros((rest.shape[0], 2 * wide - scratch[k].shape[1]), bf16)
        far = jnp.concatenate([rest, blank], axis=1)
        kept_ref[: near.shape[0], lanes] = jnp.where(first, near, far)
        given_ref[:, lanes] = jnp.where(first, far, near)


def swapped(far, parts):
    rows, hidden = parts[0].shape
    wide = -(-hidden // (2 * LANES)) * LANES
    packed = (array((2 * rows, 3 * wide), bf16), array((rows, 3 * wide), bf16))
    kept, given = call(pack_kernel, packed, [SMEM] + [HBM] * 3, parts, 62_000_000)(far, *parts)
    return kept, lax.ppermute(given, FAR, [(0, 1), (1, 0)])


def gathered(kept, taken):
    rows, width = taken.shape
    both = lax.dynamic_update_slice(kept, taken, (rows, 0))
    whole = lax.all_gather(both, GATHER, axis=0, tiled=True)
    planes = lax.axis_size(PLANE)
    near = lax.axis_size(NEAR) * lax.axis_size(CORE)
    return whole.reshape(planes, near, 2, rows, width)


VMEM = pl.BlockSpec(memory_space=pltpu.VMEM)
HBM = pl.BlockSpec(memory_space=pltpu.HBM)
SMEM = pl.BlockSpec(memory_space=pltpu.SMEM)


def call(kernel, outs, specs, fetched=(), limit=24 * 1024 * 1024, written=0, sems=()):
    scratch = [pltpu.VMEM(a.shape, a.dtype) for a in fetched]
    where = VMEM
    if written:
        where = HBM
        scratch += [pltpu.VMEM(a.shape, a.dtype) for a in outs]
    scratch += [pltpu.SemaphoreType.DMA(a) for a in sems or [(len(fetched),)] if fetched]
    if written:
        scratch.append(pltpu.SemaphoreType.DMA((len(outs), written)))
    return pl.pallas_call(
        kernel,
        out_shape=outs,
        in_specs=specs,
        out_specs=jax.tree.map(lambda _: where, outs),
        scratch_shapes=scratch,
        compiler_params=pltpu.CompilerParams(vmem_limit_bytes=limit),
    )


def array(dims, kind):
    return jax.ShapeDtypeStruct(dims, kind)


def exchange(value, axis):
    return lax.all_to_all(value, axis, 0, 0, tiled=True)


def from_everyone(value, axis):
    devices = lax.psum(1, axis)
    return exchange(jnp.broadcast_to(value[None], (devices, *value.shape)), axis)


def on_device(
    stratum_source_matrix,
    acceptance_query,
    cluster_lookup_matrix,
    cluster_payload_matrix,
    fading_logit,
    adaptation_speed_logit,
    additional_fading_exponent,
    result_switch_pair,
    attender_scaling_factor,
    present_item_factor,
    final_mapping_matrix,
    perceptron_scaling_factor,
    switching_matrix,
    widening_matrix,
    shrinking_matrix,
):
    features = perceptron_scaling_factor.shape[0]
    columns = features // lax.axis_size(TP)
    far = lax.axis_index(FAR).astype(jnp.int32).reshape(1)
    kept, taken = swapped(far, [switching_matrix, widening_matrix, shrinking_matrix.T])
    blocks = array((4, TOK, LANES), f32)
    pairs = array((6, TOK, TOK), bf16)
    doubled = array((4, TOK, 2 * LANES), bf16)
    inputs = (
        acceptance_query,
        cluster_lookup_matrix,
        cluster_payload_matrix,
        fading_logit,
        adaptation_speed_logit,
        additional_fading_exponent,
    )
    send, *found = call(
        solve_kernel,
        (array((SHARES, LANES + HALF, LANES), bf16), pairs, pairs, doubled, blocks),
        [HBM] * len(inputs),
        inputs,
        66_400_000,
        6,
        [(len(inputs), 2)],
    )(*inputs)
    place = lax.axis_index(PLANE).astype(jnp.int32).reshape(1)
    first_column = (lax.axis_index(TP) * columns).astype(jnp.uint32)
    send, taken, place, first_column = lax.optimization_barrier((send, taken, place, first_column))
    whole = gathered(kept, taken)
    planes = lax.axis_size(PLANE)
    prefix, total = call(
        row_kernel,
        (
            array((SHARES, LANES + HALF, LANES), f32),
            array((planes, LANES + HALF, LANES), bf16),
        ),
        [VMEM],
    )(exchange(send, ROW))
    total, *found = lax.optimization_barrier((total, *found))
    reading = (
        *found,
        *inputs[:3],
        result_switch_pair,
        attender_scaling_factor,
        present_item_factor,
    )
    read = call(
        read_kernel,
        (blocks, doubled, blocks, blocks),
        [HBM] * len(reading),
        reading,
        65300000,
        4,
    )(*reading)
    every, *read = lax.optimization_barrier((exchange(total, PLANE), *read))
    states = call(state_kernel, array((SHARES, HALF, LANES), bf16), [SMEM, VMEM, VMEM])(
        place, every, prefix
    )
    mixing = (exchange(states, ROW), *read, final_mapping_matrix.reshape(-1, features))
    (terms,) = call(
        mix_kernel,
        (array((features // columns, TOK, columns), bf16),),
        [HBM] * len(mixing),
        mixing,
        64_000_000,
        features // columns,
    )(*mixing)
    residual = lax.dynamic_slice(
        stratum_source_matrix, (jnp.uint32(0), first_column), (TOK, columns)
    )
    attention = jnp.sum(exchange(terms, TP).astype(f32), axis=0)
    own_state = (residual.astype(f32) + attention).astype(bf16)
    tiles = feed_forward(
        far,
        from_everyone(own_state, POOL),
        perceptron_scaling_factor.reshape(1, features),
        whole,
    )
    mixer = jnp.sum(exchange(tiles, POOL).astype(f32), axis=0)
    return (own_state.astype(f32) + mixer).astype(bf16)


def solution(mesh):
    split = Mesh(mesh.devices.reshape(8, 2, 2, 2, mesh.shape["tp"]), (*SP, TP))
    heads = P(None, SP, "tp")
    return jax.shard_map(
        on_device,
        mesh=split,
        in_specs=(
            P(SP, None),
            heads,
            heads,
            heads,
            heads,
            heads,
            heads,
            heads,
            P(None, TP),
            P(None, TP),
            P(None, TP, None),
            P(),
            P(SP, TP),
            P(SP, TP),
            P(TP, SP),
        ),
        out_specs=P(SP, TP),
        check_vma=False,
    )
```

```python
import jax
import jax.numpy as jnp
from jax import lax
from jax.experimental import pallas as pl
from jax.experimental.pallas import tpu as pltpu
from jax.sharding import Mesh
from jax.sharding import PartitionSpec as P

PLANE, FAR, NEAR, CORE, TP = "plane", "far", "near", "core", "tp"
SP = (PLANE, FAR, NEAR, CORE)
ROW = (FAR, NEAR, CORE)
GATHER = (PLANE, NEAR, CORE)
POOL = (FAR, TP)
TOK = 128
LANES = 128
HALF = 64
SHARES = 8

norm_epsilon = 1e-06
head_epsilon = 0.00064
key_epsilon = 1e-06

f32 = jnp.float32
bf16 = jnp.bfloat16


def dot_nn(a, b):
    return lax.dot_general(a, b, (((1,), (0,)), ((), ())), preferred_element_type=f32)


def dot_nt(a, b):
    return lax.dot_general(a, b, (((1,), (1,)), ((), ())), preferred_element_type=f32)


def dot_tn(a, b):
    return lax.dot_general(a, b, (((0,), (0,)), ((), ())), preferred_element_type=f32)


def halves(a):
    high = a.astype(bf16)
    return high, (a - high.astype(f32)).astype(bf16)


def mm(a, b):
    ah, al = a
    bh, bl = b
    return dot_nn(jnp.concatenate([ah, al], 1), jnp.concatenate([bh, bh], 0)) + dot_nn(ah, bl)


def mm_nt(a, b):
    ah, al = a
    bh, bl = b
    return dot_nt(jnp.concatenate([ah, al], 1), jnp.concatenate([bh, bh], 1)) + dot_nt(ah, bl)


def head_masks(group):
    lane = lax.broadcasted_iota(jnp.int32, (1, LANES), 1)
    if group == 0:
        return [(lane < HALF).astype(f32), (lane >= HALF).astype(f32)]
    return [None]


def head_sum(a, masks):
    if masks[0] is None:
        return jnp.sum(a, axis=1, keepdims=True)
    return sum(jnp.sum(a * m, axis=1, keepdims=True) * m for m in masks)


def masked(a, mask):
    return a if mask is None else a * mask


def fetch(sources, targets, sems):
    copies = [pltpu.make_async_copy(a, b, sems.at[k]) for k, (a, b) in enumerate(zip(sources, targets))]
    for copy in copies:
        copy.start()
    return copies


def slot_lanes(slot):
    cut = (slot % 2) * LANES
    return slot // 2, slice(cut, cut + LANES)


def group_copies(inputs, scratch, sems):
    copies = [
        [
            pltpu.make_async_copy(a.at[group], b.at[group], sems.at[k, group])
            for k, (a, b) in enumerate(zip(inputs, scratch))
        ]
        for group in range(2)
    ]
    for copy in copies[0] + copies[1]:
        copy.start()
    return copies


def writer(results, outputs, sems):
    pending = []

    def put(which, index, count):
        part = pl.ds(index * count, count)
        copy = pltpu.make_async_copy(
            results[which].at[part], outputs[which].at[part], sems.at[which, index]
        )
        copy.start()
        pending.append(copy)

    def finish():
        for copy in pending:
            copy.wait()

    return put, finish


def solve_kernel(*refs):
    inputs, outputs, scratch, results = refs[:6], refs[6:11], refs[11:17], refs[17:22]
    sems, out_sems = refs[22:]
    send_ref, qr_ref, qk_ref, solved_ref, grown_ref = results
    q_ref, k_ref, v_ref, f_ref, l_ref, e_ref = scratch
    copies = group_copies(inputs, scratch, sems)
    put, finish = writer(results, outputs, out_sems)
    row = lax.broadcasted_iota(jnp.int32, (TOK, TOK), 0)
    col = lax.broadcasted_iota(jnp.int32, (TOK, TOK), 1)
    strict = row > col
    inclusive = row >= col
    eye = (row == col).astype(f32)
    ones = inclusive.astype(bf16)
    slots = []
    heads = []
    for slot in range(4):
        group, lanes = slot_lanes(slot)
        if slot % 2 == 0:
            for copy in copies[group]:
                copy.wait()
        q = q_ref[group, :, lanes].astype(f32)
        k = k_ref[group, :, lanes].astype(f32)
        fade = f_ref[group, :, lanes].astype(f32)
        speed = l_ref[group, :, lanes].astype(f32)
        log_decay = e_ref[group, :, lanes] - jnp.exp(-0.5) / (1.0 + jnp.exp(-fade))
        learn = 1.0 / (1.0 + jnp.exp(-speed))
        masks = head_masks(group)
        removal = k * lax.rsqrt(head_sum(k * k, masks) + key_epsilon)
        d0 = log_decay.astype(bf16)
        rest = log_decay - d0.astype(f32)
        d1 = rest.astype(bf16)
        d2 = (rest - d1.astype(f32)).astype(bf16)
        cum = dot_nn(ones, d0) + dot_nn(ones, d1) + dot_nn(ones, d2)
        middle = cum[TOK // 2 : TOK // 2 + 1, :]
        forward = jnp.exp(cum - middle)
        backward = jnp.exp(middle - cum)
        undo = jnp.exp(-log_decay)
        right = learn * removal
        removers = -removal * undo * forward
        queries = q * forward
        sources = halves(jnp.concatenate([right * backward, k * backward], 0))
        final = cum[TOK - 1 : TOK, :]
        tail = jnp.exp(final - cum)
        grown_ref[slot] = q * jnp.exp(cum)
        put(4, slot, 1)
        slots.append(
            dict(
                masks=masks,
                v=v_ref[group, :, lanes],
                start=-removal * jnp.exp(cum - log_decay),
                ends=jnp.concatenate([right * tail, k * tail], 0).astype(bf16),
                kept=jnp.exp(final),
            )
        )
        for mask in masks:
            pairs = mm_nt(halves(masked(removers, mask)), sources)
            reads = dot_nt(masked(queries, mask).astype(bf16), sources[0])
            head = len(heads)
            qr_ref[head] = jnp.where(inclusive, reads[:, :TOK], 0.0).astype(bf16)
            qk_ref[head] = jnp.where(inclusive, reads[:, TOK:], 0.0).astype(bf16)
            put(1, head, 1)
            put(2, head, 1)
            heads.append(
                dict(
                    slot=slot,
                    mask=mask,
                    n=jnp.where(strict, pairs[:, :TOK], 0.0),
                    rk=jnp.where(strict, pairs[:, TOK:], 0.0),
                )
            )
    same = (row // 8) == (col // 8)
    for head in heads:
        head["m"] = jnp.where(same, head["n"], 0.0)
        head["x"] = eye + head["m"]
    for _ in range(2):
        for head in heads:
            m = halves(head["m"])
            head["m"] = mm(m, m)
        for head in heads:
            head["x"] = head["x"] + mm(halves(head["x"]), halves(head["m"]))
    size = 8
    while size < TOK:
        below = (row // (2 * size) == col // (2 * size)) & (row // size != col // size)
        for head in heads:
            off = halves(jnp.where(below, head["n"], 0.0))
            head["y"] = halves(mm(off, halves(head["x"])))
        for head in heads:
            head["x"] = head["x"] + mm(halves(head["x"]), head["y"])
        size *= 2
    for head in heads:
        part = slots[head["slot"]]
        high, low = halves(head["rk"])
        v = part["v"]
        pulled = dot_nn(jnp.concatenate([high, low], 1), jnp.concatenate([v, v], 0))
        target = jnp.concatenate([pulled, part["start"]], 1).astype(bf16)
        head["solved"] = dot_nn(
            jnp.concatenate(halves(head["x"]), 1), jnp.concatenate([target, target], 0)
        )
    for slot, part in enumerate(slots):
        mine = [head for head in heads if head["slot"] == slot]
        solved = mine[0]["solved"]
        if len(mine) == 2:
            first = jnp.concatenate([mine[0]["mask"]] * 2, 1) > 0.5
            solved = jnp.where(first, solved, mine[1]["solved"])
        solved = solved.astype(bf16)
        solved_ref[slot] = solved
        put(3, slot, 1)
        carried, start = solved[:, :LANES], solved[:, LANES:]
        transit = dot_tn(start, part["ends"][:TOK])
        added = dot_tn(jnp.concatenate([carried, part["v"]], 0), part["ends"])
        if len(mine) == 2:
            block = (row // HALF) == (col // HALF)
            transit = jnp.where(block, transit, 0.0)
            added = jnp.where(block, added, 0.0)
        transit = (transit + eye * part["kept"]).astype(bf16)
        added = added.astype(bf16)
        for half in range(2):
            send_ref[2 * slot + half, :LANES, :] = transit
            send_ref[2 * slot + half, LANES:, :] = added[half * HALF : (half + 1) * HALF, :]
        put(0, slot, 2)
    finish()


def read_kernel(*refs):
    inputs, outputs, scratch, results = refs[:10], refs[10:14], refs[14:24], refs[24:28]
    sems, out_sems = refs[28:]
    qr_ref, qk_ref, solved_ref, grown_ref, q_ref, k_ref, v_ref, gate_ref, gain_ref, own_ref = scratch
    out_ref, read_ref, scale_ref, extra_ref = results
    for copy in fetch(inputs, scratch, sems):
        copy.wait()
    put, finish = writer(results, outputs, out_sems)
    head = 0
    for slot in range(4):
        group, lanes = slot_lanes(slot)
        masks = head_masks(group)
        v = v_ref[group, :, lanes]
        found = local = None
        for mask in masks:
            one = dot_nn(qr_ref[head], solved_ref[slot])
            here = one[:, :LANES] + dot_nn(qk_ref[head], v)
            if found is None:
                found, local = one[:, LANES:], here
            else:
                found = jnp.where(mask > 0.5, one[:, LANES:], found)
                local = jnp.where(mask > 0.5, here, local)
            head += 1
        out_ref[slot] = local
        high, low = halves(grown_ref[slot] + found)
        read_ref[slot, :, :LANES] = high
        read_ref[slot, :, LANES:] = low
        gate = gate_ref[group, :, lanes].astype(f32)
        scale_ref[slot] = gain_ref[group : group + 1, lanes] * gate
        q = q_ref[group, :, lanes].astype(f32)
        k = k_ref[group, :, lanes].astype(f32)
        own = head_sum(q * k * own_ref[group : group + 1, lanes], masks)
        extra_ref[slot] = own * v.astype(f32) * gate
        for which in range(4):
            put(which, slot, 1)
    finish()


def row_kernel(got_ref, prefix_ref, total_ref):
    row = lax.broadcasted_iota(jnp.int32, (LANES + HALF, LANES), 0)
    col = lax.broadcasted_iota(jnp.int32, (LANES + HALF, LANES), 1)
    zero = jnp.zeros((LANES, LANES), f32)
    prefix_ref[0] = (row == col).astype(f32)
    run = got_ref[0].astype(f32)
    for k in range(1, SHARES):
        prefix_ref[k] = run
        got = got_ref[k]
        step = got[:LANES]
        high, low = halves(run)
        run = dot_nn(jnp.concatenate([high, low], 1), jnp.concatenate([step, step], 0))
        run = run + jnp.concatenate([zero, got[LANES:].astype(f32)], 0)
    total = run.astype(bf16)
    for k in range(total_ref.shape[0]):
        total_ref[k] = total


def state_kernel(place_ref, every_ref, prefix_ref, send_ref):
    place = place_ref[0]
    state = jnp.zeros((HALF, LANES), f32)
    for k in range(every_ref.shape[0] - 1):
        got = every_ref[k]
        step = got[:LANES]
        high, low = halves(state)
        grown = dot_nn(jnp.concatenate([high, low], 1), jnp.concatenate([step, step], 0))
        state = jnp.where(k < place, grown + got[LANES:].astype(f32), state)
    split = halves(state)
    for k in range(SHARES):
        moved = mm(split, halves(prefix_ref[k, :LANES, :]))
        send_ref[k] = (moved + prefix_ref[k, LANES:, :]).astype(bf16)


def mix_kernel(*refs):
    inputs, outputs, scratch, results, sems, out_sems = (
        refs[:6],
        refs[6:7],
        refs[7:13],
        refs[13:14],
        refs[14],
        refs[15],
    )
    state_ref, out_ref, read_ref, scale_ref, extra_ref, w_ref = scratch
    copies = fetch(inputs, scratch, sems)
    put, finish = writer(results, outputs, out_sems)
    for copy in copies[:5]:
        copy.wait()
    mixed = []
    for slot in range(4):
        width = HALF if slot < 2 else LANES
        masks = head_masks(slot // 2)
        state = jnp.concatenate([state_ref[2 * slot], state_ref[2 * slot + 1]], 0)
        raw = out_ref[slot] + dot_nt(read_ref[slot], jnp.concatenate([state, state], 1))
        centered = raw - head_sum(raw, masks) * (1.0 / width)
        variance = head_sum(centered * centered, masks) * (1.0 / width)
        normed = centered * lax.rsqrt(variance + head_epsilon) * scale_ref[slot]
        mixed.append((normed + extra_ref[slot]).astype(bf16))
    mixed = jnp.concatenate(mixed, 1)
    copies[5].wait()
    tiles, _, columns = results[0].shape
    for k in range(tiles):
        results[0][k] = dot_nn(mixed, w_ref[:, k * columns : (k + 1) * columns]).astype(bf16)
        put(0, k, 1)
    finish()


AHEAD = 4


def feed_kernel(
    far_ref,
    state_ref,
    gain_in_ref,
    whole_ref,
    sent_ref,
    w_ref,
    n_ref,
    acc_ref,
    x_ref,
    gain_ref,
    y_ref,
    sems,
    in_sems,
    out_sems,
):
    tokens_here = fetch([state_ref, gain_in_ref], [x_ref, gain_ref], in_sems)
    put, finish = writer([y_ref], [sent_ref], out_sems)
    planes, sides, near, rows, width = w_ref.shape
    third = width // 3
    far = far_ref[0]
    copies = [
        [
            pltpu.make_async_copy(
                whole_ref.at[k, :, jnp.where(far == side, 0, 1)],
                w_ref.at[k, side],
                sems.at[k, side],
            )
            for side in range(sides)
        ]
        for k in range(planes)
    ]
    for k in range(AHEAD):
        for copy in copies[k]:
            copy.start()
    shares, tokens, columns = x_ref.shape
    tiles = shares // sides
    for copy in tokens_here:
        copy.wait()
    scales = []
    for side in range(sides):
        total = 0.0
        for k in range(tiles):
            lanes = slice(k * columns, (k + 1) * columns)
            a = x_ref[side * tiles + k].astype(f32)
            n_ref[side * tokens : (side + 1) * tokens, lanes] = (a * gain_ref[:, lanes]).astype(
                bf16
            )
            total = total + jnp.sum(a * a, axis=1, keepdims=True)
        scales.append(lax.rsqrt(total * (1.0 / (tiles * columns)) + norm_epsilon))
    scale = jnp.concatenate(scales, 0)
    block = sides * near * rows
    for k in range(0, planes, 2):
        for step in (k, k + 1):
            for copy in copies[step]:
                copy.wait()
            if step + AHEAD < planes:
                for copy in copies[step + AHEAD]:
                    copy.start()
        part = dot_nn(
            n_ref[:, k * block : (k + 2) * block],
            w_ref[k : k + 2, :, :, :, : 2 * third].reshape(2 * block, 2 * third),
        )
        if k == 0:
            acc_ref[...] = part
        else:
            acc_ref[...] += part
    gate = acc_ref[:, :third] * scale
    up = acc_ref[:, third:] * scale
    active = (gate / (1.0 + jnp.exp(-gate)) * up).astype(bf16)
    per = planes // tiles
    for k in range(tiles):
        down = w_ref[k * per : (k + 1) * per, :, :, :, 2 * third :].reshape(per * block, third)
        out = dot_nt(active, down).astype(bf16)
        for side in range(sides):
            y_ref[side * tiles + k] = out[side * tokens : (side + 1) * tokens]
            put(0, side * tiles + k, 1)
    finish()


def feed_forward(far, state, gain, whole):
    planes, near, sides, rows, width = whole.shape
    shares, tokens, columns = state.shape
    return pl.pallas_call(
        feed_kernel,
        out_shape=array((shares, tokens, columns), bf16),
        in_specs=[SMEM, HBM, HBM, HBM],
        out_specs=HBM,
        scratch_shapes=[
            pltpu.VMEM((planes, sides, near, rows, width), bf16),
            pltpu.VMEM((sides * tokens, gain.shape[1]), bf16),
            pltpu.VMEM((sides * tokens, 2 * width // 3), f32),
            pltpu.VMEM(state.shape, bf16),
            pltpu.VMEM(gain.shape, f32),
            pltpu.VMEM(state.shape, bf16),
            pltpu.SemaphoreType.DMA((planes, sides)),
            pltpu.SemaphoreType.DMA((2,)),
            pltpu.SemaphoreType.DMA((1, shares)),
        ],
        compiler_params=pltpu.CompilerParams(vmem_limit_bytes=55_000_000),
    )(far, state, gain, whole)


def pack_kernel(far_ref, *refs):
    inputs, (kept_ref, given_ref), scratch, sems = refs[:3], refs[3:5], refs[5:8], refs[8]
    copies = fetch(inputs, scratch, sems)
    wide = kept_ref.shape[1] // 3
    first = far_ref[0] == 0
    for k, copy in enumerate(copies):
        copy.wait()
        lanes = slice(k * wide, (k + 1) * wide)
        kept_ref[given_ref.shape[0] :, lanes] = jnp.zeros((given_ref.shape[0], wide), bf16)
        near = scratch[k][:, :wide]
        rest = scratch[k][:, wide:]
        blank = jnp.zeros((rest.shape[0], 2 * wide - scratch[k].shape[1]), bf16)
        far = jnp.concatenate([rest, blank], axis=1)
        kept_ref[: near.shape[0], lanes] = jnp.where(first, near, far)
        given_ref[:, lanes] = jnp.where(first, far, near)


def swapped(far, parts):
    rows, hidden = parts[0].shape
    wide = -(-hidden // (2 * LANES)) * LANES
    packed = (array((2 * rows, 3 * wide), bf16), array((rows, 3 * wide), bf16))
    kept, given = call(pack_kernel, packed, [SMEM] + [HBM] * 3, parts, 62_000_000)(far, *parts)
    return kept, lax.ppermute(given, FAR, [(0, 1), (1, 0)])


def gathered(kept, taken):
    rows, width = taken.shape
    both = lax.dynamic_update_slice(kept, taken, (rows, 0))
    whole = lax.all_gather(both, GATHER, axis=0, tiled=True)
    planes = lax.axis_size(PLANE)
    near = lax.axis_size(NEAR) * lax.axis_size(CORE)
    return whole.reshape(planes, near, 2, rows, width)


VMEM = pl.BlockSpec(memory_space=pltpu.VMEM)
HBM = pl.BlockSpec(memory_space=pltpu.HBM)
SMEM = pl.BlockSpec(memory_space=pltpu.SMEM)


def call(kernel, outs, specs, fetched=(), limit=24 * 1024 * 1024, written=0, sems=()):
    scratch = [pltpu.VMEM(a.shape, a.dtype) for a in fetched]
    where = VMEM
    if written:
        where = HBM
        scratch += [pltpu.VMEM(a.shape, a.dtype) for a in outs]
    scratch += [pltpu.SemaphoreType.DMA(a) for a in sems or [(len(fetched),)] if fetched]
    if written:
        scratch.append(pltpu.SemaphoreType.DMA((len(outs), written)))
    return pl.pallas_call(
        kernel,
        out_shape=outs,
        in_specs=specs,
        out_specs=jax.tree.map(lambda _: where, outs),
        scratch_shapes=scratch,
        compiler_params=pltpu.CompilerParams(vmem_limit_bytes=limit),
    )


def array(dims, kind):
    return jax.ShapeDtypeStruct(dims, kind)


def exchange(value, axis):
    return lax.all_to_all(value, axis, 0, 0, tiled=True)


def from_everyone(value, axis):
    devices = lax.psum(1, axis)
    return exchange(jnp.broadcast_to(value[None], (devices, *value.shape)), axis)


def on_device(
    stratum_source_matrix,
    acceptance_query,
    cluster_lookup_matrix,
    cluster_payload_matrix,
    fading_logit,
    adaptation_speed_logit,
    additional_fading_exponent,
    result_switch_pair,
    attender_scaling_factor,
    present_item_factor,
    final_mapping_matrix,
    perceptron_scaling_factor,
    switching_matrix,
    widening_matrix,
    shrinking_matrix,
):
    features = perceptron_scaling_factor.shape[0]
    columns = features // lax.axis_size(TP)
    far = lax.axis_index(FAR).astype(jnp.int32).reshape(1)
    kept, taken = swapped(far, [switching_matrix, widening_matrix, shrinking_matrix.T])
    blocks = array((4, TOK, LANES), f32)
    pairs = array((6, TOK, TOK), bf16)
    doubled = array((4, TOK, 2 * LANES), bf16)
    inputs = (
        acceptance_query,
        cluster_lookup_matrix,
        cluster_payload_matrix,
        fading_logit,
        adaptation_speed_logit,
        additional_fading_exponent,
    )
    send, *found = call(
        solve_kernel,
        (array((SHARES, LANES + HALF, LANES), bf16), pairs, pairs, doubled, blocks),
        [HBM] * len(inputs),
        inputs,
        66_400_000,
        6,
        [(len(inputs), 2)],
    )(*inputs)
    place = lax.axis_index(PLANE).astype(jnp.int32).reshape(1)
    first_column = (lax.axis_index(TP) * columns).astype(jnp.uint32)
    send, taken, place, first_column = lax.optimization_barrier((send, taken, place, first_column))
    whole = gathered(kept, taken)
    planes = lax.axis_size(PLANE)
    prefix, total = call(
        row_kernel,
        (
            array((SHARES, LANES + HALF, LANES), f32),
            array((planes, LANES + HALF, LANES), bf16),
        ),
        [VMEM],
    )(exchange(send, ROW))
    total, first_column, *found = lax.optimization_barrier((total, first_column, *found))
    reading = (
        *found,
        *inputs[:3],
        result_switch_pair,
        attender_scaling_factor,
        present_item_factor,
    )
    read = call(
        read_kernel,
        (blocks, doubled, blocks, blocks),
        [HBM] * len(reading),
        reading,
        64_500_000,
        4,
    )(*reading)
    residual = lax.dynamic_slice(
        stratum_source_matrix, (jnp.uint32(0), first_column), (TOK, columns)
    )
    every, residual, *read = lax.optimization_barrier((exchange(total, PLANE), residual, *read))
    states = call(state_kernel, array((SHARES, HALF, LANES), bf16), [SMEM, VMEM, VMEM])(
        place, every, prefix
    )
    mixing = (exchange(states, ROW), *read, final_mapping_matrix.reshape(-1, features))
    (terms,) = call(
        mix_kernel,
        (array((features // columns, TOK, columns), bf16),),
        [HBM] * len(mixing),
        mixing,
        64_000_000,
        features // columns,
    )(*mixing)
    attention = jnp.sum(exchange(terms, TP).astype(f32), axis=0)
    own_state = (residual.astype(f32) + attention).astype(bf16)
    tiles = feed_forward(
        far,
        from_everyone(own_state, POOL),
        perceptron_scaling_factor.reshape(1, features),
        whole,
    )
    mixer = jnp.sum(exchange(tiles, POOL).astype(f32), axis=0)
    return (own_state.astype(f32) + mixer).astype(bf16)


def solution(mesh):
    split = Mesh(mesh.devices.reshape(8, 2, 2, 2, mesh.shape["tp"]), (*SP, TP))
    heads = P(None, SP, "tp")
    return jax.shard_map(
        on_device,
        mesh=split,
        in_specs=(
            P(SP, None),
            heads,
            heads,
            heads,
            heads,
            heads,
            heads,
            heads,
            P(None, TP),
            P(None, TP),
            P(None, TP, None),
            P(),
            P(SP, TP),
            P(SP, TP),
            P(TP, SP),
        ),
        out_specs=P(SP, TP),
        check_vma=False,
    )
```

```python
import jax
import jax.numpy as jnp
from jax import lax
from jax.experimental import pallas as pl
from jax.experimental.pallas import tpu as pltpu
from jax.sharding import Mesh
from jax.sharding import PartitionSpec as P

PLANE, FAR, NEAR, CORE, TP = "plane", "far", "near", "core", "tp"
SP = (PLANE, FAR, NEAR, CORE)
ROW = (FAR, NEAR, CORE)
GATHER = (PLANE, NEAR, CORE)
POOL = (FAR, TP)
TOK = 128
LANES = 128
HALF = 64
SHARES = 8

norm_epsilon = 1e-06
head_epsilon = 0.00064
key_epsilon = 1e-06

f32 = jnp.float32
bf16 = jnp.bfloat16


def dot_nn(a, b):
    return lax.dot_general(a, b, (((1,), (0,)), ((), ())), preferred_element_type=f32)


def dot_nt(a, b):
    return lax.dot_general(a, b, (((1,), (1,)), ((), ())), preferred_element_type=f32)


def dot_tn(a, b):
    return lax.dot_general(a, b, (((0,), (0,)), ((), ())), preferred_element_type=f32)


def halves(a):
    high = a.astype(bf16)
    return high, (a - high.astype(f32)).astype(bf16)


def mm(a, b):
    ah, al = a
    bh, bl = b
    return dot_nn(jnp.concatenate([ah, al], 1), jnp.concatenate([bh, bh], 0)) + dot_nn(ah, bl)


def mm_nt(a, b):
    ah, al = a
    bh, bl = b
    return dot_nt(jnp.concatenate([ah, al], 1), jnp.concatenate([bh, bh], 1)) + dot_nt(ah, bl)


def head_masks(group):
    lane = lax.broadcasted_iota(jnp.int32, (1, LANES), 1)
    if group == 0:
        return [(lane < HALF).astype(f32), (lane >= HALF).astype(f32)]
    return [None]


def head_sum(a, masks):
    if masks[0] is None:
        return jnp.sum(a, axis=1, keepdims=True)
    return sum(jnp.sum(a * m, axis=1, keepdims=True) * m for m in masks)


def masked(a, mask):
    return a if mask is None else a * mask


def fetch(sources, targets, sems):
    copies = [pltpu.make_async_copy(a, b, sems.at[k]) for k, (a, b) in enumerate(zip(sources, targets))]
    for copy in copies:
        copy.start()
    return copies


def slot_lanes(slot):
    cut = (slot % 2) * LANES
    return slot // 2, slice(cut, cut + LANES)


def group_copies(inputs, scratch, sems):
    copies = [
        [
            pltpu.make_async_copy(a.at[group], b.at[group], sems.at[k, group])
            for k, (a, b) in enumerate(zip(inputs, scratch))
        ]
        for group in range(2)
    ]
    for copy in copies[0] + copies[1]:
        copy.start()
    return copies


def writer(results, outputs, sems):
    pending = []

    def put(which, index, count):
        part = pl.ds(index * count, count)
        copy = pltpu.make_async_copy(
            results[which].at[part], outputs[which].at[part], sems.at[which, index]
        )
        copy.start()
        pending.append(copy)

    def finish():
        for copy in pending:
            copy.wait()

    return put, finish


def solve_kernel(*refs):
    inputs, outputs, scratch, results = refs[:6], refs[6:11], refs[11:17], refs[17:22]
    sems, out_sems = refs[22:]
    send_ref, qr_ref, qk_ref, solved_ref, grown_ref = results
    q_ref, k_ref, v_ref, f_ref, l_ref, e_ref = scratch
    copies = group_copies(inputs, scratch, sems)
    put, finish = writer(results, outputs, out_sems)
    row = lax.broadcasted_iota(jnp.int32, (TOK, TOK), 0)
    col = lax.broadcasted_iota(jnp.int32, (TOK, TOK), 1)
    strict = row > col
    inclusive = row >= col
    eye = (row == col).astype(f32)
    ones = inclusive.astype(bf16)
    slots = []
    heads = []
    for slot in range(4):
        group, lanes = slot_lanes(slot)
        if slot % 2 == 0:
            for copy in copies[group]:
                copy.wait()
        q = q_ref[group, :, lanes].astype(f32)
        k = k_ref[group, :, lanes].astype(f32)
        fade = f_ref[group, :, lanes].astype(f32)
        speed = l_ref[group, :, lanes].astype(f32)
        log_decay = e_ref[group, :, lanes] - jnp.exp(-0.5) / (1.0 + jnp.exp(-fade))
        learn = 1.0 / (1.0 + jnp.exp(-speed))
        masks = head_masks(group)
        removal = k * lax.rsqrt(head_sum(k * k, masks) + key_epsilon)
        d0 = log_decay.astype(bf16)
        rest = log_decay - d0.astype(f32)
        d1 = rest.astype(bf16)
        d2 = (rest - d1.astype(f32)).astype(bf16)
        cum = dot_nn(ones, d0) + dot_nn(ones, d1) + dot_nn(ones, d2)
        middle = cum[TOK // 2 : TOK // 2 + 1, :]
        forward = jnp.exp(cum - middle)
        backward = jnp.exp(middle - cum)
        undo = jnp.exp(-log_decay)
        right = learn * removal
        removers = -removal * undo * forward
        queries = q * forward
        sources = halves(jnp.concatenate([right * backward, k * backward], 0))
        final = cum[TOK - 1 : TOK, :]
        tail = jnp.exp(final - cum)
        grown_ref[slot] = q * jnp.exp(cum)
        put(4, slot, 1)
        slots.append(
            dict(
                masks=masks,
                v=v_ref[group, :, lanes],
                start=-removal * jnp.exp(cum - log_decay),
                ends=jnp.concatenate([right * tail, k * tail], 0).astype(bf16),
                kept=jnp.exp(final),
            )
        )
        for mask in masks:
            pairs = mm_nt(halves(masked(removers, mask)), sources)
            reads = dot_nt(masked(queries, mask).astype(bf16), sources[0])
            head = len(heads)
            qr_ref[head] = jnp.where(inclusive, reads[:, :TOK], 0.0).astype(bf16)
            qk_ref[head] = jnp.where(inclusive, reads[:, TOK:], 0.0).astype(bf16)
            put(1, head, 1)
            put(2, head, 1)
            heads.append(
                dict(
                    slot=slot,
                    mask=mask,
                    n=jnp.where(strict, pairs[:, :TOK], 0.0),
                    rk=jnp.where(strict, pairs[:, TOK:], 0.0),
                )
            )
    same = (row // 8) == (col // 8)
    for head in heads:
        head["m"] = jnp.where(same, head["n"], 0.0)
        head["x"] = eye + head["m"]
    for _ in range(2):
        for head in heads:
            m = halves(head["m"])
            head["m"] = mm(m, m)
        for head in heads:
            head["x"] = head["x"] + mm(halves(head["x"]), halves(head["m"]))
    size = 8
    while size < TOK:
        below = (row // (2 * size) == col // (2 * size)) & (row // size != col // size)
        for head in heads:
            off = halves(jnp.where(below, head["n"], 0.0))
            head["y"] = halves(mm(off, halves(head["x"])))
        for head in heads:
            head["x"] = head["x"] + mm(halves(head["x"]), head["y"])
        size *= 2
    for head in heads:
        part = slots[head["slot"]]
        high, low = halves(head["rk"])
        v = part["v"]
        pulled = dot_nn(jnp.concatenate([high, low], 1), jnp.concatenate([v, v], 0))
        target = jnp.concatenate([pulled, part["start"]], 1).astype(bf16)
        head["solved"] = dot_nn(
            jnp.concatenate(halves(head["x"]), 1), jnp.concatenate([target, target], 0)
        )
    for slot, part in enumerate(slots):
        mine = [head for head in heads if head["slot"] == slot]
        solved = mine[0]["solved"]
        if len(mine) == 2:
            first = jnp.concatenate([mine[0]["mask"]] * 2, 1) > 0.5
            solved = jnp.where(first, solved, mine[1]["solved"])
        solved = solved.astype(bf16)
        solved_ref[slot] = solved
        put(3, slot, 1)
        carried, start = solved[:, :LANES], solved[:, LANES:]
        transit = dot_tn(start, part["ends"][:TOK])
        added = dot_tn(jnp.concatenate([carried, part["v"]], 0), part["ends"])
        if len(mine) == 2:
            block = (row // HALF) == (col // HALF)
            transit = jnp.where(block, transit, 0.0)
            added = jnp.where(block, added, 0.0)
        transit = (transit + eye * part["kept"]).astype(bf16)
        added = added.astype(bf16)
        for half in range(2):
            send_ref[2 * slot + half, :LANES, :] = transit
            send_ref[2 * slot + half, LANES:, :] = added[half * HALF : (half + 1) * HALF, :]
        put(0, slot, 2)
    finish()


def read_kernel(*refs):
    inputs, outputs, scratch, results = refs[:10], refs[10:14], refs[14:24], refs[24:28]
    sems, out_sems = refs[28:]
    qr_ref, qk_ref, solved_ref, grown_ref, q_ref, k_ref, v_ref, gate_ref, gain_ref, own_ref = scratch
    out_ref, read_ref, scale_ref, extra_ref = results
    for copy in fetch(inputs, scratch, sems):
        copy.wait()
    put, finish = writer(results, outputs, out_sems)
    head = 0
    for slot in range(4):
        group, lanes = slot_lanes(slot)
        masks = head_masks(group)
        v = v_ref[group, :, lanes]
        found = local = None
        for mask in masks:
            one = dot_nn(qr_ref[head], solved_ref[slot])
            here = one[:, :LANES] + dot_nn(qk_ref[head], v)
            if found is None:
                found, local = one[:, LANES:], here
            else:
                found = jnp.where(mask > 0.5, one[:, LANES:], found)
                local = jnp.where(mask > 0.5, here, local)
            head += 1
        out_ref[slot] = local
        high, low = halves(grown_ref[slot] + found)
        read_ref[slot, :, :LANES] = high
        read_ref[slot, :, LANES:] = low
        gate = gate_ref[group, :, lanes].astype(f32)
        scale_ref[slot] = gain_ref[group : group + 1, lanes] * gate
        q = q_ref[group, :, lanes].astype(f32)
        k = k_ref[group, :, lanes].astype(f32)
        own = head_sum(q * k * own_ref[group : group + 1, lanes], masks)
        extra_ref[slot] = own * v.astype(f32) * gate
        for which in range(4):
            put(which, slot, 1)
    finish()


def row_kernel(got_ref, prefix_ref, total_ref):
    row = lax.broadcasted_iota(jnp.int32, (LANES + HALF, LANES), 0)
    col = lax.broadcasted_iota(jnp.int32, (LANES + HALF, LANES), 1)
    zero = jnp.zeros((LANES, LANES), f32)
    prefix_ref[0] = (row == col).astype(f32)
    run = got_ref[0].astype(f32)
    for k in range(1, SHARES):
        prefix_ref[k] = run
        got = got_ref[k]
        step = got[:LANES]
        high, low = halves(run)
        run = dot_nn(jnp.concatenate([high, low], 1), jnp.concatenate([step, step], 0))
        run = run + jnp.concatenate([zero, got[LANES:].astype(f32)], 0)
    total = run.astype(bf16)
    for k in range(total_ref.shape[0]):
        total_ref[k] = total


def state_kernel(place_ref, every_ref, prefix_ref, send_ref):
    place = place_ref[0]
    state = jnp.zeros((HALF, LANES), f32)
    for k in range(every_ref.shape[0] - 1):
        got = every_ref[k]
        step = got[:LANES]
        high, low = halves(state)
        grown = dot_nn(jnp.concatenate([high, low], 1), jnp.concatenate([step, step], 0))
        state = jnp.where(k < place, grown + got[LANES:].astype(f32), state)
    split = halves(state)
    for k in range(SHARES):
        moved = mm(split, halves(prefix_ref[k, :LANES, :]))
        send_ref[k] = (moved + prefix_ref[k, LANES:, :]).astype(bf16)


def mix_kernel(*refs):
    inputs, outputs, scratch, results, sems, out_sems = (
        refs[:6],
        refs[6:7],
        refs[7:13],
        refs[13:14],
        refs[14],
        refs[15],
    )
    state_ref, out_ref, read_ref, scale_ref, extra_ref, w_ref = scratch
    copies = fetch(inputs, scratch, sems)
    put, finish = writer(results, outputs, out_sems)
    for copy in copies[:5]:
        copy.wait()
    mixed = []
    for slot in range(4):
        width = HALF if slot < 2 else LANES
        masks = head_masks(slot // 2)
        state = jnp.concatenate([state_ref[2 * slot], state_ref[2 * slot + 1]], 0)
        raw = out_ref[slot] + dot_nt(read_ref[slot], jnp.concatenate([state, state], 1))
        centered = raw - head_sum(raw, masks) * (1.0 / width)
        variance = head_sum(centered * centered, masks) * (1.0 / width)
        normed = centered * lax.rsqrt(variance + head_epsilon) * scale_ref[slot]
        mixed.append((normed + extra_ref[slot]).astype(bf16))
    mixed = jnp.concatenate(mixed, 1)
    copies[5].wait()
    tiles, _, columns = results[0].shape
    for k in range(tiles):
        results[0][k] = dot_nn(mixed, w_ref[:, k * columns : (k + 1) * columns]).astype(bf16)
        put(0, k, 1)
    finish()


AHEAD = 16


def feed_kernel(
    far_ref,
    state_ref,
    gain_in_ref,
    whole_ref,
    sent_ref,
    w_ref,
    n_ref,
    acc_ref,
    x_ref,
    gain_ref,
    y_ref,
    sems,
    in_sems,
    out_sems,
):
    tokens_here = fetch([state_ref, gain_in_ref], [x_ref, gain_ref], in_sems)
    put, finish = writer([y_ref], [sent_ref], out_sems)
    planes, sides, near, rows, width = w_ref.shape
    third = width // 3
    far = far_ref[0]
    parts = [pl.ds(0, 2 * third), pl.ds(2 * third, third)]
    copies = [
        pltpu.make_async_copy(
            whole_ref.at[k, :, jnp.where(far == side, 0, 1), :, lanes],
            w_ref.at[k, side, :, :, lanes],
            sems.at[part, k, side],
        )
        for part, lanes in enumerate(parts)
        for k in range(planes)
        for side in range(sides)
    ]
    for copy in copies[:AHEAD]:
        copy.start()

    def arrive(part, first, count):
        start = (part * planes + first) * sides
        for k in range(start, start + count * sides):
            copies[k].wait()
            if k + AHEAD < len(copies):
                copies[k + AHEAD].start()

    shares, tokens, columns = x_ref.shape
    tiles = shares // sides
    for copy in tokens_here:
        copy.wait()
    scales = []
    for side in range(sides):
        total = 0.0
        for k in range(tiles):
            lanes = slice(k * columns, (k + 1) * columns)
            a = x_ref[side * tiles + k].astype(f32)
            n_ref[side * tokens : (side + 1) * tokens, lanes] = (a * gain_ref[:, lanes]).astype(
                bf16
            )
            total = total + jnp.sum(a * a, axis=1, keepdims=True)
        scales.append(lax.rsqrt(total * (1.0 / (tiles * columns)) + norm_epsilon))
    scale = jnp.concatenate(scales, 0)
    block = sides * near * rows
    for k in range(0, planes, 2):
        arrive(0, k, 2)
        part = dot_nn(
            n_ref[:, k * block : (k + 2) * block],
            w_ref[k : k + 2, :, :, :, : 2 * third].reshape(2 * block, 2 * third),
        )
        if k == 0:
            acc_ref[...] = part
        else:
            acc_ref[...] += part
    gate = acc_ref[:, :third] * scale
    up = acc_ref[:, third:] * scale
    active = (gate / (1.0 + jnp.exp(-gate)) * up).astype(bf16)
    per = planes // tiles
    for k in range(tiles):
        arrive(1, k * per, per)
        down = w_ref[k * per : (k + 1) * per, :, :, :, 2 * third :].reshape(per * block, third)
        out = dot_nt(active, down).astype(bf16)
        for side in range(sides):
            y_ref[side * tiles + k] = out[side * tokens : (side + 1) * tokens]
            put(0, side * tiles + k, 1)
    finish()


def feed_forward(far, state, gain, whole):
    planes, near, sides, rows, width = whole.shape
    shares, tokens, columns = state.shape
    return pl.pallas_call(
        feed_kernel,
        out_shape=array((shares, tokens, columns), bf16),
        in_specs=[SMEM, HBM, HBM, HBM],
        out_specs=HBM,
        scratch_shapes=[
            pltpu.VMEM((planes, sides, near, rows, width), bf16),
            pltpu.VMEM((sides * tokens, gain.shape[1]), bf16),
            pltpu.VMEM((sides * tokens, 2 * width // 3), f32),
            pltpu.VMEM(state.shape, bf16),
            pltpu.VMEM(gain.shape, f32),
            pltpu.VMEM(state.shape, bf16),
            pltpu.SemaphoreType.DMA((2, planes, sides)),
            pltpu.SemaphoreType.DMA((2,)),
            pltpu.SemaphoreType.DMA((1, shares)),
        ],
        compiler_params=pltpu.CompilerParams(vmem_limit_bytes=55_000_000),
    )(far, state, gain, whole)


def pack_kernel(far_ref, *refs):
    inputs, (kept_ref, given_ref), scratch, sems = refs[:3], refs[3:5], refs[5:8], refs[8]
    copies = fetch(inputs, scratch, sems)
    wide = kept_ref.shape[1] // 3
    first = far_ref[0] == 0
    for k, copy in enumerate(copies):
        copy.wait()
        lanes = slice(k * wide, (k + 1) * wide)
        kept_ref[given_ref.shape[0] :, lanes] = jnp.zeros((given_ref.shape[0], wide), bf16)
        near = scratch[k][:, :wide]
        rest = scratch[k][:, wide:]
        blank = jnp.zeros((rest.shape[0], 2 * wide - scratch[k].shape[1]), bf16)
        far = jnp.concatenate([rest, blank], axis=1)
        kept_ref[: near.shape[0], lanes] = jnp.where(first, near, far)
        given_ref[:, lanes] = jnp.where(first, far, near)


def swapped(far, parts):
    rows, hidden = parts[0].shape
    wide = -(-hidden // (2 * LANES)) * LANES
    packed = (array((2 * rows, 3 * wide), bf16), array((rows, 3 * wide), bf16))
    kept, given = call(pack_kernel, packed, [SMEM] + [HBM] * 3, parts, 62_000_000)(far, *parts)
    return kept, lax.ppermute(given, FAR, [(0, 1), (1, 0)])


def gathered(kept, taken):
    rows, width = taken.shape
    both = lax.dynamic_update_slice(kept, taken, (rows, 0))
    whole = lax.all_gather(both, GATHER, axis=0, tiled=True)
    planes = lax.axis_size(PLANE)
    near = lax.axis_size(NEAR) * lax.axis_size(CORE)
    return whole.reshape(planes, near, 2, rows, width)


VMEM = pl.BlockSpec(memory_space=pltpu.VMEM)
HBM = pl.BlockSpec(memory_space=pltpu.HBM)
SMEM = pl.BlockSpec(memory_space=pltpu.SMEM)


def call(kernel, outs, specs, fetched=(), limit=24 * 1024 * 1024, written=0, sems=()):
    scratch = [pltpu.VMEM(a.shape, a.dtype) for a in fetched]
    where = VMEM
    if written:
        where = HBM
        scratch += [pltpu.VMEM(a.shape, a.dtype) for a in outs]
    scratch += [pltpu.SemaphoreType.DMA(a) for a in sems or [(len(fetched),)] if fetched]
    if written:
        scratch.append(pltpu.SemaphoreType.DMA((len(outs), written)))
    return pl.pallas_call(
        kernel,
        out_shape=outs,
        in_specs=specs,
        out_specs=jax.tree.map(lambda _: where, outs),
        scratch_shapes=scratch,
        compiler_params=pltpu.CompilerParams(vmem_limit_bytes=limit),
    )


def array(dims, kind):
    return jax.ShapeDtypeStruct(dims, kind)


def exchange(value, axis):
    return lax.all_to_all(value, axis, 0, 0, tiled=True)


def from_everyone(value, axis):
    devices = lax.psum(1, axis)
    return exchange(jnp.broadcast_to(value[None], (devices, *value.shape)), axis)


def on_device(
    stratum_source_matrix,
    acceptance_query,
    cluster_lookup_matrix,
    cluster_payload_matrix,
    fading_logit,
    adaptation_speed_logit,
    additional_fading_exponent,
    result_switch_pair,
    attender_scaling_factor,
    present_item_factor,
    final_mapping_matrix,
    perceptron_scaling_factor,
    switching_matrix,
    widening_matrix,
    shrinking_matrix,
):
    features = perceptron_scaling_factor.shape[0]
    columns = features // lax.axis_size(TP)
    far = lax.axis_index(FAR).astype(jnp.int32).reshape(1)
    kept, taken = swapped(far, [switching_matrix, widening_matrix, shrinking_matrix.T])
    blocks = array((4, TOK, LANES), f32)
    pairs = array((6, TOK, TOK), bf16)
    doubled = array((4, TOK, 2 * LANES), bf16)
    inputs = (
        acceptance_query,
        cluster_lookup_matrix,
        cluster_payload_matrix,
        fading_logit,
        adaptation_speed_logit,
        additional_fading_exponent,
    )
    send, *found = call(
        solve_kernel,
        (array((SHARES, LANES + HALF, LANES), bf16), pairs, pairs, doubled, blocks),
        [HBM] * len(inputs),
        inputs,
        65_900_000,
        6,
        [(len(inputs), 2)],
    )(*inputs)
    place = lax.axis_index(PLANE).astype(jnp.int32).reshape(1)
    first_column = (lax.axis_index(TP) * columns).astype(jnp.uint32)
    send, taken, place, first_column = lax.optimization_barrier((send, taken, place, first_column))
    whole = gathered(kept, taken)
    planes = lax.axis_size(PLANE)
    prefix, total = call(
        row_kernel,
        (
            array((SHARES, LANES + HALF, LANES), f32),
            array((planes, LANES + HALF, LANES), bf16),
        ),
        [VMEM],
    )(exchange(send, ROW))
    total, first_column, *found = lax.optimization_barrier((total, first_column, *found))
    reading = (
        *found,
        *inputs[:3],
        result_switch_pair,
        attender_scaling_factor,
        present_item_factor,
    )
    read = call(
        read_kernel,
        (blocks, doubled, blocks, blocks),
        [HBM] * len(reading),
        reading,
        64_500_000,
        4,
    )(*reading)
    residual = lax.dynamic_slice(
        stratum_source_matrix, (jnp.uint32(0), first_column), (TOK, columns)
    )
    every, residual, *read = lax.optimization_barrier((exchange(total, PLANE), residual, *read))
    states = call(state_kernel, array((SHARES, HALF, LANES), bf16), [SMEM, VMEM, VMEM])(
        place, every, prefix
    )
    mixing = (exchange(states, ROW), *read, final_mapping_matrix.reshape(-1, features))
    (terms,) = call(
        mix_kernel,
        (array((features // columns, TOK, columns), bf16),),
        [HBM] * len(mixing),
        mixing,
        64_000_000,
        features // columns,
    )(*mixing)
    attention = jnp.sum(exchange(terms, TP).astype(f32), axis=0)
    own_state = (residual.astype(f32) + attention).astype(bf16)
    tiles = feed_forward(
        far,
        from_everyone(own_state, POOL),
        perceptron_scaling_factor.reshape(1, features),
        whole,
    )
    mixer = jnp.sum(exchange(tiles, POOL).astype(f32), axis=0)
    return (own_state.astype(f32) + mixer).astype(bf16)


def solution(mesh):
    split = Mesh(mesh.devices.reshape(8, 2, 2, 2, mesh.shape["tp"]), (*SP, TP))
    heads = P(None, SP, "tp")
    return jax.shard_map(
        on_device,
        mesh=split,
        in_specs=(
            P(SP, None),
            heads,
            heads,
            heads,
            heads,
            heads,
            heads,
            heads,
            P(None, TP),
            P(None, TP),
            P(None, TP, None),
            P(),
            P(SP, TP),
            P(SP, TP),
            P(TP, SP),
        ),
        out_specs=P(SP, TP),
        check_vma=False,
    )
```

```python
import jax
import jax.numpy as jnp
from jax import lax
from jax.experimental import pallas as pl
from jax.experimental.pallas import tpu as pltpu
from jax.sharding import Mesh
from jax.sharding import PartitionSpec as P

PLANE, FAR, NEAR, CORE, TP = "plane", "far", "near", "core", "tp"
SP = (PLANE, FAR, NEAR, CORE)
ROW = (FAR, NEAR, CORE)
GATHER = (PLANE, NEAR, CORE)
POOL = (FAR, TP)
TOK = 128
LANES = 128
HALF = 64
SHARES = 8

norm_epsilon = 1e-06
head_epsilon = 0.00064
key_epsilon = 1e-06

f32 = jnp.float32
bf16 = jnp.bfloat16


def dot_nn(a, b):
    return lax.dot_general(a, b, (((1,), (0,)), ((), ())), preferred_element_type=f32)


def dot_nt(a, b):
    return lax.dot_general(a, b, (((1,), (1,)), ((), ())), preferred_element_type=f32)


def dot_tn(a, b):
    return lax.dot_general(a, b, (((0,), (0,)), ((), ())), preferred_element_type=f32)


def halves(a):
    high = a.astype(bf16)
    return high, (a - high.astype(f32)).astype(bf16)


def mm(a, b):
    ah, al = a
    bh, bl = b
    return dot_nn(jnp.concatenate([ah, al], 1), jnp.concatenate([bh, bh], 0)) + dot_nn(ah, bl)


def mm_nt(a, b):
    ah, al = a
    bh, bl = b
    return dot_nt(jnp.concatenate([ah, al], 1), jnp.concatenate([bh, bh], 1)) + dot_nt(ah, bl)


def head_masks(group):
    lane = lax.broadcasted_iota(jnp.int32, (1, LANES), 1)
    if group == 0:
        return [(lane < HALF).astype(f32), (lane >= HALF).astype(f32)]
    return [None]


def head_sum(a, masks):
    if masks[0] is None:
        return jnp.sum(a, axis=1, keepdims=True)
    return sum(jnp.sum(a * m, axis=1, keepdims=True) * m for m in masks)


def masked(a, mask):
    return a if mask is None else a * mask


def fetch(sources, targets, sems):
    copies = [pltpu.make_async_copy(a, b, sems.at[k]) for k, (a, b) in enumerate(zip(sources, targets))]
    for copy in copies:
        copy.start()
    return copies


def slot_lanes(slot):
    cut = (slot % 2) * LANES
    return slot // 2, slice(cut, cut + LANES)


def group_copies(inputs, scratch, sems):
    copies = [
        [
            pltpu.make_async_copy(a.at[group], b.at[group], sems.at[k, group])
            for k, (a, b) in enumerate(zip(inputs, scratch))
        ]
        for group in range(2)
    ]
    for copy in copies[0] + copies[1]:
        copy.start()
    return copies


def writer(results, outputs, sems):
    pending = []

    def put(which, index, count):
        part = pl.ds(index * count, count)
        copy = pltpu.make_async_copy(
            results[which].at[part], outputs[which].at[part], sems.at[which, index]
        )
        copy.start()
        pending.append(copy)

    def finish():
        for copy in pending:
            copy.wait()

    return put, finish


def solve_kernel(*refs):
    inputs, outputs, scratch, results = refs[:6], refs[6:11], refs[11:17], refs[17:22]
    sems, out_sems = refs[22:]
    send_ref, qr_ref, qk_ref, solved_ref, grown_ref = results
    q_ref, k_ref, v_ref, f_ref, l_ref, e_ref = scratch
    copies = group_copies(inputs, scratch, sems)
    put, finish = writer(results, outputs, out_sems)
    row = lax.broadcasted_iota(jnp.int32, (TOK, TOK), 0)
    col = lax.broadcasted_iota(jnp.int32, (TOK, TOK), 1)
    strict = row > col
    inclusive = row >= col
    eye = (row == col).astype(f32)
    ones = inclusive.astype(bf16)
    slots = []
    heads = []
    for slot in range(4):
        group, lanes = slot_lanes(slot)
        if slot % 2 == 0:
            for copy in copies[group]:
                copy.wait()
        q = q_ref[group, :, lanes].astype(f32)
        k = k_ref[group, :, lanes].astype(f32)
        fade = f_ref[group, :, lanes].astype(f32)
        speed = l_ref[group, :, lanes].astype(f32)
        log_decay = e_ref[group, :, lanes] - jnp.exp(-0.5) / (1.0 + jnp.exp(-fade))
        learn = 1.0 / (1.0 + jnp.exp(-speed))
        masks = head_masks(group)
        removal = k * lax.rsqrt(head_sum(k * k, masks) + key_epsilon)
        d0 = log_decay.astype(bf16)
        rest = log_decay - d0.astype(f32)
        d1 = rest.astype(bf16)
        d2 = (rest - d1.astype(f32)).astype(bf16)
        cum = dot_nn(ones, d0) + dot_nn(ones, d1) + dot_nn(ones, d2)
        middle = cum[TOK // 2 : TOK // 2 + 1, :]
        forward = jnp.exp(cum - middle)
        backward = jnp.exp(middle - cum)
        undo = jnp.exp(-log_decay)
        right = learn * removal
        removers = -removal * undo * forward
        queries = q * forward
        sources = halves(jnp.concatenate([right * backward, k * backward], 0))
        final = cum[TOK - 1 : TOK, :]
        tail = jnp.exp(final - cum)
        grown_ref[slot] = q * jnp.exp(cum)
        put(4, slot, 1)
        slots.append(
            dict(
                masks=masks,
                v=v_ref[group, :, lanes],
                start=-removal * jnp.exp(cum - log_decay),
                ends=jnp.concatenate([right * tail, k * tail], 0).astype(bf16),
                kept=jnp.exp(final),
            )
        )
        for mask in masks:
            pairs = mm_nt(halves(masked(removers, mask)), sources)
            reads = dot_nt(masked(queries, mask).astype(bf16), sources[0])
            head = len(heads)
            qr_ref[head] = jnp.where(inclusive, reads[:, :TOK], 0.0).astype(bf16)
            qk_ref[head] = jnp.where(inclusive, reads[:, TOK:], 0.0).astype(bf16)
            put(1, head, 1)
            put(2, head, 1)
            heads.append(
                dict(
                    slot=slot,
                    mask=mask,
                    n=jnp.where(strict, pairs[:, :TOK], 0.0),
                    rk=jnp.where(strict, pairs[:, TOK:], 0.0),
                )
            )
    same = (row // 8) == (col // 8)
    for head in heads:
        head["m"] = jnp.where(same, head["n"], 0.0)
        head["x"] = eye + head["m"]
    for _ in range(2):
        for head in heads:
            m = halves(head["m"])
            head["m"] = mm(m, m)
        for head in heads:
            head["x"] = head["x"] + mm(halves(head["x"]), halves(head["m"]))
    size = 8
    while size < TOK:
        below = (row // (2 * size) == col // (2 * size)) & (row // size != col // size)
        for head in heads:
            off = halves(jnp.where(below, head["n"], 0.0))
            head["y"] = halves(mm(off, halves(head["x"])))
        for head in heads:
            head["x"] = head["x"] + mm(halves(head["x"]), head["y"])
        size *= 2
    for head in heads:
        part = slots[head["slot"]]
        high, low = halves(head["rk"])
        v = part["v"]
        pulled = dot_nn(jnp.concatenate([high, low], 1), jnp.concatenate([v, v], 0))
        target = jnp.concatenate([pulled, part["start"]], 1).astype(bf16)
        head["solved"] = dot_nn(
            jnp.concatenate(halves(head["x"]), 1), jnp.concatenate([target, target], 0)
        )
    for slot, part in enumerate(slots):
        mine = [head for head in heads if head["slot"] == slot]
        solved = mine[0]["solved"]
        if len(mine) == 2:
            first = jnp.concatenate([mine[0]["mask"]] * 2, 1) > 0.5
            solved = jnp.where(first, solved, mine[1]["solved"])
        solved = solved.astype(bf16)
        solved_ref[slot] = solved
        put(3, slot, 1)
        carried, start = solved[:, :LANES], solved[:, LANES:]
        transit = dot_tn(start, part["ends"][:TOK])
        added = dot_tn(jnp.concatenate([carried, part["v"]], 0), part["ends"])
        if len(mine) == 2:
            block = (row // HALF) == (col // HALF)
            transit = jnp.where(block, transit, 0.0)
            added = jnp.where(block, added, 0.0)
        transit = (transit + eye * part["kept"]).astype(bf16)
        added = added.astype(bf16)
        for half in range(2):
            send_ref[2 * slot + half, :LANES, :] = transit
            send_ref[2 * slot + half, LANES:, :] = added[half * HALF : (half + 1) * HALF, :]
        put(0, slot, 2)
    finish()


def read_kernel(*refs):
    inputs, outputs, scratch, results = refs[:10], refs[10:14], refs[14:24], refs[24:28]
    sems, out_sems = refs[28:]
    qr_ref, qk_ref, solved_ref, grown_ref, q_ref, k_ref, v_ref, gate_ref, gain_ref, own_ref = scratch
    out_ref, read_ref, scale_ref, extra_ref = results
    for copy in fetch(inputs, scratch, sems):
        copy.wait()
    put, finish = writer(results, outputs, out_sems)
    head = 0
    for slot in range(4):
        group, lanes = slot_lanes(slot)
        masks = head_masks(group)
        v = v_ref[group, :, lanes]
        found = local = None
        for mask in masks:
            one = dot_nn(qr_ref[head], solved_ref[slot])
            here = one[:, :LANES] + dot_nn(qk_ref[head], v)
            if found is None:
                found, local = one[:, LANES:], here
            else:
                found = jnp.where(mask > 0.5, one[:, LANES:], found)
                local = jnp.where(mask > 0.5, here, local)
            head += 1
        out_ref[slot] = local
        high, low = halves(grown_ref[slot] + found)
        read_ref[slot, :, :LANES] = high
        read_ref[slot, :, LANES:] = low
        gate = gate_ref[group, :, lanes].astype(f32)
        scale_ref[slot] = gain_ref[group : group + 1, lanes] * gate
        q = q_ref[group, :, lanes].astype(f32)
        k = k_ref[group, :, lanes].astype(f32)
        own = head_sum(q * k * own_ref[group : group + 1, lanes], masks)
        extra_ref[slot] = own * v.astype(f32) * gate
        for which in range(4):
            put(which, slot, 1)
    finish()


def row_kernel(got_ref, prefix_ref, total_ref):
    row = lax.broadcasted_iota(jnp.int32, (LANES + HALF, LANES), 0)
    col = lax.broadcasted_iota(jnp.int32, (LANES + HALF, LANES), 1)
    zero = jnp.zeros((LANES, LANES), f32)
    prefix_ref[0] = (row == col).astype(f32)
    run = got_ref[0].astype(f32)
    for k in range(1, SHARES):
        prefix_ref[k] = run
        got = got_ref[k]
        step = got[:LANES]
        high, low = halves(run)
        run = dot_nn(jnp.concatenate([high, low], 1), jnp.concatenate([step, step], 0))
        run = run + jnp.concatenate([zero, got[LANES:].astype(f32)], 0)
    total = run.astype(bf16)
    for k in range(total_ref.shape[0]):
        total_ref[k] = total


def state_kernel(place_ref, every_ref, prefix_ref, send_ref):
    place = place_ref[0]
    state = jnp.zeros((HALF, LANES), f32)
    for k in range(every_ref.shape[0] - 1):
        got = every_ref[k]
        step = got[:LANES]
        high, low = halves(state)
        grown = dot_nn(jnp.concatenate([high, low], 1), jnp.concatenate([step, step], 0))
        state = jnp.where(k < place, grown + got[LANES:].astype(f32), state)
    split = halves(state)
    for k in range(SHARES):
        moved = mm(split, halves(prefix_ref[k, :LANES, :]))
        send_ref[k] = (moved + prefix_ref[k, LANES:, :]).astype(bf16)


def mix_kernel(*refs):
    inputs, outputs, scratch, results, sems, out_sems = (
        refs[:6],
        refs[6:7],
        refs[7:13],
        refs[13:14],
        refs[14],
        refs[15],
    )
    state_ref, out_ref, read_ref, scale_ref, extra_ref, w_ref = scratch
    copies = fetch(inputs, scratch, sems)
    put, finish = writer(results, outputs, out_sems)
    for copy in copies[:5]:
        copy.wait()
    mixed = []
    for slot in range(4):
        width = HALF if slot < 2 else LANES
        masks = head_masks(slot // 2)
        state = jnp.concatenate([state_ref[2 * slot], state_ref[2 * slot + 1]], 0)
        raw = out_ref[slot] + dot_nt(read_ref[slot], jnp.concatenate([state, state], 1))
        centered = raw - head_sum(raw, masks) * (1.0 / width)
        variance = head_sum(centered * centered, masks) * (1.0 / width)
        normed = centered * lax.rsqrt(variance + head_epsilon) * scale_ref[slot]
        mixed.append((normed + extra_ref[slot]).astype(bf16))
    mixed = jnp.concatenate(mixed, 1)
    copies[5].wait()
    tiles, _, columns = results[0].shape
    for k in range(tiles):
        results[0][k] = dot_nn(mixed, w_ref[:, k * columns : (k + 1) * columns]).astype(bf16)
        put(0, k, 1)
    finish()


AHEAD = 24


def feed_kernel(
    far_ref,
    x_ref,
    gain_in_ref,
    whole_ref,
    sent_ref,
    w_ref,
    n_ref,
    acc_ref,
    gain_ref,
    y_ref,
    sems,
    in_sems,
    out_sems,
):
    (gain_here,) = fetch([gain_in_ref], [gain_ref], in_sems)
    put, finish = writer([y_ref], [sent_ref], out_sems)
    planes, sides, near, rows, width = w_ref.shape
    third = width // 3
    far = far_ref[0]
    parts = [pl.ds(0, 2 * third), pl.ds(2 * third, third)]
    copies = [
        pltpu.make_async_copy(
            whole_ref.at[k, :, jnp.where(far == side, 0, 1), :, lanes],
            w_ref.at[k, side, :, :, lanes],
            sems.at[part, k, side],
        )
        for part, lanes in enumerate(parts)
        for k in range(planes)
        for side in range(sides)
    ]
    for copy in copies[:AHEAD]:
        copy.start()

    def arrive(part, first, count):
        start = (part * planes + first) * sides
        for k in range(start, start + count * sides):
            copies[k].wait()
            if k + AHEAD < len(copies):
                copies[k + AHEAD].start()

    shares, tokens, columns = x_ref.shape
    tiles = shares // sides
    gain_here.wait()
    scales = []
    for side in range(sides):
        total = 0.0
        for k in range(tiles):
            lanes = slice(k * columns, (k + 1) * columns)
            a = x_ref[side * tiles + k].astype(f32)
            n_ref[side * tokens : (side + 1) * tokens, lanes] = (a * gain_ref[:, lanes]).astype(
                bf16
            )
            total = total + jnp.sum(a * a, axis=1, keepdims=True)
        scales.append(lax.rsqrt(total * (1.0 / (tiles * columns)) + norm_epsilon))
    scale = jnp.concatenate(scales, 0)
    block = sides * near * rows
    for k in range(0, planes, 2):
        arrive(0, k, 2)
        part = dot_nn(
            n_ref[:, k * block : (k + 2) * block],
            w_ref[k : k + 2, :, :, :, : 2 * third].reshape(2 * block, 2 * third),
        )
        if k == 0:
            acc_ref[...] = part
        else:
            acc_ref[...] += part
    gate = acc_ref[:, :third] * scale
    up = acc_ref[:, third:] * scale
    active = (gate / (1.0 + jnp.exp(-gate)) * up).astype(bf16)
    per = planes // tiles
    for k in range(tiles):
        arrive(1, k * per, per)
        down = w_ref[k * per : (k + 1) * per, :, :, :, 2 * third :].reshape(per * block, third)
        out = dot_nt(active, down).astype(bf16)
        for side in range(sides):
            y_ref[side * tiles + k] = out[side * tokens : (side + 1) * tokens]
            put(0, side * tiles + k, 1)
    finish()


def feed_forward(far, state, gain, whole):
    planes, near, sides, rows, width = whole.shape
    shares, tokens, columns = state.shape
    return pl.pallas_call(
        feed_kernel,
        out_shape=array((shares, tokens, columns), bf16),
        in_specs=[SMEM, VMEM, HBM, HBM],
        out_specs=HBM,
        scratch_shapes=[
            pltpu.VMEM((planes, sides, near, rows, width), bf16),
            pltpu.VMEM((sides * tokens, gain.shape[1]), bf16),
            pltpu.VMEM((sides * tokens, 2 * width // 3), f32),
            pltpu.VMEM(gain.shape, f32),
            pltpu.VMEM(state.shape, bf16),
            pltpu.SemaphoreType.DMA((2, planes, sides)),
            pltpu.SemaphoreType.DMA((1,)),
            pltpu.SemaphoreType.DMA((1, shares)),
        ],
        compiler_params=pltpu.CompilerParams(vmem_limit_bytes=52_000_000),
    )(far, state, gain, whole)


def pack_kernel(far_ref, *refs):
    inputs, (kept_ref, given_ref), scratch, sems = refs[:3], refs[3:5], refs[5:8], refs[8]
    copies = fetch(inputs, scratch, sems)
    wide = kept_ref.shape[1] // 3
    first = far_ref[0] == 0
    for k, copy in enumerate(copies):
        copy.wait()
        lanes = slice(k * wide, (k + 1) * wide)
        kept_ref[given_ref.shape[0] :, lanes] = jnp.zeros((given_ref.shape[0], wide), bf16)
        near = scratch[k][:, :wide]
        rest = scratch[k][:, wide:]
        blank = jnp.zeros((rest.shape[0], 2 * wide - scratch[k].shape[1]), bf16)
        far = jnp.concatenate([rest, blank], axis=1)
        kept_ref[: near.shape[0], lanes] = jnp.where(first, near, far)
        given_ref[:, lanes] = jnp.where(first, far, near)


def swapped(far, parts):
    rows, hidden = parts[0].shape
    wide = -(-hidden // (2 * LANES)) * LANES
    packed = (array((2 * rows, 3 * wide), bf16), array((rows, 3 * wide), bf16))
    kept, given = call(pack_kernel, packed, [SMEM] + [HBM] * 3, parts, 62_000_000)(far, *parts)
    return kept, lax.ppermute(given, FAR, [(0, 1), (1, 0)])


def gathered(kept, taken):
    rows, width = taken.shape
    both = lax.dynamic_update_slice(kept, taken, (rows, 0))
    whole = lax.all_gather(both, GATHER, axis=0, tiled=True)
    planes = lax.axis_size(PLANE)
    near = lax.axis_size(NEAR) * lax.axis_size(CORE)
    return whole.reshape(planes, near, 2, rows, width)


VMEM = pl.BlockSpec(memory_space=pltpu.VMEM)
HBM = pl.BlockSpec(memory_space=pltpu.HBM)
SMEM = pl.BlockSpec(memory_space=pltpu.SMEM)


def call(kernel, outs, specs, fetched=(), limit=24 * 1024 * 1024, written=0, sems=()):
    scratch = [pltpu.VMEM(a.shape, a.dtype) for a in fetched]
    where = VMEM
    if written:
        where = HBM
        scratch += [pltpu.VMEM(a.shape, a.dtype) for a in outs]
    scratch += [pltpu.SemaphoreType.DMA(a) for a in sems or [(len(fetched),)] if fetched]
    if written:
        scratch.append(pltpu.SemaphoreType.DMA((len(outs), written)))
    return pl.pallas_call(
        kernel,
        out_shape=outs,
        in_specs=specs,
        out_specs=jax.tree.map(lambda _: where, outs),
        scratch_shapes=scratch,
        compiler_params=pltpu.CompilerParams(vmem_limit_bytes=limit),
    )


def array(dims, kind):
    return jax.ShapeDtypeStruct(dims, kind)


def exchange(value, axis):
    return lax.all_to_all(value, axis, 0, 0, tiled=True)


def from_everyone(value, axis):
    devices = lax.psum(1, axis)
    return exchange(jnp.broadcast_to(value[None], (devices, *value.shape)), axis)


def on_device(
    stratum_source_matrix,
    acceptance_query,
    cluster_lookup_matrix,
    cluster_payload_matrix,
    fading_logit,
    adaptation_speed_logit,
    additional_fading_exponent,
    result_switch_pair,
    attender_scaling_factor,
    present_item_factor,
    final_mapping_matrix,
    perceptron_scaling_factor,
    switching_matrix,
    widening_matrix,
    shrinking_matrix,
):
    features = perceptron_scaling_factor.shape[0]
    columns = features // lax.axis_size(TP)
    far = lax.axis_index(FAR).astype(jnp.int32).reshape(1)
    kept, taken = swapped(far, [switching_matrix, widening_matrix, shrinking_matrix.T])
    blocks = array((4, TOK, LANES), f32)
    pairs = array((6, TOK, TOK), bf16)
    doubled = array((4, TOK, 2 * LANES), bf16)
    inputs = (
        acceptance_query,
        cluster_lookup_matrix,
        cluster_payload_matrix,
        fading_logit,
        adaptation_speed_logit,
        additional_fading_exponent,
    )
    send, *found = call(
        solve_kernel,
        (array((SHARES, LANES + HALF, LANES), bf16), pairs, pairs, doubled, blocks),
        [HBM] * len(inputs),
        inputs,
        65_900_000,
        6,
        [(len(inputs), 2)],
    )(*inputs)
    place = lax.axis_index(PLANE).astype(jnp.int32).reshape(1)
    first_column = (lax.axis_index(TP) * columns).astype(jnp.uint32)
    send, taken, place, first_column = lax.optimization_barrier((send, taken, place, first_column))
    whole = gathered(kept, taken)
    planes = lax.axis_size(PLANE)
    prefix, total = call(
        row_kernel,
        (
            array((SHARES, LANES + HALF, LANES), f32),
            array((planes, LANES + HALF, LANES), bf16),
        ),
        [VMEM],
    )(exchange(send, ROW))
    total, first_column, *found = lax.optimization_barrier((total, first_column, *found))
    reading = (
        *found,
        *inputs[:3],
        result_switch_pair,
        attender_scaling_factor,
        present_item_factor,
    )
    read = call(
        read_kernel,
        (blocks, doubled, blocks, blocks),
        [HBM] * len(reading),
        reading,
        64_500_000,
        4,
    )(*reading)
    residual = lax.dynamic_slice(
        stratum_source_matrix, (jnp.uint32(0), first_column), (TOK, columns)
    )
    every, residual, *read = lax.optimization_barrier((exchange(total, PLANE), residual, *read))
    states = call(state_kernel, array((SHARES, HALF, LANES), bf16), [SMEM, VMEM, VMEM])(
        place, every, prefix
    )
    mixing = (exchange(states, ROW), *read, final_mapping_matrix.reshape(-1, features))
    (terms,) = call(
        mix_kernel,
        (array((features // columns, TOK, columns), bf16),),
        [HBM] * len(mixing),
        mixing,
        64_000_000,
        features // columns,
    )(*mixing)
    attention = jnp.sum(exchange(terms, TP).astype(f32), axis=0)
    own_state = (residual.astype(f32) + attention).astype(bf16)
    tiles = feed_forward(
        far,
        from_everyone(own_state, POOL),
        perceptron_scaling_factor.reshape(1, features),
        whole,
    )
    mixer = jnp.sum(exchange(tiles, POOL).astype(f32), axis=0)
    return (own_state.astype(f32) + mixer).astype(bf16)


def solution(mesh):
    split = Mesh(mesh.devices.reshape(8, 2, 2, 2, mesh.shape["tp"]), (*SP, TP))
    heads = P(None, SP, "tp")
    return jax.shard_map(
        on_device,
        mesh=split,
        in_specs=(
            P(SP, None),
            heads,
            heads,
            heads,
            heads,
            heads,
            heads,
            heads,
            P(None, TP),
            P(None, TP),
            P(None, TP, None),
            P(),
            P(SP, TP),
            P(SP, TP),
            P(TP, SP),
        ),
        out_specs=P(SP, TP),
        check_vma=False,
    )
```

```python
import jax
import jax.numpy as jnp
from jax import lax
from jax.experimental import pallas as pl
from jax.experimental.pallas import tpu as pltpu
from jax.sharding import Mesh
from jax.sharding import PartitionSpec as P

PLANE, FAR, NEAR, CORE, TP = "plane", "far", "near", "core", "tp"
SP = (PLANE, FAR, NEAR, CORE)
ROW = (FAR, NEAR, CORE)
GATHER = (PLANE, NEAR, CORE)
POOL = (FAR, TP)
TOK = 128
LANES = 128
HALF = 64
SHARES = 8

norm_epsilon = 1e-06
head_epsilon = 0.00064
key_epsilon = 1e-06

f32 = jnp.float32
bf16 = jnp.bfloat16


def dot_nn(a, b):
    return lax.dot_general(a, b, (((1,), (0,)), ((), ())), preferred_element_type=f32)


def dot_nt(a, b):
    return lax.dot_general(a, b, (((1,), (1,)), ((), ())), preferred_element_type=f32)


def dot_tn(a, b):
    return lax.dot_general(a, b, (((0,), (0,)), ((), ())), preferred_element_type=f32)


def halves(a):
    high = a.astype(bf16)
    return high, (a - high.astype(f32)).astype(bf16)


def mm(a, b):
    ah, al = a
    bh, bl = b
    return dot_nn(jnp.concatenate([ah, al], 1), jnp.concatenate([bh, bh], 0)) + dot_nn(ah, bl)


def mm_nt(a, b):
    ah, al = a
    bh, bl = b
    return dot_nt(jnp.concatenate([ah, al], 1), jnp.concatenate([bh, bh], 1)) + dot_nt(ah, bl)


def head_masks(group):
    lane = lax.broadcasted_iota(jnp.int32, (1, LANES), 1)
    if group == 0:
        return [(lane < HALF).astype(f32), (lane >= HALF).astype(f32)]
    return [None]


def head_sum(a, masks):
    if masks[0] is None:
        return jnp.sum(a, axis=1, keepdims=True)
    return sum(jnp.sum(a * m, axis=1, keepdims=True) * m for m in masks)


def masked(a, mask):
    return a if mask is None else a * mask


def fetch(sources, targets, sems):
    copies = [pltpu.make_async_copy(a, b, sems.at[k]) for k, (a, b) in enumerate(zip(sources, targets))]
    for copy in copies:
        copy.start()
    return copies


def slot_lanes(slot):
    cut = (slot % 2) * LANES
    return slot // 2, slice(cut, cut + LANES)


def group_copies(inputs, scratch, sems):
    copies = [
        [
            pltpu.make_async_copy(a.at[group], b.at[group], sems.at[k, group])
            for k, (a, b) in enumerate(zip(inputs, scratch))
        ]
        for group in range(2)
    ]
    for copy in copies[0] + copies[1]:
        copy.start()
    return copies


def writer(results, outputs, sems):
    pending = []

    def put(which, index, count):
        part = pl.ds(index * count, count)
        copy = pltpu.make_async_copy(
            results[which].at[part], outputs[which].at[part], sems.at[which, index]
        )
        copy.start()
        pending.append(copy)

    def finish():
        for copy in pending:
            copy.wait()

    return put, finish


def solve_kernel(*refs):
    inputs, outputs, scratch, results = refs[:6], refs[6:11], refs[11:17], refs[17:22]
    sems, out_sems = refs[22:]
    send_ref, qr_ref, qk_ref, solved_ref, grown_ref = results
    q_ref, k_ref, v_ref, f_ref, l_ref, e_ref = scratch
    copies = group_copies(inputs, scratch, sems)
    put, finish = writer(results, outputs, out_sems)
    row = lax.broadcasted_iota(jnp.int32, (TOK, TOK), 0)
    col = lax.broadcasted_iota(jnp.int32, (TOK, TOK), 1)
    strict = row > col
    inclusive = row >= col
    eye = (row == col).astype(f32)
    ones = inclusive.astype(bf16)
    slots = []
    heads = []
    for slot in range(4):
        group, lanes = slot_lanes(slot)
        if slot % 2 == 0:
            for copy in copies[group]:
                copy.wait()
        q = q_ref[group, :, lanes].astype(f32)
        k = k_ref[group, :, lanes].astype(f32)
        fade = f_ref[group, :, lanes].astype(f32)
        speed = l_ref[group, :, lanes].astype(f32)
        log_decay = e_ref[group, :, lanes] - jnp.exp(-0.5) / (1.0 + jnp.exp(-fade))
        learn = 1.0 / (1.0 + jnp.exp(-speed))
        masks = head_masks(group)
        removal = k * lax.rsqrt(head_sum(k * k, masks) + key_epsilon)
        d0 = log_decay.astype(bf16)
        rest = log_decay - d0.astype(f32)
        d1 = rest.astype(bf16)
        d2 = (rest - d1.astype(f32)).astype(bf16)
        cum = dot_nn(ones, d0) + dot_nn(ones, d1) + dot_nn(ones, d2)
        middle = cum[TOK // 2 : TOK // 2 + 1, :]
        forward = jnp.exp(cum - middle)
        backward = jnp.exp(middle - cum)
        undo = jnp.exp(-log_decay)
        right = learn * removal
        removers = -removal * undo * forward
        queries = q * forward
        sources = halves(jnp.concatenate([right * backward, k * backward], 0))
        final = cum[TOK - 1 : TOK, :]
        tail = jnp.exp(final - cum)
        grown_ref[slot] = q * jnp.exp(cum)
        put(4, slot, 1)
        slots.append(
            dict(
                masks=masks,
                v=v_ref[group, :, lanes],
                start=-removal * jnp.exp(cum - log_decay),
                ends=jnp.concatenate([right * tail, k * tail], 0).astype(bf16),
                kept=jnp.exp(final),
            )
        )
        for mask in masks:
            pairs = mm_nt(halves(masked(removers, mask)), sources)
            reads = dot_nt(masked(queries, mask).astype(bf16), sources[0])
            head = len(heads)
            qr_ref[head] = jnp.where(inclusive, reads[:, :TOK], 0.0).astype(bf16)
            qk_ref[head] = jnp.where(inclusive, reads[:, TOK:], 0.0).astype(bf16)
            put(1, head, 1)
            put(2, head, 1)
            heads.append(
                dict(
                    slot=slot,
                    mask=mask,
                    n=jnp.where(strict, pairs[:, :TOK], 0.0),
                    rk=jnp.where(strict, pairs[:, TOK:], 0.0),
                )
            )
    same = (row // 8) == (col // 8)
    for head in heads:
        head["m"] = jnp.where(same, head["n"], 0.0)
        head["x"] = eye + head["m"]
    for _ in range(2):
        for head in heads:
            m = halves(head["m"])
            head["m"] = mm(m, m)
        for head in heads:
            head["x"] = head["x"] + mm(halves(head["x"]), halves(head["m"]))
    size = 8
    while size < TOK:
        below = (row // (2 * size) == col // (2 * size)) & (row // size != col // size)
        for head in heads:
            off = halves(jnp.where(below, head["n"], 0.0))
            head["y"] = halves(mm(off, halves(head["x"])))
        for head in heads:
            head["x"] = head["x"] + mm(halves(head["x"]), head["y"])
        size *= 2
    for head in heads:
        part = slots[head["slot"]]
        high, low = halves(head["rk"])
        v = part["v"]
        pulled = dot_nn(jnp.concatenate([high, low], 1), jnp.concatenate([v, v], 0))
        target = jnp.concatenate([pulled, part["start"]], 1).astype(bf16)
        head["solved"] = dot_nn(
            jnp.concatenate(halves(head["x"]), 1), jnp.concatenate([target, target], 0)
        )
    for slot, part in enumerate(slots):
        mine = [head for head in heads if head["slot"] == slot]
        solved = mine[0]["solved"]
        if len(mine) == 2:
            first = jnp.concatenate([mine[0]["mask"]] * 2, 1) > 0.5
            solved = jnp.where(first, solved, mine[1]["solved"])
        solved = solved.astype(bf16)
        solved_ref[slot] = solved
        put(3, slot, 1)
        carried, start = solved[:, :LANES], solved[:, LANES:]
        transit = dot_tn(start, part["ends"][:TOK])
        added = dot_tn(jnp.concatenate([carried, part["v"]], 0), part["ends"])
        if len(mine) == 2:
            block = (row // HALF) == (col // HALF)
            transit = jnp.where(block, transit, 0.0)
            added = jnp.where(block, added, 0.0)
        transit = (transit + eye * part["kept"]).astype(bf16)
        added = added.astype(bf16)
        for half in range(2):
            send_ref[2 * slot + half, :LANES, :] = transit
            send_ref[2 * slot + half, LANES:, :] = added[half * HALF : (half + 1) * HALF, :]
        put(0, slot, 2)
    finish()


def read_kernel(*refs):
    inputs, outputs, scratch, results = refs[:10], refs[10:14], refs[14:24], refs[24:28]
    sems, out_sems = refs[28:]
    qr_ref, qk_ref, solved_ref, grown_ref, q_ref, k_ref, v_ref, gate_ref, gain_ref, own_ref = scratch
    out_ref, read_ref, scale_ref, extra_ref = results
    for copy in fetch(inputs, scratch, sems):
        copy.wait()
    put, finish = writer(results, outputs, out_sems)
    head = 0
    for slot in range(4):
        group, lanes = slot_lanes(slot)
        masks = head_masks(group)
        v = v_ref[group, :, lanes]
        found = local = None
        for mask in masks:
            one = dot_nn(qr_ref[head], solved_ref[slot])
            here = one[:, :LANES] + dot_nn(qk_ref[head], v)
            if found is None:
                found, local = one[:, LANES:], here
            else:
                found = jnp.where(mask > 0.5, one[:, LANES:], found)
                local = jnp.where(mask > 0.5, here, local)
            head += 1
        out_ref[slot] = local
        high, low = halves(grown_ref[slot] + found)
        read_ref[slot, :, :LANES] = high
        read_ref[slot, :, LANES:] = low
        gate = gate_ref[group, :, lanes].astype(f32)
        scale_ref[slot] = gain_ref[group : group + 1, lanes] * gate
        q = q_ref[group, :, lanes].astype(f32)
        k = k_ref[group, :, lanes].astype(f32)
        own = head_sum(q * k * own_ref[group : group + 1, lanes], masks)
        extra_ref[slot] = own * v.astype(f32) * gate
        for which in range(4):
            put(which, slot, 1)
    finish()


def row_kernel(got_ref, prefix_ref, total_ref):
    row = lax.broadcasted_iota(jnp.int32, (LANES + HALF, LANES), 0)
    col = lax.broadcasted_iota(jnp.int32, (LANES + HALF, LANES), 1)
    zero = jnp.zeros((LANES, LANES), f32)
    prefix_ref[0] = (row == col).astype(f32)
    run = got_ref[0].astype(f32)
    for k in range(1, SHARES):
        prefix_ref[k] = run
        got = got_ref[k]
        step = got[:LANES]
        high, low = halves(run)
        run = dot_nn(jnp.concatenate([high, low], 1), jnp.concatenate([step, step], 0))
        run = run + jnp.concatenate([zero, got[LANES:].astype(f32)], 0)
    total = run.astype(bf16)
    for k in range(total_ref.shape[0]):
        total_ref[k] = total


def state_kernel(place_ref, every_ref, prefix_ref, send_ref):
    place = place_ref[0]
    state = jnp.zeros((HALF, LANES), f32)
    for k in range(every_ref.shape[0] - 1):
        got = every_ref[k]
        step = got[:LANES]
        high, low = halves(state)
        grown = dot_nn(jnp.concatenate([high, low], 1), jnp.concatenate([step, step], 0))
        state = jnp.where(k < place, grown + got[LANES:].astype(f32), state)
    split = halves(state)
    for k in range(SHARES):
        moved = mm(split, halves(prefix_ref[k, :LANES, :]))
        send_ref[k] = (moved + prefix_ref[k, LANES:, :]).astype(bf16)


def mix_kernel(*refs):
    inputs, outputs, scratch, results, sems, out_sems = (
        refs[:6],
        refs[6:7],
        refs[7:13],
        refs[13:14],
        refs[14],
        refs[15],
    )
    state_ref, out_ref, read_ref, scale_ref, extra_ref, w_ref = scratch
    copies = fetch(inputs, scratch, sems)
    put, finish = writer(results, outputs, out_sems)
    for copy in copies[:5]:
        copy.wait()
    mixed = []
    for slot in range(4):
        width = HALF if slot < 2 else LANES
        masks = head_masks(slot // 2)
        state = jnp.concatenate([state_ref[2 * slot], state_ref[2 * slot + 1]], 0)
        raw = out_ref[slot] + dot_nt(read_ref[slot], jnp.concatenate([state, state], 1))
        centered = raw - head_sum(raw, masks) * (1.0 / width)
        variance = head_sum(centered * centered, masks) * (1.0 / width)
        normed = centered * lax.rsqrt(variance + head_epsilon) * scale_ref[slot]
        mixed.append((normed + extra_ref[slot]).astype(bf16))
    mixed = jnp.concatenate(mixed, 1)
    copies[5].wait()
    tiles, _, columns = results[0].shape
    for k in range(tiles):
        results[0][k] = dot_nn(mixed, w_ref[:, k * columns : (k + 1) * columns]).astype(bf16)
        put(0, k, 1)
    finish()


AHEAD = 24


def feed_kernel(
    far_ref,
    x_ref,
    gain_in_ref,
    whole_ref,
    sent_ref,
    w_ref,
    n_ref,
    acc_ref,
    gain_ref,
    y_ref,
    sems,
    in_sems,
    out_sems,
):
    (gain_here,) = fetch([gain_in_ref], [gain_ref], in_sems)
    put, finish = writer([y_ref], [sent_ref], out_sems)
    planes, sides, near, rows, width = w_ref.shape
    third = width // 3
    far = far_ref[0]
    parts = [pl.ds(0, 2 * third), pl.ds(2 * third, third)]
    copies = [
        pltpu.make_async_copy(
            whole_ref.at[k, :, jnp.where(far == side, 0, 1), :, lanes],
            w_ref.at[k, side, :, :, lanes],
            sems.at[part, k, side],
        )
        for part, lanes in enumerate(parts)
        for k in range(planes)
        for side in range(sides)
    ]
    for copy in copies[:AHEAD]:
        copy.start()

    def arrive(part, first, count):
        start = (part * planes + first) * sides
        for k in range(start, start + count * sides):
            copies[k].wait()
            if k + AHEAD < len(copies):
                copies[k + AHEAD].start()

    shares, tokens, columns = x_ref.shape
    tiles = shares // sides
    gain_here.wait()
    scales = []
    for side in range(sides):
        total = 0.0
        for k in range(tiles):
            lanes = slice(k * columns, (k + 1) * columns)
            a = x_ref[side * tiles + k].astype(f32)
            n_ref[side * tokens : (side + 1) * tokens, lanes] = (a * gain_ref[:, lanes]).astype(
                bf16
            )
            total = total + jnp.sum(a * a, axis=1, keepdims=True)
        scales.append(lax.rsqrt(total * (1.0 / (tiles * columns)) + norm_epsilon))
    scale = jnp.concatenate(scales, 0)
    block = sides * near * rows
    for k in range(0, planes, 2):
        arrive(0, k, 2)
        part = dot_nn(
            n_ref[:, k * block : (k + 2) * block],
            w_ref[k : k + 2, :, :, :, : 2 * third].reshape(2 * block, 2 * third),
        )
        if k == 0:
            acc_ref[...] = part
        else:
            acc_ref[...] += part
    gate = acc_ref[:, :third] * scale
    up = acc_ref[:, third:] * scale
    active = (gate / (1.0 + jnp.exp(-gate)) * up).astype(bf16)
    per = planes // tiles
    for k in range(tiles):
        arrive(1, k * per, per)
        down = w_ref[k * per : (k + 1) * per, :, :, :, 2 * third :].reshape(per * block, third)
        out = dot_nt(active, down).astype(bf16)
        for side in range(sides):
            y_ref[side * tiles + k] = out[side * tokens : (side + 1) * tokens]
            put(0, side * tiles + k, 1)
    finish()


def feed_forward(far, state, gain, whole):
    planes, near, sides, rows, width = whole.shape
    shares, tokens, columns = state.shape
    return pl.pallas_call(
        feed_kernel,
        out_shape=array((shares, tokens, columns), bf16),
        in_specs=[SMEM, VMEM, HBM, HBM],
        out_specs=HBM,
        scratch_shapes=[
            pltpu.VMEM((planes, sides, near, rows, width), bf16),
            pltpu.VMEM((sides * tokens, gain.shape[1]), bf16),
            pltpu.VMEM((sides * tokens, 2 * width // 3), f32),
            pltpu.VMEM(gain.shape, f32),
            pltpu.VMEM(state.shape, bf16),
            pltpu.SemaphoreType.DMA((2, planes, sides)),
            pltpu.SemaphoreType.DMA((1,)),
            pltpu.SemaphoreType.DMA((1, shares)),
        ],
        compiler_params=pltpu.CompilerParams(vmem_limit_bytes=52_000_000),
    )(far, state, gain, whole)


def pack_kernel(far_ref, *refs):
    inputs, outputs, scratch, (kept_ref, given_ref), sems, out_sems = (
        refs[:3],
        refs[3:5],
        refs[5:8],
        refs[8:10],
        refs[10],
        refs[11],
    )
    rows = given_ref.shape[0]
    puts = []
    copies = fetch(inputs, scratch, sems)
    wide = kept_ref.shape[1] // 3
    first = far_ref[0] == 0
    for k, copy in enumerate(copies):
        copy.wait()
        lanes = slice(k * wide, (k + 1) * wide)
        near = scratch[k][:, :wide]
        rest = scratch[k][:, wide:]
        blank = jnp.zeros((rest.shape[0], 2 * wide - scratch[k].shape[1]), bf16)
        far = jnp.concatenate([rest, blank], axis=1)
        kept_ref[:rows, lanes] = jnp.where(first, near, far)
        given_ref[:, lanes] = jnp.where(first, far, near)
        window = (pl.ds(0, rows), pl.ds(k * wide, wide))
        for which, (a, b) in enumerate(zip((kept_ref, given_ref), outputs)):
            put = pltpu.make_async_copy(a.at[window], b.at[window], out_sems.at[which, k])
            put.start()
            puts.append(put)
    for put in puts:
        put.wait()


def swapped(far, parts):
    rows, hidden = parts[0].shape
    wide = -(-hidden // (2 * LANES)) * LANES
    packed = (array((2 * rows, 3 * wide), bf16), array((rows, 3 * wide), bf16))
    kept, given = call(pack_kernel, packed, [SMEM] + [HBM] * 3, parts, 62_000_000, 3)(far, *parts)
    return kept, lax.ppermute(given, FAR, [(0, 1), (1, 0)])


def gathered(kept, taken):
    rows, width = taken.shape
    both = lax.dynamic_update_slice(kept, taken, (rows, 0))
    whole = lax.all_gather(both, GATHER, axis=0, tiled=True)
    planes = lax.axis_size(PLANE)
    near = lax.axis_size(NEAR) * lax.axis_size(CORE)
    return whole.reshape(planes, near, 2, rows, width)


VMEM = pl.BlockSpec(memory_space=pltpu.VMEM)
HBM = pl.BlockSpec(memory_space=pltpu.HBM)
SMEM = pl.BlockSpec(memory_space=pltpu.SMEM)


def call(kernel, outs, specs, fetched=(), limit=24 * 1024 * 1024, written=0, sems=()):
    scratch = [pltpu.VMEM(a.shape, a.dtype) for a in fetched]
    where = VMEM
    if written:
        where = HBM
        scratch += [pltpu.VMEM(a.shape, a.dtype) for a in outs]
    scratch += [pltpu.SemaphoreType.DMA(a) for a in sems or [(len(fetched),)] if fetched]
    if written:
        scratch.append(pltpu.SemaphoreType.DMA((len(outs), written)))
    return pl.pallas_call(
        kernel,
        out_shape=outs,
        in_specs=specs,
        out_specs=jax.tree.map(lambda _: where, outs),
        scratch_shapes=scratch,
        compiler_params=pltpu.CompilerParams(vmem_limit_bytes=limit),
    )


def array(dims, kind):
    return jax.ShapeDtypeStruct(dims, kind)


def exchange(value, axis):
    return lax.all_to_all(value, axis, 0, 0, tiled=True)


def from_everyone(value, axis):
    devices = lax.psum(1, axis)
    return exchange(jnp.broadcast_to(value[None], (devices, *value.shape)), axis)


def on_device(
    stratum_source_matrix,
    acceptance_query,
    cluster_lookup_matrix,
    cluster_payload_matrix,
    fading_logit,
    adaptation_speed_logit,
    additional_fading_exponent,
    result_switch_pair,
    attender_scaling_factor,
    present_item_factor,
    final_mapping_matrix,
    perceptron_scaling_factor,
    switching_matrix,
    widening_matrix,
    shrinking_matrix,
):
    features = perceptron_scaling_factor.shape[0]
    columns = features // lax.axis_size(TP)
    far = lax.axis_index(FAR).astype(jnp.int32).reshape(1)
    kept, taken = swapped(far, [switching_matrix, widening_matrix, shrinking_matrix.T])
    blocks = array((4, TOK, LANES), f32)
    pairs = array((6, TOK, TOK), bf16)
    doubled = array((4, TOK, 2 * LANES), bf16)
    inputs = (
        acceptance_query,
        cluster_lookup_matrix,
        cluster_payload_matrix,
        fading_logit,
        adaptation_speed_logit,
        additional_fading_exponent,
    )
    send, *found = call(
        solve_kernel,
        (array((SHARES, LANES + HALF, LANES), bf16), pairs, pairs, doubled, blocks),
        [HBM] * len(inputs),
        inputs,
        65_900_000,
        6,
        [(len(inputs), 2)],
    )(*inputs)
    place = lax.axis_index(PLANE).astype(jnp.int32).reshape(1)
    first_column = (lax.axis_index(TP) * columns).astype(jnp.uint32)
    send, place, first_column = lax.optimization_barrier((send, place, first_column))
    whole = gathered(kept, taken)
    planes = lax.axis_size(PLANE)
    prefix, total = call(
        row_kernel,
        (
            array((SHARES, LANES + HALF, LANES), f32),
            array((planes, LANES + HALF, LANES), bf16),
        ),
        [VMEM],
    )(exchange(send, ROW))
    total, first_column, *found = lax.optimization_barrier((total, first_column, *found))
    reading = (
        *found,
        *inputs[:3],
        result_switch_pair,
        attender_scaling_factor,
        present_item_factor,
    )
    read = call(
        read_kernel,
        (blocks, doubled, blocks, blocks),
        [HBM] * len(reading),
        reading,
        64_500_000,
        4,
    )(*reading)
    residual = lax.dynamic_slice(
        stratum_source_matrix, (jnp.uint32(0), first_column), (TOK, columns)
    )
    every, residual, *read = lax.optimization_barrier((exchange(total, PLANE), residual, *read))
    states = call(state_kernel, array((SHARES, HALF, LANES), bf16), [SMEM, VMEM, VMEM])(
        place, every, prefix
    )
    mixing = (exchange(states, ROW), *read, final_mapping_matrix.reshape(-1, features))
    (terms,) = call(
        mix_kernel,
        (array((features // columns, TOK, columns), bf16),),
        [HBM] * len(mixing),
        mixing,
        64_000_000,
        features // columns,
    )(*mixing)
    attention = jnp.sum(exchange(terms, TP).astype(f32), axis=0)
    own_state = (residual.astype(f32) + attention).astype(bf16)
    tiles = feed_forward(
        far,
        from_everyone(own_state, POOL),
        perceptron_scaling_factor.reshape(1, features),
        whole,
    )
    mixer = jnp.sum(exchange(tiles, POOL).astype(f32), axis=0)
    return (own_state.astype(f32) + mixer).astype(bf16)


def solution(mesh):
    split = Mesh(mesh.devices.reshape(8, 2, 2, 2, mesh.shape["tp"]), (*SP, TP))
    heads = P(None, SP, "tp")
    return jax.shard_map(
        on_device,
        mesh=split,
        in_specs=(
            P(SP, None),
            heads,
            heads,
            heads,
            heads,
            heads,
            heads,
            heads,
            P(None, TP),
            P(None, TP),
            P(None, TP, None),
            P(),
            P(SP, TP),
            P(SP, TP),
            P(TP, SP),
        ),
        out_specs=P(SP, TP),
        check_vma=False,
    )
```

```python
import jax
import jax.numpy as jnp
from jax import lax
from jax.experimental import pallas as pl
from jax.experimental.pallas import tpu as pltpu
from jax.sharding import Mesh
from jax.sharding import PartitionSpec as P

PLANE, FAR, NEAR, CORE, TP = "plane", "far", "near", "core", "tp"
SP = (PLANE, FAR, NEAR, CORE)
ROW = (FAR, NEAR, CORE)
GATHER = (PLANE, NEAR, CORE)
POOL = (FAR, TP)
TOK = 128
LANES = 128
HALF = 64
SHARES = 8

norm_epsilon = 1e-06
head_epsilon = 0.00064
key_epsilon = 1e-06

f32 = jnp.float32
bf16 = jnp.bfloat16


def dot_nn(a, b):
    return lax.dot_general(a, b, (((1,), (0,)), ((), ())), preferred_element_type=f32)


def dot_nt(a, b):
    return lax.dot_general(a, b, (((1,), (1,)), ((), ())), preferred_element_type=f32)


def dot_tn(a, b):
    return lax.dot_general(a, b, (((0,), (0,)), ((), ())), preferred_element_type=f32)


def halves(a):
    high = a.astype(bf16)
    return high, (a - high.astype(f32)).astype(bf16)


def mm(a, b):
    ah, al = a
    bh, bl = b
    return dot_nn(jnp.concatenate([ah, al], 1), jnp.concatenate([bh, bh], 0)) + dot_nn(ah, bl)


def mm_nt(a, b):
    ah, al = a
    bh, bl = b
    return dot_nt(jnp.concatenate([ah, al], 1), jnp.concatenate([bh, bh], 1)) + dot_nt(ah, bl)


def head_masks(group):
    lane = lax.broadcasted_iota(jnp.int32, (1, LANES), 1)
    if group == 0:
        return [(lane < HALF).astype(f32), (lane >= HALF).astype(f32)]
    return [None]


def head_sum(a, masks):
    if masks[0] is None:
        return jnp.sum(a, axis=1, keepdims=True)
    return sum(jnp.sum(a * m, axis=1, keepdims=True) * m for m in masks)


def masked(a, mask):
    return a if mask is None else a * mask


def fetch(sources, targets, sems):
    copies = [pltpu.make_async_copy(a, b, sems.at[k]) for k, (a, b) in enumerate(zip(sources, targets))]
    for copy in copies:
        copy.start()
    return copies


def slot_lanes(slot):
    cut = (slot % 2) * LANES
    return slot // 2, slice(cut, cut + LANES)


def group_copies(inputs, scratch, sems):
    copies = [
        [
            pltpu.make_async_copy(a.at[group], b.at[group], sems.at[k, group])
            for k, (a, b) in enumerate(zip(inputs, scratch))
        ]
        for group in range(2)
    ]
    for copy in copies[0] + copies[1]:
        copy.start()
    return copies


def writer(results, outputs, sems):
    pending = []

    def put(which, index, count):
        part = pl.ds(index * count, count)
        copy = pltpu.make_async_copy(
            results[which].at[part], outputs[which].at[part], sems.at[which, index]
        )
        copy.start()
        pending.append(copy)

    def finish():
        for copy in pending:
            copy.wait()

    return put, finish


def solve_kernel(*refs):
    inputs, outputs, scratch, results = refs[:6], refs[6:11], refs[11:17], refs[17:22]
    sems, out_sems = refs[22:]
    send_ref, qr_ref, qk_ref, solved_ref, grown_ref = results
    q_ref, k_ref, v_ref, f_ref, l_ref, e_ref = scratch
    copies = group_copies(inputs, scratch, sems)
    put, finish = writer(results, outputs, out_sems)
    row = lax.broadcasted_iota(jnp.int32, (TOK, TOK), 0)
    col = lax.broadcasted_iota(jnp.int32, (TOK, TOK), 1)
    strict = row > col
    inclusive = row >= col
    eye = (row == col).astype(f32)
    ones = inclusive.astype(bf16)
    slots = []
    heads = []
    for slot in range(4):
        group, lanes = slot_lanes(slot)
        if slot % 2 == 0:
            for copy in copies[group]:
                copy.wait()
        q = q_ref[group, :, lanes].astype(f32)
        k = k_ref[group, :, lanes].astype(f32)
        fade = f_ref[group, :, lanes].astype(f32)
        speed = l_ref[group, :, lanes].astype(f32)
        log_decay = e_ref[group, :, lanes] - jnp.exp(-0.5) / (1.0 + jnp.exp(-fade))
        learn = 1.0 / (1.0 + jnp.exp(-speed))
        masks = head_masks(group)
        removal = k * lax.rsqrt(head_sum(k * k, masks) + key_epsilon)
        d0 = log_decay.astype(bf16)
        rest = log_decay - d0.astype(f32)
        d1 = rest.astype(bf16)
        d2 = (rest - d1.astype(f32)).astype(bf16)
        cum = dot_nn(ones, d0) + dot_nn(ones, d1) + dot_nn(ones, d2)
        middle = cum[TOK // 2 : TOK // 2 + 1, :]
        forward = jnp.exp(cum - middle)
        backward = jnp.exp(middle - cum)
        undo = jnp.exp(-log_decay)
        right = learn * removal
        removers = -removal * undo * forward
        queries = q * forward
        sources = halves(jnp.concatenate([right * backward, k * backward], 0))
        final = cum[TOK - 1 : TOK, :]
        tail = jnp.exp(final - cum)
        grown_ref[slot] = q * jnp.exp(cum)
        put(4, slot, 1)
        slots.append(
            dict(
                masks=masks,
                v=v_ref[group, :, lanes],
                start=-removal * jnp.exp(cum - log_decay),
                ends=jnp.concatenate([right * tail, k * tail], 0).astype(bf16),
                kept=jnp.exp(final),
            )
        )
        for mask in masks:
            pairs = mm_nt(halves(masked(removers, mask)), sources)
            reads = dot_nt(masked(queries, mask).astype(bf16), sources[0])
            head = len(heads)
            qr_ref[head] = jnp.where(inclusive, reads[:, :TOK], 0.0).astype(bf16)
            qk_ref[head] = jnp.where(inclusive, reads[:, TOK:], 0.0).astype(bf16)
            put(1, head, 1)
            put(2, head, 1)
            heads.append(
                dict(
                    slot=slot,
                    mask=mask,
                    n=jnp.where(strict, pairs[:, :TOK], 0.0),
                    rk=jnp.where(strict, pairs[:, TOK:], 0.0),
                )
            )
    same = (row // 8) == (col // 8)
    for head in heads:
        head["m"] = jnp.where(same, head["n"], 0.0)
        head["x"] = eye + head["m"]
    for _ in range(2):
        for head in heads:
            m = halves(head["m"])
            head["m"] = mm(m, m)
        for head in heads:
            head["x"] = head["x"] + mm(halves(head["x"]), halves(head["m"]))
    size = 8
    while size < TOK:
        below = (row // (2 * size) == col // (2 * size)) & (row // size != col // size)
        for head in heads:
            off = halves(jnp.where(below, head["n"], 0.0))
            head["y"] = halves(mm(off, halves(head["x"])))
        for head in heads:
            head["x"] = head["x"] + mm(halves(head["x"]), head["y"])
        size *= 2
    for head in heads:
        part = slots[head["slot"]]
        high, low = halves(head["rk"])
        v = part["v"]
        pulled = dot_nn(jnp.concatenate([high, low], 1), jnp.concatenate([v, v], 0))
        target = jnp.concatenate([pulled, part["start"]], 1).astype(bf16)
        head["solved"] = dot_nn(
            jnp.concatenate(halves(head["x"]), 1), jnp.concatenate([target, target], 0)
        )
    for slot, part in enumerate(slots):
        mine = [head for head in heads if head["slot"] == slot]
        solved = mine[0]["solved"]
        if len(mine) == 2:
            first = jnp.concatenate([mine[0]["mask"]] * 2, 1) > 0.5
            solved = jnp.where(first, solved, mine[1]["solved"])
        solved = solved.astype(bf16)
        solved_ref[slot] = solved
        put(3, slot, 1)
        carried, start = solved[:, :LANES], solved[:, LANES:]
        transit = dot_tn(start, part["ends"][:TOK])
        added = dot_tn(jnp.concatenate([carried, part["v"]], 0), part["ends"])
        if len(mine) == 2:
            block = (row // HALF) == (col // HALF)
            transit = jnp.where(block, transit, 0.0)
            added = jnp.where(block, added, 0.0)
        transit = (transit + eye * part["kept"]).astype(bf16)
        added = added.astype(bf16)
        for half in range(2):
            send_ref[2 * slot + half, :LANES, :] = transit
            send_ref[2 * slot + half, LANES:, :] = added[half * HALF : (half + 1) * HALF, :]
        put(0, slot, 2)
    finish()


def read_kernel(*refs):
    inputs, outputs, scratch, results = refs[:10], refs[10:14], refs[14:24], refs[24:28]
    sems, out_sems = refs[28:]
    qr_ref, qk_ref, solved_ref, grown_ref, q_ref, k_ref, v_ref, gate_ref, gain_ref, own_ref = scratch
    out_ref, read_ref, scale_ref, extra_ref = results
    for copy in fetch(inputs, scratch, sems):
        copy.wait()
    put, finish = writer(results, outputs, out_sems)
    head = 0
    for slot in range(4):
        group, lanes = slot_lanes(slot)
        masks = head_masks(group)
        v = v_ref[group, :, lanes]
        found = local = None
        for mask in masks:
            one = dot_nn(qr_ref[head], solved_ref[slot])
            here = one[:, :LANES] + dot_nn(qk_ref[head], v)
            if found is None:
                found, local = one[:, LANES:], here
            else:
                found = jnp.where(mask > 0.5, one[:, LANES:], found)
                local = jnp.where(mask > 0.5, here, local)
            head += 1
        out_ref[slot] = local
        high, low = halves(grown_ref[slot] + found)
        read_ref[slot, :, :LANES] = high
        read_ref[slot, :, LANES:] = low
        gate = gate_ref[group, :, lanes].astype(f32)
        scale_ref[slot] = gain_ref[group : group + 1, lanes] * gate
        q = q_ref[group, :, lanes].astype(f32)
        k = k_ref[group, :, lanes].astype(f32)
        own = head_sum(q * k * own_ref[group : group + 1, lanes], masks)
        extra_ref[slot] = own * v.astype(f32) * gate
        for which in range(4):
            put(which, slot, 1)
    finish()


def row_kernel(got_ref, prefix_ref, total_ref):
    row = lax.broadcasted_iota(jnp.int32, (LANES + HALF, LANES), 0)
    col = lax.broadcasted_iota(jnp.int32, (LANES + HALF, LANES), 1)
    zero = jnp.zeros((LANES, LANES), f32)
    prefix_ref[0] = (row == col).astype(f32)
    run = got_ref[0].astype(f32)
    for k in range(1, SHARES):
        prefix_ref[k] = run
        got = got_ref[k]
        step = got[:LANES]
        high, low = halves(run)
        run = dot_nn(jnp.concatenate([high, low], 1), jnp.concatenate([step, step], 0))
        run = run + jnp.concatenate([zero, got[LANES:].astype(f32)], 0)
    total = run.astype(bf16)
    for k in range(total_ref.shape[0]):
        total_ref[k] = total


def state_kernel(place_ref, every_ref, prefix_ref, send_ref):
    place = place_ref[0]
    state = jnp.zeros((HALF, LANES), f32)
    for k in range(every_ref.shape[0] - 1):
        got = every_ref[k]
        step = got[:LANES]
        high, low = halves(state)
        grown = dot_nn(jnp.concatenate([high, low], 1), jnp.concatenate([step, step], 0))
        state = jnp.where(k < place, grown + got[LANES:].astype(f32), state)
    split = halves(state)
    for k in range(SHARES):
        moved = mm(split, halves(prefix_ref[k, :LANES, :]))
        send_ref[k] = (moved + prefix_ref[k, LANES:, :]).astype(bf16)


def mix_kernel(*refs):
    inputs, outputs, scratch, results, sems, out_sems = (
        refs[:6],
        refs[6:7],
        refs[7:13],
        refs[13:14],
        refs[14],
        refs[15],
    )
    state_ref, out_ref, read_ref, scale_ref, extra_ref, w_ref = scratch
    copies = fetch(inputs, scratch, sems)
    put, finish = writer(results, outputs, out_sems)
    for copy in copies[:5]:
        copy.wait()
    mixed = []
    for slot in range(4):
        width = HALF if slot < 2 else LANES
        masks = head_masks(slot // 2)
        state = jnp.concatenate([state_ref[2 * slot], state_ref[2 * slot + 1]], 0)
        raw = out_ref[slot] + dot_nt(read_ref[slot], jnp.concatenate([state, state], 1))
        centered = raw - head_sum(raw, masks) * (1.0 / width)
        variance = head_sum(centered * centered, masks) * (1.0 / width)
        normed = centered * lax.rsqrt(variance + head_epsilon) * scale_ref[slot]
        mixed.append((normed + extra_ref[slot]).astype(bf16))
    mixed = jnp.concatenate(mixed, 1)
    copies[5].wait()
    tiles, _, columns = results[0].shape
    for k in range(tiles):
        results[0][k] = dot_nn(mixed, w_ref[:, k * columns : (k + 1) * columns]).astype(bf16)
        put(0, k, 1)
    finish()


AHEAD = 24


def feed_kernel(
    far_ref,
    x_ref,
    gain_in_ref,
    whole_ref,
    sent_ref,
    w_ref,
    n_ref,
    acc_ref,
    gain_ref,
    y_ref,
    sems,
    in_sems,
    out_sems,
):
    (gain_here,) = fetch([gain_in_ref], [gain_ref], in_sems)
    put, finish = writer([y_ref], [sent_ref], out_sems)
    planes, sides, near, rows, width = w_ref.shape
    third = width // 3
    far = far_ref[0]
    parts = [pl.ds(0, 2 * third), pl.ds(2 * third, third)]
    copies = [
        pltpu.make_async_copy(
            whole_ref.at[k, :, jnp.where(far == side, 0, 1), :, lanes],
            w_ref.at[k, side, :, :, lanes],
            sems.at[part, k, side],
        )
        for part, lanes in enumerate(parts)
        for k in range(planes)
        for side in range(sides)
    ]
    for copy in copies[:AHEAD]:
        copy.start()

    def arrive(part, first, count):
        start = (part * planes + first) * sides
        for k in range(start, start + count * sides):
            copies[k].wait()
            if k + AHEAD < len(copies):
                copies[k + AHEAD].start()

    shares, tokens, columns = x_ref.shape
    tiles = shares // sides
    gain_here.wait()
    scales = []
    for side in range(sides):
        total = 0.0
        for k in range(tiles):
            lanes = slice(k * columns, (k + 1) * columns)
            a = x_ref[side * tiles + k].astype(f32)
            n_ref[side * tokens : (side + 1) * tokens, lanes] = (a * gain_ref[:, lanes]).astype(
                bf16
            )
            total = total + jnp.sum(a * a, axis=1, keepdims=True)
        scales.append(lax.rsqrt(total * (1.0 / (tiles * columns)) + norm_epsilon))
    scale = jnp.concatenate(scales, 0)
    block = sides * near * rows
    for k in range(0, planes, 2):
        arrive(0, k, 2)
        part = dot_nn(
            n_ref[:, k * block : (k + 2) * block],
            w_ref[k : k + 2, :, :, :, : 2 * third].reshape(2 * block, 2 * third),
        )
        if k == 0:
            acc_ref[...] = part
        else:
            acc_ref[...] += part
    gate = acc_ref[:, :third] * scale
    up = acc_ref[:, third:] * scale
    active = (gate / (1.0 + jnp.exp(-gate)) * up).astype(bf16)
    per = planes // tiles
    for k in range(tiles):
        arrive(1, k * per, per)
        down = w_ref[k * per : (k + 1) * per, :, :, :, 2 * third :].reshape(per * block, third)
        out = dot_nt(active, down).astype(bf16)
        for side in range(sides):
            y_ref[side * tiles + k] = out[side * tokens : (side + 1) * tokens]
            put(0, side * tiles + k, 1)
    finish()


def feed_forward(far, state, gain, whole):
    planes, near, sides, rows, width = whole.shape
    shares, tokens, columns = state.shape
    return pl.pallas_call(
        feed_kernel,
        out_shape=array((shares, tokens, columns), bf16),
        in_specs=[SMEM, VMEM, HBM, HBM],
        out_specs=HBM,
        scratch_shapes=[
            pltpu.VMEM((planes, sides, near, rows, width), bf16),
            pltpu.VMEM((sides * tokens, gain.shape[1]), bf16),
            pltpu.VMEM((sides * tokens, 2 * width // 3), f32),
            pltpu.VMEM(gain.shape, f32),
            pltpu.VMEM(state.shape, bf16),
            pltpu.SemaphoreType.DMA((2, planes, sides)),
            pltpu.SemaphoreType.DMA((1,)),
            pltpu.SemaphoreType.DMA((1, shares)),
        ],
        compiler_params=pltpu.CompilerParams(vmem_limit_bytes=52_000_000),
    )(far, state, gain, whole)


def pack_kernel(far_ref, *refs):
    inputs, outputs, scratch, (kept_ref, given_ref), sems, out_sems = (
        refs[:3],
        refs[3:5],
        refs[5:8],
        refs[8:10],
        refs[10],
        refs[11],
    )
    rows = given_ref.shape[0]
    puts = []
    copies = fetch(inputs, scratch, sems)
    wide = kept_ref.shape[1] // 3
    first = far_ref[0] == 0
    for k, copy in enumerate(copies):
        copy.wait()
        lanes = slice(k * wide, (k + 1) * wide)
        near = scratch[k][:, :wide]
        rest = scratch[k][:, wide:]
        blank = jnp.zeros((rest.shape[0], 2 * wide - scratch[k].shape[1]), bf16)
        far = jnp.concatenate([rest, blank], axis=1)
        kept_ref[:rows, lanes] = jnp.where(first, near, far)
        given_ref[:, lanes] = jnp.where(first, far, near)
        window = (pl.ds(0, rows), pl.ds(k * wide, wide))
        for which, (a, b) in enumerate(zip((kept_ref, given_ref), outputs)):
            put = pltpu.make_async_copy(a.at[window], b.at[window], out_sems.at[which, k])
            put.start()
            puts.append(put)
    for put in puts:
        put.wait()


def swapped(far, parts):
    rows, hidden = parts[0].shape
    wide = -(-hidden // (2 * LANES)) * LANES
    packed = (array((2 * rows, 3 * wide), bf16), array((rows, 3 * wide), bf16))
    kept, given = call(pack_kernel, packed, [SMEM] + [HBM] * 3, parts, 62_000_000, 3)(far, *parts)
    return kept, lax.ppermute(given, FAR, [(0, 1), (1, 0)])


def gathered(kept, taken):
    rows, width = taken.shape
    both = lax.dynamic_update_slice(kept, taken, (rows, 0))
    whole = lax.all_gather(both, GATHER, axis=0, tiled=True)
    planes = lax.axis_size(PLANE)
    near = lax.axis_size(NEAR) * lax.axis_size(CORE)
    return whole.reshape(planes, near, 2, rows, width)


VMEM = pl.BlockSpec(memory_space=pltpu.VMEM)
HBM = pl.BlockSpec(memory_space=pltpu.HBM)
SMEM = pl.BlockSpec(memory_space=pltpu.SMEM)


def call(kernel, outs, specs, fetched=(), limit=24 * 1024 * 1024, written=0, sems=()):
    scratch = [pltpu.VMEM(a.shape, a.dtype) for a in fetched]
    where = VMEM
    if written:
        where = HBM
        scratch += [pltpu.VMEM(a.shape, a.dtype) for a in outs]
    scratch += [pltpu.SemaphoreType.DMA(a) for a in sems or [(len(fetched),)] if fetched]
    if written:
        scratch.append(pltpu.SemaphoreType.DMA((len(outs), written)))
    return pl.pallas_call(
        kernel,
        out_shape=outs,
        in_specs=specs,
        out_specs=jax.tree.map(lambda _: where, outs),
        scratch_shapes=scratch,
        compiler_params=pltpu.CompilerParams(vmem_limit_bytes=limit),
    )


def array(dims, kind):
    return jax.ShapeDtypeStruct(dims, kind)


def exchange(value, axis):
    return lax.all_to_all(value, axis, 0, 0, tiled=True)


def from_everyone(value, axis):
    devices = lax.psum(1, axis)
    return exchange(jnp.broadcast_to(value[None], (devices, *value.shape)), axis)


def on_device(
    stratum_source_matrix,
    acceptance_query,
    cluster_lookup_matrix,
    cluster_payload_matrix,
    fading_logit,
    adaptation_speed_logit,
    additional_fading_exponent,
    result_switch_pair,
    attender_scaling_factor,
    present_item_factor,
    final_mapping_matrix,
    perceptron_scaling_factor,
    switching_matrix,
    widening_matrix,
    shrinking_matrix,
):
    features = perceptron_scaling_factor.shape[0]
    columns = features // lax.axis_size(TP)
    far = lax.axis_index(FAR).astype(jnp.int32).reshape(1)
    kept, taken = swapped(far, [switching_matrix, widening_matrix, shrinking_matrix.T])
    blocks = array((4, TOK, LANES), f32)
    pairs = array((6, TOK, TOK), bf16)
    doubled = array((4, TOK, 2 * LANES), bf16)
    inputs = (
        acceptance_query,
        cluster_lookup_matrix,
        cluster_payload_matrix,
        fading_logit,
        adaptation_speed_logit,
        additional_fading_exponent,
    )
    send, *found = call(
        solve_kernel,
        (array((SHARES, LANES + HALF, LANES), bf16), pairs, pairs, doubled, blocks),
        [HBM] * len(inputs),
        inputs,
        65_900_000,
        6,
        [(len(inputs), 2)],
    )(*inputs)
    place = lax.axis_index(PLANE).astype(jnp.int32).reshape(1)
    first_column = (lax.axis_index(TP) * columns).astype(jnp.uint32)
    send, taken, place, first_column = lax.optimization_barrier((send, taken, place, first_column))
    whole = gathered(kept, taken)
    planes = lax.axis_size(PLANE)
    prefix, total = call(
        row_kernel,
        (
            array((SHARES, LANES + HALF, LANES), f32),
            array((planes, LANES + HALF, LANES), bf16),
        ),
        [VMEM],
    )(exchange(send, ROW))
    total, first_column, *found = lax.optimization_barrier((total, first_column, *found))
    reading = (
        *found,
        *inputs[:3],
        result_switch_pair,
        attender_scaling_factor,
        present_item_factor,
    )
    read = call(
        read_kernel,
        (blocks, doubled, blocks, blocks),
        [HBM] * len(reading),
        reading,
        64_500_000,
        4,
    )(*reading)
    residual = lax.dynamic_slice(
        stratum_source_matrix, (jnp.uint32(0), first_column), (TOK, columns)
    )
    every, residual, *read = lax.optimization_barrier((exchange(total, PLANE), residual, *read))
    states = call(state_kernel, array((SHARES, HALF, LANES), bf16), [SMEM, VMEM, VMEM])(
        place, every, prefix
    )
    mixing = (exchange(states, ROW), *read, final_mapping_matrix.reshape(-1, features))
    (terms,) = call(
        mix_kernel,
        (array((features // columns, TOK, columns), bf16),),
        [HBM] * len(mixing),
        mixing,
        64_000_000,
        features // columns,
    )(*mixing)
    attention = jnp.sum(exchange(terms, TP).astype(f32), axis=0)
    own_state = (residual.astype(f32) + attention).astype(bf16)
    tiles = feed_forward(
        far,
        from_everyone(own_state, POOL),
        perceptron_scaling_factor.reshape(1, features),
        whole,
    )
    mixer = jnp.sum(exchange(tiles, POOL).astype(f32), axis=0)
    return (own_state.astype(f32) + mixer).astype(bf16)


def solution(mesh):
    split = Mesh(mesh.devices.reshape(8, 2, 2, 2, mesh.shape["tp"]), (*SP, TP))
    heads = P(None, SP, "tp")
    return jax.shard_map(
        on_device,
        mesh=split,
        in_specs=(
            P(SP, None),
            heads,
            heads,
            heads,
            heads,
            heads,
            heads,
            heads,
            P(None, TP),
            P(None, TP),
            P(None, TP, None),
            P(),
            P(SP, TP),
            P(SP, TP),
            P(TP, SP),
        ),
        out_specs=P(SP, TP),
        check_vma=False,
    )
```
